128 devices in a mesh: sp: 16 (over z, x), tp: 8 (over y, core).
Axes of the slice: x: 4, y: 4, z: 4, core: 2. Of those that a mesh axis runs over, the one named last changes fastest.
Arguments:
- latent: bfloat16 [8192, 4096], P('sp'), may hold values from -64 to 64
- context: bfloat16 [1024, 4096], P('sp'), may hold values from -6 to 6
- condition: bfloat16 [4096], P('sp'), may hold values from -6 to 6
- context_condition: bfloat16 [4096], P('sp'), may hold values from -6 to 6
- shift_weight: bfloat16 [4096, 4096], P('sp', 'tp'), may hold values from -0.125 to 0.125
- scale_weight: bfloat16 [4096, 4096], P('sp', 'tp'), may hold values from -0.125 to 0.125
- gate_weight: bfloat16 [4096, 4096], P('sp', 'tp'), may hold values from -0.25 to 0.25
- norm_gain: float32 [4096], replicated, may hold values from 0.1 to 1.9
- query_weight: bfloat16 [4096, 2048], P(None, 'tp'), may hold values from -0.09375 to 0.09375
- key_weight: bfloat16 [4096, 2048], P(None, 'tp'), may hold values from -0.09375 to 0.09375
- value_weight: bfloat16 [4096, 2048], P(None, 'tp'), may hold values from -0.09375 to 0.09375
- write_weight: bfloat16 [4096, 2, 16], replicated, may hold values from -0.09375 to 0.09375
- decay_weight: bfloat16 [4096, 2, 16], replicated, may hold values from -0.09375 to 0.09375
- write_bias: float32 [2, 16], replicated, may hold values from -12 to 1
- decay_bias: float32 [2, 16], replicated, may hold values from -16 to -4
- log_rate: float32 [2, 16], replicated, may hold values from 0 to 1.4
- head_gain: float32 [128], replicated, may hold values from 0.1 to 1.9
- out_weight: bfloat16 [2048, 4096], P(None, 'tp'), may hold values from -0.125 to 0.125
Outputs:
- updated: bfloat16 [8192, 4096], P('sp', 'tp')
The draws below stay inside these ranges and needn't reach their ends.
All inputs are finite; a program needn't handle non-finite values.
Results may differ from the reference program's by a relative error of at most 0.013.
Values may be sent and summed in bfloat16 or wider, within the bound.
A program may use at most 128 MiB of HBM per device.

```python
import math
import jax
import jax.numpy as jnp
from jax import lax

D = 4096
HEADS = 16
HEAD_DIM = 128
BLOCK = 64
TOKENS = 8192
CTX = 1024


def draw_latent(key, part):
    segment_count = (TOKENS + 127) // 128
    offsets = jnp.clip(jax.random.normal(jax.random.fold_in(key, 22), (segment_count, D), jnp.float32), -3.0, 3.0)
    segment_index = jnp.arange(TOKENS) // 128
    noise = jnp.clip(jax.random.normal(jax.random.fold_in(key, 21), (TOKENS, D), jnp.float32), -6.0, 6.0)
    return (noise + offsets[segment_index]).astype(jnp.bfloat16)


def head_speeds(key):
    chooser = jax.random.uniform(jax.random.fold_in(key, 31), (2, HEADS), jnp.float32)
    return chooser < 0.7


def draw_decay_bias(key, part):
    keeping = head_speeds(key)
    spread = jax.random.uniform(jax.random.fold_in(key, 32), (2, HEADS), jnp.float32, -0.5, 0.5)
    slow_value = math.log(0.05 / (TOKENS + CTX)) + spread
    fast_value = -5.0 + spread
    return jnp.where(keeping, slow_value, fast_value).astype(jnp.float32)


def draw_write_bias(key, part):
    keeping = head_speeds(key)
    spread = jax.random.uniform(jax.random.fold_in(key, 33), (2, HEADS), jnp.float32, -0.5, 0.5)
    slow_value = math.log(HEAD_DIM / (TOKENS + CTX)) - 1.5 + spread
    fast_value = spread
    return jnp.where(keeping, slow_value, fast_value).astype(jnp.float32)


def block_levels(rng, shape, cuts, least, high):
    level = 1.0
    for position, blocks in cuts:
        draws = jax.random.uniform(jax.random.fold_in(jax.random.fold_in(rng, 6), position), (blocks,), jnp.float32, least / len(cuts), high / len(cuts))
        level = level * jnp.repeat(jnp.exp(draws), shape[position] // blocks).reshape((-1,) + (1,) * (len(shape) - 1 - position))
    return level


def gaussian(key, extent, scale, most, split=(), held_as=jnp.bfloat16):
    drawn = jax.random.normal(key, extent, jnp.float32) * scale
    if len(split) > 0:
        drawn = block_levels(key, extent, split, -0.22, 0.18) * drawn
    return jnp.clip(drawn, min=-most, max=most).astype(held_as)


def setup_inputs(seed: int = 0) -> dict:
    keys = jax.random.split(jax.random.key(seed), 19)
    return {
        "latent": draw_latent(jax.random.fold_in(keys[18], 71), 0),
        "context": gaussian(keys[1], (CTX, D), 1.0, 6.0, ((0, 16),)),
        "condition": gaussian(keys[2], (D,), 1.0, 6.0, ((0, 16),)),
        "context_condition": gaussian(keys[3], (D,), 1.0, 6.0, ((0, 16),)),
        "shift_weight": gaussian(keys[4], (D, D), (D // 2) ** -0.5, 0.125, ((0, 16), (1, 8))),
        "scale_weight": gaussian(keys[5], (D, D), (D // 2) ** -0.5, 0.125, ((0, 16), (1, 8))),
        "gate_weight": gaussian(keys[6], (D, D), (D // 8) ** -0.5, 0.25, ((0, 16), (1, 8))),
        "norm_gain": jnp.clip(1.0 + 0.18 * jax.random.normal(keys[7], (D,), jnp.float32), 0.1, 1.9),
        "query_weight": gaussian(keys[8], (D, HEADS * HEAD_DIM), D ** -0.5, 0.09375, ((1, 8),)),
        "key_weight": gaussian(keys[9], (D, HEADS * HEAD_DIM), D ** -0.5, 0.09375, ((1, 8),)),
        "value_weight": gaussian(keys[10], (D, HEADS * HEAD_DIM), D ** -0.5, 0.09375, ((1, 8),)),
        "write_weight": gaussian(keys[11], (D, 2, HEADS), D ** -0.5, 0.09375),
        "decay_weight": gaussian(keys[12], (D, 2, HEADS), D ** -0.5, 0.09375),
        "write_bias": draw_write_bias(jax.random.fold_in(keys[18], 71), 0),
        "decay_bias": draw_decay_bias(jax.random.fold_in(keys[18], 71), 0),
        "log_rate": jnp.clip(jax.random.uniform(keys[15], (2, HEADS), jnp.float32, 0.0, 1.4), 0.0, 1.4),
        "head_gain": jnp.clip(1.0 + 0.18 * jax.random.normal(keys[16], (HEAD_DIM,), jnp.float32), 0.1, 1.9),
        "out_weight": gaussian(keys[17], (HEADS * HEAD_DIM, D), (HEADS * HEAD_DIM) ** -0.5, 0.125, ((1, 8),)),
    }


epsilon = 0.0001
highest = lax.Precision.HIGHEST

def rms_rows(row_data, row_gain):
    values = row_data.astype(jnp.float32)
    scaled = values * lax.rsqrt(lax.optimization_barrier(jnp.mean(values * values, axis=-1, keepdims=True)) + epsilon)
    return scaled * row_gain.astype(jnp.float32)

def unit_heads(matrix, head_count):
    split_heads = matrix.astype(jnp.float32).reshape(matrix.shape[0], head_count, -1)
    return split_heads * lax.rsqrt(lax.optimization_barrier(jnp.sum(split_heads * split_heads, axis=-1, keepdims=True)) + epsilon)

def head_gates(write_pre, decay_pre, write_bias, decay_bias, log_rate):
    write_rate = jax.nn.sigmoid(write_pre.astype(jnp.float32) + write_bias)
    log_decay = -jnp.exp(log_rate) * jax.nn.softplus(decay_pre.astype(jnp.float32) + decay_bias)
    return (write_rate, log_decay)

def project(matrix, weight):
    return jnp.dot(matrix.astype(jnp.float32), weight.astype(jnp.float32), preferred_element_type=jnp.float32).astype(jnp.bfloat16)

def to_blocks(source):
    heads_first = jnp.moveaxis(source, 1, 0)
    block_count = heads_first.shape[1] // BLOCK
    return heads_first.reshape((heads_first.shape[0], block_count, BLOCK) + heads_first.shape[2:])

def prepare_keys(key_vecs, value_vecs, log_decay, write_rate):
    block_keys = to_blocks(key_vecs)
    block_values = to_blocks(value_vecs)
    running = jnp.cumsum(to_blocks(log_decay), axis=-1)
    block_rates = to_blocks(write_rate)
    offsets = jnp.arange(BLOCK)
    lower_mask = offsets[:, None] >= offsets[None, :]
    strict_mask = offsets[:, None] > offsets[None, :]
    spread = running[..., :, None] - running[..., None, :]
    decay_mat = jnp.where(lower_mask, jnp.exp(jnp.where(lower_mask, spread, 0.0)), 0.0)
    scaled = block_keys * block_rates[..., None]
    system = jnp.einsum('hnid,hnjd->hnij', scaled, block_keys, precision=highest) * decay_mat
    system = jnp.where(strict_mask, system, 0.0) + jnp.eye(BLOCK, dtype=system.dtype)
    fresh_values = jax.scipy.linalg.solve_triangular(system, block_values * block_rates[..., None], lower=True, unit_diagonal=True)
    key_weights = jax.scipy.linalg.solve_triangular(system, scaled * jnp.exp(running)[..., None], lower=True, unit_diagonal=True)
    last_gate = running[..., -1]
    late_keys = block_keys * jnp.exp(last_gate[..., None] - running)[..., None]
    return (block_keys, running, decay_mat, fresh_values, key_weights, last_gate, late_keys)

def prepare_queries(query_vecs, prepared):
    block_queries = to_blocks(query_vecs)
    query_keys = jnp.einsum('hnid,hnjd->hnij', block_queries, prepared[0], precision=highest) * prepared[2]
    early_queries = block_queries * jnp.exp(prepared[1])[..., None]
    return (query_keys, early_queries)

def run_blocks(prepared, queried, start):
    inputs = tuple((jnp.moveaxis(item, 1, 0) for item in (prepared[3], prepared[4], queried[0], queried[1], prepared[6], prepared[5])))

    def advance(carried, pieces):
        new_in, key_in, score_in, query_in, late_in, gate_in = pieces
        corrected = new_in - jnp.einsum('hcd,hde->hce', key_in, carried, precision=highest)
        output = jnp.einsum('hcd,hde->hce', query_in, carried, precision=highest)
        output = output + jnp.einsum('hij,hje->hie', score_in, corrected, precision=highest)
        carried = carried * jnp.exp(gate_in)[:, None, None] + jnp.einsum('hcd,hce->hde', late_in, corrected, precision=highest)
        return (carried, output)
    closing, outputs = lax.scan(advance, start, inputs)
    merged = jnp.transpose(outputs, (0, 2, 1, 3))
    return merged.reshape(-1, merged.shape[2], merged.shape[3])

def final_state(prepared, start):
    inputs = tuple((jnp.moveaxis(item, 1, 0) for item in (prepared[3], prepared[4], prepared[6], prepared[5])))

    def advance(carried, pieces):
        new_in, key_in, late_in, gate_in = pieces
        corrected = new_in - jnp.einsum('hcd,hde->hce', key_in, carried, precision=highest)
        carried = carried * jnp.exp(gate_in)[:, None, None] + jnp.einsum('hcd,hce->hde', late_in, corrected, precision=highest)
        return (carried, None)
    closing, unused = lax.scan(advance, start, inputs)
    return closing

def reference(latent, context, condition, context_condition, shift_weight, scale_weight, gate_weight, norm_gain, query_weight, key_weight, value_weight, write_weight, decay_weight, write_bias, decay_bias, log_rate, head_gain, out_weight):
    head_count = write_bias.shape[1]
    width = write_weight.shape[0]
    stacked = jnp.stack([condition, context_condition]).astype(jnp.float32)
    silu_rows = jax.nn.silu(stacked).astype(jnp.bfloat16)
    shift_rows = jnp.dot(silu_rows.astype(jnp.float32), shift_weight.astype(jnp.float32), preferred_element_type=jnp.float32)
    scale_rows = jnp.dot(silu_rows.astype(jnp.float32), scale_weight.astype(jnp.float32), preferred_element_type=jnp.float32)
    gate_row = jnp.dot(silu_rows[0].astype(jnp.float32), gate_weight.astype(jnp.float32), preferred_element_type=jnp.float32)
    modulated = (rms_rows(latent, norm_gain) * (1.0 + scale_rows[0]) + shift_rows[0]).astype(jnp.bfloat16)
    ctx_modulated = (rms_rows(context, norm_gain) * (1.0 + scale_rows[1]) + shift_rows[1]).astype(jnp.bfloat16)
    write_flat = write_weight.reshape(width, -1)
    decay_flat = decay_weight.reshape(width, -1)
    ctx_keys = unit_heads(project(ctx_modulated, key_weight), head_count)
    ctx_values = project(ctx_modulated, value_weight).astype(jnp.float32).reshape(-1, head_count, HEAD_DIM)
    ctx_rate, ctx_log = head_gates(project(ctx_modulated, write_flat).reshape(-1, 2, head_count), project(ctx_modulated, decay_flat).reshape(-1, 2, head_count), write_bias, decay_bias, log_rate)
    start_zero = jnp.zeros((head_count, HEAD_DIM, HEAD_DIM), jnp.float32)
    ctx_forward = final_state(prepare_keys(ctx_keys, ctx_values, ctx_log[:, 0], ctx_rate[:, 0]), start_zero)
    ctx_backward = final_state(prepare_keys(jnp.flip(ctx_keys, 0), jnp.flip(ctx_values, 0), jnp.flip(ctx_log[:, 1], 0), jnp.flip(ctx_rate[:, 1], 0)), start_zero)
    queries = unit_heads(project(modulated, query_weight), head_count) * HEAD_DIM ** (-0.5)
    key_vecs = unit_heads(project(modulated, key_weight), head_count)
    value_vecs = project(modulated, value_weight).astype(jnp.float32).reshape(-1, head_count, HEAD_DIM)
    write_rate, log_decay = head_gates(project(modulated, write_flat).reshape(-1, 2, head_count), project(modulated, decay_flat).reshape(-1, 2, head_count), write_bias, decay_bias, log_rate)
    forward_prep = prepare_keys(key_vecs, value_vecs, log_decay[:, 0], write_rate[:, 0])
    forward_out = run_blocks(forward_prep, prepare_queries(queries, forward_prep), ctx_forward)
    backward_prep = prepare_keys(jnp.flip(key_vecs, 0), jnp.flip(value_vecs, 0), jnp.flip(log_decay[:, 1], 0), jnp.flip(write_rate[:, 1], 0))
    backward_out = jnp.flip(run_blocks(backward_prep, prepare_queries(jnp.flip(queries, 0), backward_prep), ctx_backward), 0)
    combined = forward_out + backward_out
    head_out = combined * lax.rsqrt(lax.optimization_barrier(jnp.mean(combined * combined, axis=-1, keepdims=True)) + epsilon) * head_gain.astype(jnp.float32)
    head_out = head_out.astype(jnp.bfloat16).reshape(combined.shape[0], -1)
    branch = jnp.dot(head_out.astype(jnp.float32), out_weight.astype(jnp.float32), preferred_element_type=jnp.float32)
    return (latent.astype(jnp.float32) + gate_row * branch).astype(jnp.bfloat16)
```

```python
import jax
import jax.numpy as jnp
from jax import lax
from jax.experimental import pallas as pl
from jax.experimental.pallas import tpu as pltpu
from jax.sharding import Mesh
from jax.sharding import PartitionSpec as P

HEAD_DIM = 128
SP = ("sp_0", "sp_1")
EPS = 0.0001
F32 = jnp.float32
BF16 = jnp.bfloat16
TILE = 128
LEVELS = (1, 2, 3, 4, 5, 6)


def mm(a, b):
    return jnp.dot(a.astype(BF16), b.astype(BF16), preferred_element_type=F32)


def mm_nt(a, b):
    return lax.dot_general(a, b, (((1,), (1,)), ((), ())), preferred_element_type=F32)


def mm_tn(a, b):
    return lax.dot_general(a, b, (((0,), (0,)), ((), ())), preferred_element_type=F32)


def iota2(shape, dim):
    return lax.broadcasted_iota(jnp.int32, shape, dim)


def softplus(u):
    return jnp.maximum(u, 0.0) + jnp.log1p(jnp.exp(-jnp.abs(u)))


def inv_norm(rows_bf16):
    r = rows_bf16.astype(F32)
    return lax.rsqrt(jnp.sum(r * r, axis=-1, keepdims=True) + EPS)


def modulate_rows(lat_ref, ctx_ref, gain_ref, rows_ref, ab_ref, mod_ref):
    for s in range(2):
        ab_ref[2 * s] = gain_ref[...] * (1.0 + rows_ref[2 + s : 3 + s, :])
        ab_ref[2 * s + 1] = rows_ref[s : s + 1, :]
    n_lat = lat_ref.shape[0] // 16
    n_ctx = ctx_ref.shape[0] // 16

    def one(src_ref, base, s):
        def step(i, carry):
            x = src_ref[pl.ds(i * 16, 16), :].astype(F32)
            inv = lax.rsqrt(jnp.mean(x * x, axis=-1, keepdims=True) + EPS)
            y = x * inv * ab_ref[2 * s] + ab_ref[2 * s + 1]
            mod_ref[pl.ds(base + i * 16, 16), :] = y.astype(BF16)
            return carry

        return step

    lax.fori_loop(0, n_lat, one(lat_ref, 0, 0), 0)
    lax.fori_loop(0, n_ctx, one(ctx_ref, lat_ref.shape[0], 1), 0)


def gate_rows(first_head, pre_ref, wb_ref, db_ref, lr_ref, rows_ref, n_lat, n_ctx):
    width = n_lat + TILE
    lane = iota2((8, width), 1)
    is_ctx = lane >= n_lat
    pos = jnp.where(is_ctx, lane - n_lat, lane)
    size = jnp.where(is_ctx, n_ctx, n_lat)
    valid = pos < size
    row = iota2((8, width), 0)
    rates = jnp.zeros((8, width), F32)
    logd = jnp.zeros((8, width), F32)
    for c in range(4):
        d, h = c // 2, c % 2
        head = first_head + h
        at = d * 16 + head
        w = pre_ref[pl.ds(at, 1), :] + wb_ref[d, head]
        u = pre_ref[pl.ds(32 + at, 1), :] + db_ref[d, head]
        rate = 1.0 / (1.0 + jnp.exp(-w))
        step = -jnp.exp(jnp.full((1, width), lr_ref[d, head], F32)) * softplus(u)
        rates = jnp.where(row == c, rate, rates)
        logd = jnp.where(row == c, step, logd)
    rates = jnp.where(valid, rates, 0.0)
    logd = jnp.where(valid, logd, 0.0)
    fwd = logd
    bwd = logd
    s = 1
    while s < n_lat:
        fwd = fwd + jnp.where(pos >= s, pltpu.roll(fwd, s, 1), 0.0)
        bwd = bwd + jnp.where(pos + s < size, pltpu.roll(bwd, width - s, 1), 0.0)
        s *= 2
    g = jnp.where(row < 2, fwd, bwd)
    g = jnp.where(valid, g, 0.0)
    whole_lat = jnp.sum(jnp.where(is_ctx, 0.0, logd), axis=1, keepdims=True)
    whole_ctx = jnp.sum(jnp.where(is_ctx, logd, 0.0), axis=1, keepdims=True)
    late = jnp.exp(jnp.where(is_ctx, whole_ctx, whole_lat) - g)
    eg = jnp.exp(g)
    parts = []
    for a in (rates, g, late, eg):
        up = pltpu.roll(pltpu.roll(a, n_ctx, 1), 6, 0)
        a = jnp.where(lane >= n_lat + n_ctx, up, a)
        parts.append(a)
    rows_ref[...] = jnp.zeros_like(rows_ref)
    for n, a in enumerate(parts):
        rows_ref[8 * n : 8 * n + 8, :] = a
    return jnp.exp(whole_lat), jnp.exp(whole_ctx)


def tile_inverse(a_ref, t_ref, index, ones_diag, xor):
    a = a_ref[index].astype(F32)
    t = ones_diag - jnp.where(xor == 1, a, 0.0)
    return a, t


def recurrence(first_head, q_ref, k_ref, v_ref, pre_ref, wb_ref, db_ref, lr_ref, scratch, outs, n_lat, n_ctx):
    rows_ref, cols_ref, gk_ref, qk_ref, ad_ref, t_ref, ao_ref, p_ref, x_ref, xl_ref = scratch
    o1_ref, q2_ref, lat_map_ref, ctx_map_ref = outs
    blocks = n_lat // TILE
    width = n_lat + TILE
    dec_lat, dec_ctx = gate_rows(first_head, pre_ref, wb_ref, db_ref, lr_ref, rows_ref, n_lat, n_ctx)
    for b in range(blocks + 1):
        cols_ref[b * TILE : (b + 1) * TILE, :] = jnp.transpose(rows_ref[:, b * TILE : (b + 1) * TILE])
    RATE, G, LATE, EG = 0, 8, 16, 24

    def kcols(h):
        return k_ref[0:n_lat, h * TILE : (h + 1) * TILE]

    def kctx(h):
        kc = k_ref[n_lat : n_lat + n_ctx, h * TILE : (h + 1) * TILE]
        return jnp.concatenate([kc, kc], axis=0)

    def vctx(h):
        vc = v_ref[n_lat : n_lat + n_ctx, h * TILE : (h + 1) * TILE]
        return jnp.concatenate([vc, vc], axis=0)

    kinv = []
    for h in range(2):
        kinv.append(jnp.concatenate([inv_norm(kcols(h)), inv_norm(kctx(h))], axis=0))
    lane128 = iota2((width, TILE), 1)
    both = jnp.where(lane128 == 0, kinv[0], jnp.where(lane128 == 1, kinv[1], 0.0))
    for b in range(blocks + 1):
        rows_ref[:, b * TILE : (b + 1) * TILE] = jnp.where(
            (iota2((TILE, TILE), 0) < 32),
            rows_ref[:, b * TILE : (b + 1) * TILE],
            pltpu.roll(jnp.transpose(both[b * TILE : (b + 1) * TILE, :]), 32, 0),
        )
    KINV = 32
    ii = iota2((TILE, TILE), 0)
    jj = iota2((TILE, TILE), 1)
    xor = ii ^ jj
    qinvs = []
    for h in range(2):
        qh = q_ref[0:n_lat, h * TILE : (h + 1) * TILE]
        qinv = inv_norm(qh) * (HEAD_DIM**-0.5)
        qinvs.append(qinv)
        krow = rows_ref[KINV + h : KINV + h + 1, 0:n_lat]
        gk_ref[h] = mm_nt(kcols(h), kcols(h)) * kinv[h][0:n_lat] * krow
        qk_ref[h] = mm_nt(qh, kcols(h)) * qinv * krow

    def spread(c, i, j):
        gi = cols_ref[i * TILE : (i + 1) * TILE, G + c : G + c + 1]
        gj = rows_ref[G + c : G + c + 1, j * TILE : (j + 1) * TILE]
        return gi - gj

    for c in range(4):
        d, h = c // 2, c % 2
        for i in range(blocks):
            ri = cols_ref[i * TILE : (i + 1) * TILE, RATE + c : RATE + c + 1]
            for j in range(blocks):
                if (d == 0 and j > i) or (d == 1 and j < i):
                    continue
                at = (slice(i * TILE, (i + 1) * TILE), slice(j * TILE, (j + 1) * TILE))
                sp = spread(c, i, j)
                if i == j:
                    keep = (ii >= jj) if d == 0 else (ii <= jj)
                    dm = jnp.where(keep, jnp.exp(jnp.where(keep, sp, 0.0)), 0.0)
                else:
                    dm = jnp.exp(sp)
                a = gk_ref[(h, *at)] * dm * ri
                if i == j:
                    ad_ref[c * blocks + i] = jnp.where(ii == jj, 0.0, a).astype(BF16)
                else:
                    ao_ref[(c, *at)] = a.astype(BF16)
                p_ref[(c, *at)] = (qk_ref[(h, *at)] * dm).astype(BF16)
    for h in range(2):
        kc = kctx(h)
        g2 = mm_nt(kc, kc) * kinv[h][n_lat:] * rows_ref[KINV + h : KINV + h + 1, n_lat:]
        keep = jnp.where(
            ii < n_ctx, jnp.where(jj < ii, 1, 0), jnp.where(jj > ii, 1, 0)
        )
        keep = jnp.where((ii < n_ctx) == (jj < n_ctx), keep, 0) == 1
        sp = (
            cols_ref[n_lat:, G + h : G + h + 1]
            - rows_ref[G + h : G + h + 1, n_lat:]
        )
        dm = jnp.where(keep, jnp.exp(jnp.where(keep, sp, 0.0)), 0.0)
        ad_ref[4 * blocks + h] = (g2 * dm * cols_ref[n_lat:, RATE + h : RATE + h + 1]).astype(BF16)

    tiles = 4 * blocks + 2
    group = tiles // 2

    def invert(part, carry):
        base = part * group
        eye = jnp.where(xor == 0, 1.0, 0.0)
        ts = []
        for n in range(group):
            a = ad_ref[base + n].astype(F32)
            ts.append((eye - jnp.where(xor == 1, a, 0.0)).astype(BF16))
        for level in LEVELS:
            xs = []
            for n in range(group):
                off = jnp.where((xor >> level) == 1, ad_ref[base + n].astype(F32), 0.0).astype(BF16)
                xs.append(mm(ts[n], off).astype(BF16))
            ts = [(t.astype(F32) - mm(x, t)).astype(BF16) for x, t in zip(xs, ts)]
        for n in range(group):
            t_ref[base + n] = ts[n]
        return carry

    lax.fori_loop(0, 2, invert, 0)

    for c in range(4):
        d, h = c // 2, c % 2
        order = list(range(blocks)) if d == 0 else list(reversed(range(blocks)))
        for n, i in enumerate(order):
            r = slice(i * TILE, (i + 1) * TILE)
            rate = cols_ref[r, RATE + c : RATE + c + 1]
            eg = cols_ref[r, EG + c : EG + c + 1]
            late = cols_ref[r, LATE + c : LATE + c + 1]
            ki = kinv[h][r]
            vi = v_ref[r, h * TILE : (h + 1) * TILE].astype(F32) * rate
            wi = k_ref[r, h * TILE : (h + 1) * TILE].astype(F32) * (rate * eg * ki)
            b = jnp.concatenate([vi, wi], axis=1)
            if n > 0:
                done = slice(0, i * TILE) if d == 0 else slice((i + 1) * TILE, n_lat)
                b = b - mm(ao_ref[c, r, done], x_ref[c, done, :])
            x = mm(t_ref[c * blocks + i], b)
            x_ref[c, r, :] = x.astype(BF16)
            xl_ref[c, r, :] = (x * (late * ki)).astype(BF16)
    for h in range(2):
        o1 = []
        for d in range(2):
            c = d * 2 + h
            for i in range(blocks):
                r = slice(i * TILE, (i + 1) * TILE)
                seen = slice(0, (i + 1) * TILE) if d == 0 else slice(i * TILE, n_lat)
                ow = mm(p_ref[c, r, seen], x_ref[c, seen, :])
                qi = q_ref[r, h * TILE : (h + 1) * TILE].astype(F32)
                early = qi * (cols_ref[r, EG + c : EG + c + 1] * qinvs[h][r])
                q2_ref[h, r, d * TILE : (d + 1) * TILE] = (early - ow[:, TILE:]).astype(BF16)
                if d == 0:
                    o1.append(ow[:, :TILE])
                else:
                    o1_ref[h, r, :] = o1[i] + ow[:, :TILE]
            m = mm_tn(kcols(h), xl_ref[c])
            diag = jnp.where(xor == 0, dec_lat[c : c + 1, :], 0.0)
            lat_map_ref[c] = jnp.concatenate([diag - m[:, TILE:], m[:, :TILE]], axis=1).astype(BF16)
    for h in range(2):
        ci = kinv[h][n_lat:]
        cr = slice(n_lat, n_lat + TILE)
        rate = cols_ref[cr, RATE + h : RATE + h + 1]
        eg = cols_ref[cr, EG + h : EG + h + 1]
        late = cols_ref[cr, LATE + h : LATE + h + 1]
        kc = kctx(h)
        b = jnp.concatenate([vctx(h).astype(F32) * rate, kc.astype(F32) * (rate * eg * ci)], axis=1)
        x = mm(t_ref[4 * blocks + h], b)
        xl = (x * (late * ci)).astype(BF16)
        for d in range(2):
            c = d * 2 + h
            m = mm_tn(kc[0:n_ctx], xl[d * n_ctx : (d + 1) * n_ctx])
            diag = jnp.where(xor == 0, dec_ctx[c : c + 1, :], 0.0)
            ctx_map_ref[c] = jnp.concatenate([diag - m[:, TILE:], m[:, :TILE]], axis=1).astype(BF16)


def make_local_kernel(first_head_of):
    def kernel(
        lat_ref, ctx_ref, rows_in, gain_ref, wq_hbm, wk_hbm, wv_hbm, ww_ref, wd_ref, wb_ref, db_ref, lr_ref,
        o1_ref, q2_ref, lat_map_ref, ctx_map_ref,
        w_ref, sem, ab_ref, mod_ref, q_ref, k_ref, v_ref, pre_ref, *scratch,
    ):
        n_lat, n_ctx = lat_ref.shape[0], ctx_ref.shape[0]
        copies = [
            pltpu.make_async_copy(src, w_ref.at[n], sem.at[n])
            for n, src in enumerate((wk_hbm, wv_hbm, wq_hbm))
        ]
        for copy in copies:
            copy.start()
        modulate_rows(lat_ref, ctx_ref, gain_ref, rows_in, ab_ref, mod_ref)
        pre_ref[...] = jnp.zeros_like(pre_ref)
        for n, w in enumerate((ww_ref, wd_ref)):
            r = slice(32 * n, 32 * n + 32)
            pre_ref[r, 0:n_lat] = mm_nt(w[...], mod_ref[0:n_lat, :]).astype(BF16).astype(F32)
            pre_ref[r, n_lat : n_lat + n_ctx] = mm_nt(w[...], mod_ref[n_lat:, :]).astype(BF16).astype(F32)
        copies[0].wait()
        k_ref[...] = mm(mod_ref[...], w_ref[0]).astype(BF16)
        copies[1].wait()
        v_ref[...] = mm(mod_ref[...], w_ref[1]).astype(BF16)
        copies[2].wait()
        q_ref[...] = mm(mod_ref[0:n_lat, :], w_ref[2]).astype(BF16)
        recurrence(
            first_head_of(), q_ref, k_ref, v_ref, pre_ref, wb_ref, db_ref, lr_ref, scratch,
            (o1_ref, q2_ref, lat_map_ref, ctx_map_ref), n_lat, n_ctx,
        )

    return kernel


def local_scratch(n_lat, n_ctx, width):
    blocks = n_lat // TILE
    tiles = 4 * blocks + 2
    return [
        pltpu.VMEM((3, width, 2 * TILE), BF16),
        pltpu.SemaphoreType.DMA((3,)),
        pltpu.VMEM((4, 1, width), F32),
        pltpu.VMEM((n_lat + n_ctx, width), BF16),
        pltpu.VMEM((n_lat, 2 * TILE), BF16),
        pltpu.VMEM((n_lat + n_ctx, 2 * TILE), BF16),
        pltpu.VMEM((n_lat + n_ctx, 2 * TILE), BF16),
        pltpu.VMEM((64, n_lat + TILE), F32),
        pltpu.VMEM((TILE, n_lat + TILE), F32),
        pltpu.VMEM((n_lat + TILE, TILE), F32),
        pltpu.VMEM((2, n_lat, n_lat), F32),
        pltpu.VMEM((2, n_lat, n_lat), F32),
        pltpu.VMEM((tiles, TILE, TILE), BF16),
        pltpu.VMEM((tiles, TILE, TILE), BF16),
        pltpu.VMEM((4, n_lat, n_lat), BF16),
        pltpu.VMEM((4, n_lat, n_lat), BF16),
        pltpu.VMEM((4, n_lat, 2 * TILE), BF16),
        pltpu.VMEM((4, n_lat, 2 * TILE), BF16),
    ]


def local_call(first_head_of, args):
    latent, context = args[0], args[1]
    n_lat, width = latent.shape
    n_ctx = context.shape[0]
    vm = pl.BlockSpec(memory_space=pltpu.VMEM)
    sm = pl.BlockSpec(memory_space=pltpu.SMEM)
    hb = pl.BlockSpec(memory_space=pl.ANY)
    return pl.pallas_call(
        make_local_kernel(first_head_of),
        out_shape=(
            jax.ShapeDtypeStruct((2, n_lat, TILE), F32),
            jax.ShapeDtypeStruct((2, n_lat, 2 * TILE), BF16),
            jax.ShapeDtypeStruct((4, TILE, 2 * TILE), BF16),
            jax.ShapeDtypeStruct((4, TILE, 2 * TILE), BF16),
        ),
        in_specs=[vm, vm, vm, vm, hb, hb, hb, vm, vm, sm, sm, sm],
        out_specs=(vm, vm, vm, vm),
        scratch_shapes=local_scratch(n_lat, n_ctx, width),
        compiler_params=pltpu.CompilerParams(vmem_limit_bytes=60 * 1024 * 1024),
        name="local_tokens",
    )(*args)


def split_rows(x):
    hi = x.astype(BF16)
    lo = (x - hi.astype(F32)).astype(BF16)
    return hi, lo


def mul_precise(m_bf16, x):
    hi, lo = split_rows(x)
    n = x.shape[1]
    y = jnp.dot(m_bf16, jnp.concatenate([hi, lo], axis=1), preferred_element_type=F32)
    return y[:, :n] + y[:, n:]


def then(next_map, total):
    y = mul_precise(next_map[:, :TILE], total)
    zero = jnp.zeros((TILE, TILE), F32)
    return y + jnp.concatenate([zero, next_map[:, TILE:].astype(F32)], axis=1)


def row_scan_kernel(x_of):
    def kernel(maps_ref, prefix_ref, total_ref):
        backwards = x_of() >= 2
        peers = maps_ref.shape[0]
        for part in range(2):
            total = None
            for n in range(peers):
                at = jnp.where(backwards, peers - 1 - n, n)
                one = maps_ref[at, part]
                if part == 1:
                    if n == 0:
                        eye = jnp.where(iota2((TILE, 2 * TILE), 0) == iota2((TILE, 2 * TILE), 1), 1.0, 0.0)
                        prefix_ref[at] = eye
                    else:
                        prefix_ref[at] = total
                total = one.astype(F32) if n == 0 else then(one, total)
            total_ref[part] = total.astype(BF16)

    return kernel


def column_scan_kernel(x_of, z_of):
    def kernel(totals_ref, prefix_ref, start_ref):
        backwards = x_of() >= 2
        groups = totals_ref.shape[0]
        state = None
        for n in range(groups):
            at = jnp.where(backwards, groups - 1 - n, n)
            one = totals_ref[at, 0]
            off = one[:, TILE:].astype(F32)
            state = off if n == 0 else mul_precise(one[:, :TILE], state) + off
        z = z_of()
        place = jnp.where(backwards, groups - 1 - z, z)
        for n in range(groups - 1):
            at = jnp.where(backwards, groups - 1 - n, n)
            one = totals_ref[at, 1]
            new = mul_precise(one[:, :TILE], state) + one[:, TILE:].astype(F32)
            state = jnp.where(n < place, new, state)
        for k in range(prefix_ref.shape[0]):
            mk = prefix_ref[k]
            hi, lo = split_rows(mk[:, :TILE])
            s = mul_precise(hi, state) + mm(lo, state) + mk[:, TILE:]
            start_ref[k] = s.astype(BF16)

    return kernel


def apply_kernel(o1_ref, q2_ref, s_ref, gain_ref, out_ref):
    for h in range(2):
        both = jnp.concatenate([s_ref[h], s_ref[2 + h]], axis=0)
        y = o1_ref[h] + jnp.dot(q2_ref[h], both, preferred_element_type=F32)
        y = y * lax.rsqrt(jnp.mean(y * y, axis=-1, keepdims=True) + EPS) * gain_ref[...]
        out_ref[:, h * TILE : (h + 1) * TILE] = y.astype(BF16)


def body(
    latent, context, condition, context_condition, shift_weight, scale_weight, gate_weight, norm_gain,
    query_weight, key_weight, value_weight, write_weight, decay_weight, write_bias, decay_bias, log_rate,
    head_gain, out_weight,
):
    own_cols = gate_weight.shape[1]
    col_start = lax.axis_index("tp") * own_cols
    stacked = jnp.stack([condition, context_condition]).astype(F32)
    silu_rows = jax.nn.silu(stacked).astype(BF16)
    part = jnp.concatenate(
        [
            jnp.dot(silu_rows, shift_weight, preferred_element_type=F32),
            jnp.dot(silu_rows, scale_weight, preferred_element_type=F32),
            jnp.dot(silu_rows[:1], gate_weight, preferred_element_type=F32),
        ],
        axis=0,
    )
    copies = jnp.broadcast_to(part, (16, *part.shape))
    summed = jnp.sum(lax.all_to_all(copies, SP, split_axis=0, concat_axis=0, tiled=True), axis=0)
    gate_row = summed[4:5]
    mod_rows = lax.all_gather(summed[:4], "tp", axis=1, tiled=True)
    gates = [jnp.transpose(w, (1, 2, 0)).reshape(32, -1) for w in (write_weight, decay_weight)]
    o1, q2, lat_map, ctx_map = local_call(
        lambda: lax.axis_index("tp") * 2,
        (
            latent, context, mod_rows, norm_gain.reshape(1, -1), query_weight, key_weight, value_weight,
            *gates, write_bias, decay_bias, log_rate,
        ),
    )
    vm = pl.BlockSpec(memory_space=pltpu.VMEM)
    maps = lax.all_to_all(
        jnp.stack([ctx_map, lat_map], axis=1), "sp_1", split_axis=0, concat_axis=0, tiled=True
    )
    prefix, totals = pl.pallas_call(
        row_scan_kernel(lambda: lax.axis_index("sp_1")),
        out_shape=(
            jax.ShapeDtypeStruct((4, TILE, 2 * TILE), F32),
            jax.ShapeDtypeStruct((2, TILE, 2 * TILE), BF16),
        ),
        in_specs=[vm], out_specs=(vm, vm), name="row_scan",
    )(maps)
    all_totals = lax.all_gather(totals, "sp_0", axis=0)
    starts = pl.pallas_call(
        column_scan_kernel(lambda: lax.axis_index("sp_1"), lambda: lax.axis_index("sp_0")),
        out_shape=jax.ShapeDtypeStruct((4, TILE, TILE), BF16),
        in_specs=[vm, vm], out_specs=vm, name="column_scan",
    )(all_totals, prefix)
    mine = lax.all_to_all(starts, "sp_1", split_axis=0, concat_axis=0, tiled=True)
    head_out = pl.pallas_call(
        apply_kernel,
        out_shape=jax.ShapeDtypeStruct((latent.shape[0], 2 * TILE), BF16),
        in_specs=[vm] * 4, out_specs=vm, name="apply_start",
    )(o1, q2, mine, head_gain.reshape(1, -1))
    branch = jnp.dot(
        lax.all_gather(head_out, "tp", axis=1, tiled=True), out_weight, preferred_element_type=F32
    )
    residual = lax.dynamic_slice_in_dim(latent, col_start, own_cols, 1).astype(F32)
    return (residual + gate_row * branch).astype(BF16)


def solution(mesh):
    torus = Mesh(mesh.devices.reshape(4, 4, mesh.shape["tp"]), ("sp_0", "sp_1", "tp"))
    placed = (
        P(SP, None), P(SP, None), P(SP), P(SP), P(SP, "tp"), P(SP, "tp"), P(SP, "tp"), P(),
        P(None, "tp"), P(None, "tp"), P(None, "tp"), P(), P(), P(), P(), P(), P(), P(None, "tp"),
    )
    return jax.shard_map(body, mesh=torus, in_specs=placed, out_specs=P(SP, "tp"), check_vma=False)
```

```python
import jax
import jax.numpy as jnp
from jax import lax
from jax.experimental import pallas as pl
from jax.experimental.pallas import tpu as pltpu
from jax.sharding import Mesh
from jax.sharding import PartitionSpec as P

HEAD_DIM = 128
SP = ("sp_0", "sp_1")
EPS = 0.0001
F32 = jnp.float32
BF16 = jnp.bfloat16
TILE = 128
MESH = pl.DeviceIdType.MESH
LEVELS = (1, 2, 3, 4, 5, 6)


def mm(a, b):
    return jnp.dot(a.astype(BF16), b.astype(BF16), preferred_element_type=F32)


def mm_nt(a, b):
    return lax.dot_general(a, b, (((1,), (1,)), ((), ())), preferred_element_type=F32)


def mm_tn(a, b):
    return lax.dot_general(a, b, (((0,), (0,)), ((), ())), preferred_element_type=F32)


def iota2(shape, dim):
    return lax.broadcasted_iota(jnp.int32, shape, dim)


def softplus(u):
    return jnp.maximum(u, 0.0) + jnp.log1p(jnp.exp(-jnp.abs(u)))


def inv_norm(rows_bf16):
    r = rows_bf16.astype(F32)
    return lax.rsqrt(jnp.sum(r * r, axis=-1, keepdims=True) + EPS)


def gate_rows(first_head, pre_ref, wb_ref, db_ref, lr_ref, rows_ref, n_lat, n_ctx):
    width = n_lat + TILE
    lane = iota2((8, width), 1)
    is_ctx = lane >= n_lat
    pos = jnp.where(is_ctx, lane - n_lat, lane)
    size = jnp.where(is_ctx, n_ctx, n_lat)
    valid = pos < size
    row = iota2((8, width), 0)
    rates = jnp.zeros((8, width), F32)
    logd = jnp.zeros((8, width), F32)
    for c in range(4):
        d, h = c // 2, c % 2
        head = first_head + h
        at = d * 16 + head
        w = pre_ref[pl.ds(at, 1), :] + wb_ref[d, head]
        u = pre_ref[pl.ds(32 + at, 1), :] + db_ref[d, head]
        rate = 1.0 / (1.0 + jnp.exp(-w))
        step = -jnp.exp(jnp.full((1, width), lr_ref[d, head], F32)) * softplus(u)
        rates = jnp.where(row == c, rate, rates)
        logd = jnp.where(row == c, step, logd)
    rates = jnp.where(valid, rates, 0.0)
    logd = jnp.where(valid, logd, 0.0)
    fwd = logd
    bwd = logd
    s = 1
    while s < n_lat:
        fwd = fwd + jnp.where(pos >= s, pltpu.roll(fwd, s, 1), 0.0)
        bwd = bwd + jnp.where(pos + s < size, pltpu.roll(bwd, width - s, 1), 0.0)
        s *= 2
    g = jnp.where(row < 2, fwd, bwd)
    g = jnp.where(valid, g, 0.0)
    whole_lat = jnp.sum(jnp.where(is_ctx, 0.0, logd), axis=1, keepdims=True)
    whole_ctx = jnp.sum(jnp.where(is_ctx, logd, 0.0), axis=1, keepdims=True)
    late = jnp.exp(jnp.where(is_ctx, whole_ctx, whole_lat) - g)
    eg = jnp.exp(g)
    parts = []
    for a in (rates, g, late, eg):
        up = pltpu.roll(pltpu.roll(a, n_ctx, 1), 6, 0)
        a = jnp.where(lane >= n_lat + n_ctx, up, a)
        parts.append(a)
    rows_ref[...] = jnp.zeros_like(rows_ref)
    for n, a in enumerate(parts):
        rows_ref[8 * n : 8 * n + 8, :] = a
    return jnp.exp(whole_lat), jnp.exp(whole_ctx)


def split_rows(x):
    hi = x.astype(BF16)
    lo = (x - hi.astype(F32)).astype(BF16)
    return hi, lo


def mul_precise(m_bf16, x):
    hi, lo = split_rows(x)
    n = x.shape[1]
    y = jnp.dot(m_bf16, jnp.concatenate([hi, lo], axis=1), preferred_element_type=F32)
    return y[:, :n] + y[:, n:]


def then(next_map, total):
    y = mul_precise(next_map[:, :TILE], total)
    zero = jnp.zeros((TILE, TILE), F32)
    return y + jnp.concatenate([zero, next_map[:, TILE:].astype(F32)], axis=1)


RATE, G, LATE, EG, KINV = 0, 8, 16, 24, 32


def remote(src, dst, send_sem, recv_sem, axis, peer):
    return pltpu.make_async_remote_copy(
        src_ref=src, dst_ref=dst, send_sem=send_sem, recv_sem=recv_sem, device_id={axis: peer}, device_id_type=MESH
    )


def greet(barrier, peers):
    for axis, peer in peers:
        pl.semaphore_signal(barrier, inc=1, device_id={axis: peer}, device_id_type=MESH)


def ring_peers(axis, size):
    me = lax.axis_index(axis)
    return [(axis, lax.rem(me + k, size)) for k in range(1, size)]


def project_kernel(
    cond_ref, cctx_ref, shift_ref, scale_ref, gate_ref, gain_ref, ww_ref, wd_ref,
    lat_hbm, ctx_hbm, wq_hbm, wk_hbm, wv_hbm,
    q_ref, k_ref, v_ref, pre_ref, gate_row_ref,
    lat_ref, ctx_ref, w_ref, load_sem, inv_ref, ab_ref, mod_ref,
    part_ref, sum_ref, own_ref, xbuf, zbuf, tbuf, send_sem, recv_sem,
):
    barrier = pltpu.get_barrier_semaphore()
    xs, zs, ts = ring_peers("sp_1", 4), ring_peers("sp_0", 4), ring_peers("tp", 8)
    greet(barrier, xs + zs + ts)
    loads = [
        pltpu.make_async_copy(src, dst, load_sem.at[n])
        for n, (src, dst) in enumerate(
            (
                (lat_hbm, lat_ref), (ctx_hbm, ctx_ref), (wk_hbm, w_ref.at[0]), (wv_hbm, w_ref.at[1]), (wq_hbm, w_ref.at[2]),
            )
        )
    ]
    for load in loads:
        load.start()
    n_lat, n_ctx = lat_ref.shape[0], ctx_ref.shape[0]
    u = jnp.concatenate([cond_ref[...].astype(F32), cctx_ref[...].astype(F32)], axis=0)
    silu = (u / (1.0 + jnp.exp(-u))).astype(BF16)
    part_ref[...] = jnp.zeros_like(part_ref)
    part_ref[0:2, :] = jnp.dot(silu, shift_ref[...], preferred_element_type=F32)
    part_ref[2:4, :] = jnp.dot(silu, scale_ref[...], preferred_element_type=F32)
    part_ref[4:5, :] = jnp.dot(silu, gate_ref[...], preferred_element_type=F32)[0:1]
    pl.semaphore_wait(barrier, len(xs + zs + ts))
    phase_x = [
        remote(part_ref, xbuf.at[n], send_sem.at[n], recv_sem.at[n], *peer) for n, peer in enumerate(xs)
    ]
    for copy in phase_x:
        copy.start()
    loads[0].wait()
    loads[1].wait()

    def norms(src_ref, base):
        def step(i, carry):
            x = src_ref[pl.ds(i * 16, 16), :].astype(F32)
            inv = lax.rsqrt(jnp.mean(x * x, axis=-1, keepdims=True) + EPS)
            inv_ref[pl.ds(base + i * 16, 16), :] = jnp.broadcast_to(inv, (16, TILE))
            return carry

        return step

    lax.fori_loop(0, n_lat // 16, norms(lat_ref, 0), 0)
    lax.fori_loop(0, n_ctx // 16, norms(ctx_ref, n_lat), 0)
    for copy in phase_x:
        copy.wait()
    sum_ref[...] = part_ref[...] + xbuf[0] + xbuf[1] + xbuf[2]
    phase_z = [
        remote(sum_ref, zbuf.at[n], send_sem.at[3 + n], recv_sem.at[3 + n], *peer) for n, peer in enumerate(zs)
    ]
    for copy in phase_z:
        copy.start()
    for copy in phase_z:
        copy.wait()
    whole = sum_ref[...] + zbuf[0] + zbuf[1] + zbuf[2]
    own_ref[...] = whole[0:4]
    gate_row_ref[...] = whole[4:5]
    t = lax.axis_index("tp")
    phase_t = [
        remote(own_ref, tbuf.at[t], send_sem.at[6 + n], recv_sem.at[6 + n], *peer) for n, peer in enumerate(ts)
    ]
    for copy in phase_t:
        copy.start()
    tbuf[t] = own_ref[...]
    pre_ref[...] = jnp.zeros_like(pre_ref)
    for copy in phase_t:
        copy.wait()
    own_cols = own_ref.shape[1]
    for n in range(8):
        cols = slice(n * own_cols, (n + 1) * own_cols)
        for s in range(2):
            ab_ref[2 * s, :, cols] = gain_ref[:, cols] * (1.0 + tbuf[n, 2 + s : 3 + s, :])
            ab_ref[2 * s + 1, :, cols] = tbuf[n, s : s + 1, :]

    def scaled(src_ref, base, s):
        def step(i, carry):
            x = src_ref[pl.ds(i * 16, 16), :].astype(F32)
            inv = inv_ref[pl.ds(base + i * 16, 16), 0:1]
            y = x * inv * ab_ref[2 * s] + ab_ref[2 * s + 1]
            mod_ref[pl.ds(base + i * 16, 16), :] = y.astype(BF16)
            return carry

        return step

    lax.fori_loop(0, n_lat // 16, scaled(lat_ref, 0, 0), 0)
    lax.fori_loop(0, n_ctx // 16, scaled(ctx_ref, n_lat, 1), 0)
    for n, w in enumerate((ww_ref, wd_ref)):
        r = slice(32 * n, 32 * n + 32)
        pre_ref[r, 0:n_lat] = mm_nt(w[...], mod_ref[0:n_lat, :]).astype(BF16).astype(F32)
        pre_ref[r, n_lat : n_lat + n_ctx] = mm_nt(w[...], mod_ref[n_lat:, :]).astype(BF16).astype(F32)
    for load in loads[2:]:
        load.wait()
    k_ref[...] = mm(mod_ref[...], w_ref[0]).astype(BF16)
    v_ref[...] = mm(mod_ref[...], w_ref[1]).astype(BF16)
    q_ref[...] = mm(mod_ref[0:n_lat, :], w_ref[2]).astype(BF16)


def inverses(ad_ref, t_ref, base, count):
    xor = iota2((TILE, TILE), 0) ^ iota2((TILE, TILE), 1)
    eye = jnp.where(xor == 0, 1.0, 0.0)
    ts = []
    for n in range(count):
        a = ad_ref[base + n].astype(F32)
        ts.append((eye - jnp.where(xor == 1, a, 0.0)).astype(BF16))
    for level in LEVELS:
        xs = []
        for n in range(count):
            off = jnp.where((xor >> level) == 1, ad_ref[base + n].astype(F32), 0.0).astype(BF16)
            xs.append(mm(ts[n], off).astype(BF16))
        ts = [(t.astype(F32) - mm(x, t)).astype(BF16) for x, t in zip(xs, ts)]
    for n in range(count):
        t_ref[base + n] = ts[n]


def token_kernel(
    q_ref, k_ref, v_ref, pre_ref, gate_row_ref, gain_ref, wb_ref, db_ref, lr_ref, lat_hbm, ow_hbm,
    out_ref,
    ow_ref, res_ref, load_sem,
    rows_ref, cols_ref, gk_ref, qk_ref, ad_ref, t_ref, ao_ref, p_ref, x_ref, xl_ref, o1_ref, q2_ref,
    lat_map, ctx_map, lat_all, ctx_all, prefix_ref, lat_total, ctx_total, lat_totals, ctx_totals,
    start_ref, mine_ref, ho_ref, send_sem, recv_sem, ho_send, ho_recv,
):
    n_lat = q_ref.shape[0]
    n_ctx = k_ref.shape[0] - n_lat
    blocks = n_lat // TILE
    width = n_lat + TILE
    x_at, z_at, t_at = lax.axis_index("sp_1"), lax.axis_index("sp_0"), lax.axis_index("tp")
    y_at, core = t_at // 2, lax.rem(t_at, 2)
    up = lax.rem(y_at + 1, 4) * 2 + core
    down = lax.rem(y_at + 3, 4) * 2 + core
    across = lax.rem(y_at + 2, 4) * 2 + core
    mate = y_at * 2 + 1 - core
    barrier = pltpu.get_barrier_semaphore()
    xs, zs = ring_peers("sp_1", 4), ring_peers("sp_0", 4)
    greet(barrier, xs + zs + [("tp", up), ("tp", down), ("tp", mate)])
    own_cols = out_ref.shape[1]
    load_w = pltpu.make_async_copy(ow_hbm, ow_ref, load_sem.at[0])
    load_r = pltpu.make_async_copy(
        lat_hbm.at[:, pl.ds(pl.multiple_of(t_at * own_cols, own_cols), own_cols)], res_ref, load_sem.at[1]
    )
    load_w.start()
    load_r.start()

    dec_lat, dec_ctx = gate_rows(t_at * 2, pre_ref, wb_ref, db_ref, lr_ref, rows_ref, n_lat, n_ctx)
    for b in range(blocks + 1):
        cols_ref[b * TILE : (b + 1) * TILE, :] = jnp.transpose(rows_ref[:, b * TILE : (b + 1) * TILE])

    def kcols(h):
        return k_ref[0:n_lat, h * TILE : (h + 1) * TILE]

    def kctx(h):
        kc = k_ref[n_lat : n_lat + n_ctx, h * TILE : (h + 1) * TILE]
        return jnp.concatenate([kc, kc], axis=0)

    def vctx(h):
        vc = v_ref[n_lat : n_lat + n_ctx, h * TILE : (h + 1) * TILE]
        return jnp.concatenate([vc, vc], axis=0)

    kinv = []
    for h in range(2):
        kinv.append(jnp.concatenate([inv_norm(kcols(h)), inv_norm(kctx(h))], axis=0))
    lane128 = iota2((width, TILE), 1)
    both = jnp.where(lane128 == 0, kinv[0], jnp.where(lane128 == 1, kinv[1], 0.0))
    ii = iota2((TILE, TILE), 0)
    jj = iota2((TILE, TILE), 1)
    xor = ii ^ jj
    for b in range(blocks + 1):
        rows_ref[:, b * TILE : (b + 1) * TILE] = jnp.where(
            ii < KINV,
            rows_ref[:, b * TILE : (b + 1) * TILE],
            pltpu.roll(jnp.transpose(both[b * TILE : (b + 1) * TILE, :]), KINV, 0),
        )

    for h in range(2):
        kc = kctx(h)
        g2 = mm_nt(kc, kc) * kinv[h][n_lat:] * rows_ref[KINV + h : KINV + h + 1, n_lat:]
        keep = jnp.where(ii < n_ctx, jnp.where(jj < ii, 1, 0), jnp.where(jj > ii, 1, 0))
        keep = jnp.where((ii < n_ctx) == (jj < n_ctx), keep, 0) == 1
        sp = cols_ref[n_lat:, G + h : G + h + 1] - rows_ref[G + h : G + h + 1, n_lat:]
        dm = jnp.where(keep, jnp.exp(jnp.where(keep, sp, 0.0)), 0.0)
        ad_ref[4 * blocks + h] = (g2 * dm * cols_ref[n_lat:, RATE + h : RATE + h + 1]).astype(BF16)
    inverses(ad_ref, t_ref, 4 * blocks, 2)
    for h in range(2):
        ci = kinv[h][n_lat:]
        cr = slice(n_lat, n_lat + TILE)
        rate = cols_ref[cr, RATE + h : RATE + h + 1]
        eg = cols_ref[cr, EG + h : EG + h + 1]
        late = cols_ref[cr, LATE + h : LATE + h + 1]
        kc = kctx(h)
        b = jnp.concatenate([vctx(h).astype(F32) * rate, kc.astype(F32) * (rate * eg * ci)], axis=1)
        x = mm(t_ref[4 * blocks + h], b)
        xl = (x * (late * ci)).astype(BF16)
        for d in range(2):
            c = d * 2 + h
            m = mm_tn(kc[0:n_ctx], xl[d * n_ctx : (d + 1) * n_ctx])
            diag = jnp.where(xor == 0, dec_ctx[c : c + 1, :], 0.0)
            ctx_map[c] = jnp.concatenate([diag - m[:, TILE:], m[:, :TILE]], axis=1).astype(BF16)

    pl.semaphore_wait(barrier, 9)

    def to_row(base, maps, everyone):
        copies = [
            remote(maps.at[peer], everyone.at[x_at], send_sem.at[base + n], recv_sem.at[base + n], axis, peer)
            for n, (axis, peer) in enumerate(xs)
        ]
        for copy in copies:
            copy.start()
        everyone[x_at] = maps[x_at]
        return copies

    def to_column(base, total, everyone):
        copies = [
            remote(total, everyone.at[z_at], send_sem.at[base + n], recv_sem.at[base + n], axis, peer)
            for n, (axis, peer) in enumerate(zs)
        ]
        for copy in copies:
            copy.start()
        everyone[z_at] = total[...]
        return copies

    ctx_rows = to_row(0, ctx_map, ctx_all)

    qinvs = []
    for h in range(2):
        qh = q_ref[0:n_lat, h * TILE : (h + 1) * TILE]
        qinv = inv_norm(qh) * (HEAD_DIM**-0.5)
        qinvs.append(qinv)
        krow = rows_ref[KINV + h : KINV + h + 1, 0:n_lat]
        gk_ref[h] = mm_nt(kcols(h), kcols(h)) * kinv[h][0:n_lat] * krow
        qk_ref[h] = mm_nt(qh, kcols(h)) * qinv * krow
    for c in range(4):
        d, h = c // 2, c % 2
        for i in range(blocks):
            ri = cols_ref[i * TILE : (i + 1) * TILE, RATE + c : RATE + c + 1]
            gi = cols_ref[i * TILE : (i + 1) * TILE, G + c : G + c + 1]
            for j in range(blocks):
                if (d == 0 and j > i) or (d == 1 and j < i):
                    continue
                at = (slice(i * TILE, (i + 1) * TILE), slice(j * TILE, (j + 1) * TILE))
                sp = gi - rows_ref[G + c : G + c + 1, j * TILE : (j + 1) * TILE]
                if i == j:
                    keep = (ii >= jj) if d == 0 else (ii <= jj)
                    dm = jnp.where(keep, jnp.exp(jnp.where(keep, sp, 0.0)), 0.0)
                else:
                    dm = jnp.exp(sp)
                a = gk_ref[(h, *at)] * dm * ri
                if i == j:
                    ad_ref[c * blocks + i] = jnp.where(ii == jj, 0.0, a).astype(BF16)
                else:
                    ao_ref[(c, *at)] = a.astype(BF16)
                p_ref[(c, *at)] = (qk_ref[(h, *at)] * dm).astype(BF16)

    def invert(part, carry):
        inverses(ad_ref, t_ref, part * 8, 8)
        return carry

    lax.fori_loop(0, 4 * blocks // 8, invert, 0)

    backwards = x_at >= 2

    def place(n, size):
        return jnp.where(backwards, size - 1 - n, n)

    for copy in ctx_rows:
        copy.wait()
    total = ctx_all[place(0, 4)].astype(F32)
    for n in range(1, 4):
        total = then(ctx_all[place(n, 4)], total)
    ctx_total[...] = total.astype(BF16)
    ctx_columns = to_column(3, ctx_total, ctx_totals)

    for c in range(4):
        d, h = c // 2, c % 2
        order = list(range(blocks)) if d == 0 else list(reversed(range(blocks)))
        for n, i in enumerate(order):
            r = slice(i * TILE, (i + 1) * TILE)
            rate = cols_ref[r, RATE + c : RATE + c + 1]
            eg = cols_ref[r, EG + c : EG + c + 1]
            late = cols_ref[r, LATE + c : LATE + c + 1]
            ki = kinv[h][r]
            vi = v_ref[r, h * TILE : (h + 1) * TILE].astype(F32) * rate
            wi = k_ref[r, h * TILE : (h + 1) * TILE].astype(F32) * (rate * eg * ki)
            b = jnp.concatenate([vi, wi], axis=1)
            if n > 0:
                done = slice(0, i * TILE) if d == 0 else slice((i + 1) * TILE, n_lat)
                b = b - mm(ao_ref[c, r, done], x_ref[c, done, :])
            x = mm(t_ref[c * blocks + i], b)
            x_ref[c, r, :] = x.astype(BF16)
            xl_ref[c, r, :] = (x * (late * ki)).astype(BF16)
    for c in range(4):
        m = mm_tn(kcols(c % 2), xl_ref[c])
        diag = jnp.where(xor == 0, dec_lat[c : c + 1, :], 0.0)
        lat_map[c] = jnp.concatenate([diag - m[:, TILE:], m[:, :TILE]], axis=1).astype(BF16)
    lat_rows = to_row(6, lat_map, lat_all)

    for h in range(2):
        o1 = []
        for d in range(2):
            c = d * 2 + h
            for i in range(blocks):
                r = slice(i * TILE, (i + 1) * TILE)
                seen = slice(0, (i + 1) * TILE) if d == 0 else slice(i * TILE, n_lat)
                ow = mm(p_ref[c, r, seen], x_ref[c, seen, :])
                qi = q_ref[r, h * TILE : (h + 1) * TILE].astype(F32)
                early = qi * (cols_ref[r, EG + c : EG + c + 1] * qinvs[h][r])
                q2_ref[h, r, d * TILE : (d + 1) * TILE] = (early - ow[:, TILE:]).astype(BF16)
                if d == 0:
                    o1.append(ow[:, :TILE])
                else:
                    o1_ref[h, r, :] = o1[i] + ow[:, :TILE]

    for copy in ctx_columns:
        copy.wait()
    state = None
    for n in range(4):
        one = ctx_totals[place(n, 4)]
        off = one[:, TILE:].astype(F32)
        state = off if n == 0 else mul_precise(one[:, :TILE], state) + off
    for copy in lat_rows:
        copy.wait()
    total = None
    for n in range(4):
        at = place(n, 4)
        one = lat_all[at]
        if n > 0:
            prefix_ref[at] = total
        total = one.astype(F32) if n == 0 else then(one, total)
    lat_total[...] = total.astype(BF16)
    lat_columns = to_column(9, lat_total, lat_totals)
    for copy in lat_columns:
        copy.wait()
    z_place = place(z_at, 4)
    for n in range(3):
        one = lat_totals[place(n, 4)]
        new = mul_precise(one[:, :TILE], state) + one[:, TILE:].astype(F32)
        state = jnp.where(n < z_place, new, state)
    start_ref[place(0, 4)] = state.astype(BF16)
    for n in range(1, 4):
        at = place(n, 4)
        mk = prefix_ref[at]
        hi, lo = split_rows(mk[:, :TILE])
        start_ref[at] = (mul_precise(hi, state) + mm(lo, state) + mk[:, TILE:]).astype(BF16)
    starts = to_row(12, start_ref, mine_ref)
    for copy in starts:
        copy.wait()

    half = n_lat // 2
    A, B = slice(0, half), slice(half, n_lat)

    def finish(r):
        for h in range(2):
            both_s = jnp.concatenate([mine_ref[h], mine_ref[2 + h]], axis=0)
            y = o1_ref[h, r, :] + jnp.dot(q2_ref[h, r, :], both_s, preferred_element_type=F32)
            y = y * lax.rsqrt(jnp.mean(y * y, axis=-1, keepdims=True) + EPS) * gain_ref[...]
            ho_ref[t_at, r, h * TILE : (h + 1) * TILE] = y.astype(BF16)

    def hand(n, block, r, peer):
        copy = remote(ho_ref.at[block, r], ho_ref.at[block, r], ho_send.at[n], ho_recv.at[n], "tp", peer)
        copy.start()
        return copy

    hands = {}
    finish(A)
    hands[0] = hand(0, t_at, A, up)
    hands[4] = hand(4, t_at, A, mate)
    finish(B)
    hands[3] = hand(3, t_at, B, down)
    hands[1] = hand(1, t_at, B, up)
    hands[2] = hand(2, t_at, A, down)
    hands[5] = hand(5, t_at, B, mate)
    load_w.wait()
    load_r.wait()
    depth = 2 * TILE

    def add(block):
        w = ow_ref[pl.ds(pl.multiple_of(block * depth, depth), depth), :]
        return jnp.dot(ho_ref[block], w, preferred_element_type=F32)

    hands[0].wait_recv()
    hands[6] = hand(6, down, A, up)
    hands[8] = hand(8, down, A, mate)
    hands[3].wait_recv()
    hands[7] = hand(7, up, B, down)
    hands[11] = hand(11, up, B, mate)
    hands[4].wait_recv()
    hands[5].wait_recv()
    acc = add(t_at) + add(mate)
    hands[1].wait_recv()
    hands[9] = hand(9, down, B, mate)
    hands[2].wait_recv()
    hands[10] = hand(10, up, A, mate)
    acc = acc + add(down) + add(up)
    hands[6].wait_recv()
    hands[12] = hand(12, across, A, mate)
    hands[7].wait_recv()
    hands[13] = hand(13, across, B, mate)
    for n in range(8, 12):
        hands[n].wait_recv()

    def other(block):
        return block + 1 - 2 * core

    acc = acc + add(other(down)) + add(other(up)) + add(across)
    hands[12].wait_recv()
    hands[13].wait_recv()
    acc = acc + add(other(across))
    out_ref[...] = (res_ref[...].astype(F32) + gate_row_ref[...] * acc).astype(BF16)
    for n in range(14):
        hands[n].wait_send()


def body(
    latent, context, condition, context_condition, shift_weight, scale_weight, gate_weight, norm_gain,
    query_weight, key_weight, value_weight, write_weight, decay_weight, write_bias, decay_bias, log_rate,
    head_gain, out_weight,
):
    n_lat, d = latent.shape
    n_ctx = context.shape[0]
    n_all = n_lat + n_ctx
    own_cols = gate_weight.shape[1]
    pair = query_weight.shape[1]
    blocks = n_lat // TILE
    tiles = 4 * blocks + 2
    width = n_lat + TILE
    vm = pl.BlockSpec(memory_space=pltpu.VMEM)
    sm = pl.BlockSpec(memory_space=pltpu.SMEM)
    hb = pl.BlockSpec(memory_space=pl.ANY)
    gates = [jnp.transpose(w, (1, 2, 0)).reshape(32, -1) for w in (write_weight, decay_weight)]
    shape = jax.ShapeDtypeStruct
    q, k, v, pre, gate_row = pl.pallas_call(
        project_kernel,
        out_shape=(
            shape((n_lat, pair), BF16), shape((n_all, pair), BF16), shape((n_all, pair), BF16),
            shape((64, width), F32), shape((1, own_cols), F32),
        ),
        in_specs=[vm] * 8 + [hb] * 5,
        out_specs=(vm,) * 5,
        scratch_shapes=[
            pltpu.VMEM((n_lat, d), BF16), pltpu.VMEM((n_ctx, d), BF16), pltpu.VMEM((3, d, pair), BF16),
            pltpu.SemaphoreType.DMA((5,)), pltpu.VMEM((n_all, TILE), F32), pltpu.VMEM((4, 1, d), F32),
            pltpu.VMEM((n_all, d), BF16), pltpu.VMEM((8, own_cols), F32), pltpu.VMEM((8, own_cols), F32),
            pltpu.VMEM((4, own_cols), F32), pltpu.VMEM((3, 8, own_cols), F32), pltpu.VMEM((3, 8, own_cols), F32),
            pltpu.VMEM((8, 4, own_cols), F32), pltpu.SemaphoreType.DMA((13,)), pltpu.SemaphoreType.DMA((13,)),
        ],
        compiler_params=pltpu.CompilerParams(
            collective_id=0, has_side_effects=True, vmem_limit_bytes=48 * 1024 * 1024
        ),
        name="project",
    )(
        condition.reshape(1, -1), context_condition.reshape(1, -1), shift_weight, scale_weight, gate_weight,
        norm_gain.reshape(1, -1), *gates, latent, context, query_weight, key_weight, value_weight,
    )
    one_map = (TILE, 2 * TILE)
    return pl.pallas_call(
        token_kernel,
        out_shape=shape((n_lat, own_cols), BF16),
        in_specs=[vm] * 6 + [sm] * 3 + [hb] * 2,
        out_specs=vm,
        scratch_shapes=[
            pltpu.VMEM(out_weight.shape, BF16), pltpu.VMEM((n_lat, own_cols), BF16), pltpu.SemaphoreType.DMA((2,)),
            pltpu.VMEM((TILE, width), F32), pltpu.VMEM((width, TILE), F32),
            pltpu.VMEM((2, n_lat, n_lat), F32), pltpu.VMEM((2, n_lat, n_lat), F32),
            pltpu.VMEM((tiles, TILE, TILE), BF16), pltpu.VMEM((tiles, TILE, TILE), BF16),
            pltpu.VMEM((4, n_lat, n_lat), BF16), pltpu.VMEM((4, n_lat, n_lat), BF16),
            pltpu.VMEM((4, n_lat, 2 * TILE), BF16), pltpu.VMEM((4, n_lat, 2 * TILE), BF16),
            pltpu.VMEM((2, n_lat, TILE), F32), pltpu.VMEM((2, n_lat, 2 * TILE), BF16),
            pltpu.VMEM((4, *one_map), BF16), pltpu.VMEM((4, *one_map), BF16),
            pltpu.VMEM((4, *one_map), BF16), pltpu.VMEM((4, *one_map), BF16),
            pltpu.VMEM((4, *one_map), F32), pltpu.VMEM(one_map, BF16), pltpu.VMEM(one_map, BF16),
            pltpu.VMEM((4, *one_map), BF16), pltpu.VMEM((4, *one_map), BF16),
            pltpu.VMEM((4, TILE, TILE), BF16), pltpu.VMEM((4, TILE, TILE), BF16),
            pltpu.VMEM((8, n_lat, pair), BF16),
            pltpu.SemaphoreType.DMA((15,)), pltpu.SemaphoreType.DMA((15,)),
            pltpu.SemaphoreType.DMA((14,)), pltpu.SemaphoreType.DMA((14,)),
        ],
        compiler_params=pltpu.CompilerParams(
            collective_id=1, has_side_effects=True, vmem_limit_bytes=48 * 1024 * 1024
        ),
        name="tokens",
    )(q, k, v, pre, gate_row, head_gain.reshape(1, -1), write_bias, decay_bias, log_rate, latent, out_weight)


def solution(mesh):
    torus = Mesh(mesh.devices.reshape(4, 4, mesh.shape["tp"]), ("sp_0", "sp_1", "tp"))
    placed = (
        P(SP, None), P(SP, None), P(SP), P(SP), P(SP, "tp"), P(SP, "tp"), P(SP, "tp"), P(),
        P(None, "tp"), P(None, "tp"), P(None, "tp"), P(), P(), P(), P(), P(), P(), P(None, "tp"),
    )
    return jax.shard_map(body, mesh=torus, in_specs=placed, out_specs=P(SP, "tp"), check_vma=False)
```

```python
import jax
import jax.numpy as jnp
from jax import lax
from jax.experimental import pallas as pl
from jax.experimental.pallas import tpu as pltpu
from jax.sharding import Mesh
from jax.sharding import PartitionSpec as P

HEAD_DIM = 128
SP = ("sp_0", "sp_1")
EPS = 0.0001
F32 = jnp.float32
BF16 = jnp.bfloat16
TILE = 128
MESH = pl.DeviceIdType.MESH
LEVELS = (1, 2, 3, 4, 5, 6)


def mm(a, b):
    return jnp.dot(a.astype(BF16), b.astype(BF16), preferred_element_type=F32)


def mm_nt(a, b):
    return lax.dot_general(a, b, (((1,), (1,)), ((), ())), preferred_element_type=F32)


def mm_tn(a, b):
    return lax.dot_general(a, b, (((0,), (0,)), ((), ())), preferred_element_type=F32)


def iota2(shape, dim):
    return lax.broadcasted_iota(jnp.int32, shape, dim)


def softplus(u):
    return jnp.maximum(u, 0.0) + jnp.log1p(jnp.exp(-jnp.abs(u)))


def inv_norm(rows_bf16):
    r = rows_bf16.astype(F32)
    return lax.rsqrt(jnp.sum(r * r, axis=-1, keepdims=True) + EPS)


def gate_rows(first_head, pre_ref, wb_ref, db_ref, lr_ref, rows_ref, n_lat, n_ctx):
    width = n_lat + TILE
    lane = iota2((8, width), 1)
    is_ctx = lane >= n_lat
    pos = jnp.where(is_ctx, lane - n_lat, lane)
    size = jnp.where(is_ctx, n_ctx, n_lat)
    valid = pos < size
    row = iota2((8, width), 0)
    rates = jnp.zeros((8, width), F32)
    logd = jnp.zeros((8, width), F32)
    for c in range(4):
        d, h = c // 2, c % 2
        head = first_head + h
        at = d * 16 + head
        w = pre_ref[pl.ds(at, 1), :] + wb_ref[d, head]
        u = pre_ref[pl.ds(32 + at, 1), :] + db_ref[d, head]
        rate = 1.0 / (1.0 + jnp.exp(-w))
        step = -jnp.exp(jnp.full((1, width), lr_ref[d, head], F32)) * softplus(u)
        rates = jnp.where(row == c, rate, rates)
        logd = jnp.where(row == c, step, logd)
    rates = jnp.where(valid, rates, 0.0)
    logd = jnp.where(valid, logd, 0.0)
    fwd = logd
    bwd = logd
    s = 1
    while s < n_lat:
        fwd = fwd + jnp.where(pos >= s, pltpu.roll(fwd, s, 1), 0.0)
        bwd = bwd + jnp.where(pos + s < size, pltpu.roll(bwd, width - s, 1), 0.0)
        s *= 2
    g = jnp.where(row < 2, fwd, bwd)
    g = jnp.where(valid, g, 0.0)
    whole_lat = jnp.sum(jnp.where(is_ctx, 0.0, logd), axis=1, keepdims=True)
    whole_ctx = jnp.sum(jnp.where(is_ctx, logd, 0.0), axis=1, keepdims=True)
    late = jnp.exp(jnp.where(is_ctx, whole_ctx, whole_lat) - g)
    eg = jnp.exp(g)
    parts = []
    for a in (rates, g, late, eg):
        up = pltpu.roll(pltpu.roll(a, n_ctx, 1), 6, 0)
        a = jnp.where(lane >= n_lat + n_ctx, up, a)
        parts.append(a)
    rows_ref[...] = jnp.zeros_like(rows_ref)
    for n, a in enumerate(parts):
        rows_ref[8 * n : 8 * n + 8, :] = a
    return jnp.exp(whole_lat), jnp.exp(whole_ctx)


def split_rows(x):
    hi = x.astype(BF16)
    lo = (x - hi.astype(F32)).astype(BF16)
    return hi, lo


def mul_precise(m_bf16, x):
    hi, lo = split_rows(x)
    n = x.shape[1]
    y = jnp.dot(m_bf16, jnp.concatenate([hi, lo], axis=1), preferred_element_type=F32)
    return y[:, :n] + y[:, n:]


def then(next_map, total):
    y = mm(next_map[:, :TILE], total)
    zero = jnp.zeros((TILE, TILE), F32)
    return y + jnp.concatenate([zero, next_map[:, TILE:].astype(F32)], axis=1)


RATE, G, LATE, EG, KINV = 0, 8, 16, 24, 32


def remote(src, dst, send_sem, recv_sem, axis, peer):
    return pltpu.make_async_remote_copy(
        src_ref=src, dst_ref=dst, send_sem=send_sem, recv_sem=recv_sem, device_id={axis: peer}, device_id_type=MESH
    )


def greet(barrier, peers):
    for axis, peer in peers:
        pl.semaphore_signal(barrier, inc=1, device_id={axis: peer}, device_id_type=MESH)


def ring_peers(axis, size):
    me = lax.axis_index(axis)
    return [(axis, lax.rem(me + k, size)) for k in range(1, size)]


def project_kernel(
    cond_hbm, cctx_hbm, shift_hbm, scale_hbm, gate_hbm, gain_hbm, ww_hbm, wd_hbm,
    lat_hbm, ctx_hbm, wq_hbm, wk_hbm, wv_hbm,
    q_ref, k_ref, v_ref, pre_ref, gate_row_ref,
    cond_ref, cctx_ref, mod_w_ref, gain_ref, wg_ref, lat_ref, ctx_ref, w_ref, load_sem,
    inv_ref, piece_ref, acc_ref, pre_acc,
    part_ref, sum_ref, own_ref, xbuf, zbuf, tbuf, send_sem, recv_sem,
):
    barrier = pltpu.get_barrier_semaphore()
    t = lax.axis_index("tp")
    y_at, core = t // 2, lax.rem(t, 2)
    up = lax.rem(y_at + 1, 4) * 2 + core
    down = lax.rem(y_at + 3, 4) * 2 + core
    across = lax.rem(y_at + 2, 4) * 2 + core

    def other(block):
        return block + 1 - 2 * core

    targets = [other(t), up, down, other(up), other(down), across, other(across)]
    sources = [other(t), down, up, other(down), other(up), across, other(across)]
    xs, zs = ring_peers("sp_1", 4), ring_peers("sp_0", 4)
    greet(barrier, xs + zs + [("tp", peer) for peer in targets])
    loads = [
        pltpu.make_async_copy(src, dst, load_sem.at[n])
        for n, (src, dst) in enumerate(
            (
                (cond_hbm, cond_ref), (cctx_hbm, cctx_ref), (shift_hbm, mod_w_ref.at[0]), (scale_hbm, mod_w_ref.at[1]),
                (gate_hbm, mod_w_ref.at[2]), (lat_hbm, lat_ref), (ctx_hbm, ctx_ref), (gain_hbm, gain_ref),
                (ww_hbm, wg_ref.at[0:32]), (wd_hbm, wg_ref.at[32:64]),
                (wk_hbm, w_ref.at[0]), (wv_hbm, w_ref.at[1]), (wq_hbm, w_ref.at[2]),
            )
        )
    ]
    for load in loads:
        load.start()
    n_lat, n_ctx = lat_ref.shape[0], ctx_ref.shape[0]
    n_all = n_lat + n_ctx
    acc_ref[...] = jnp.zeros_like(acc_ref)
    pre_acc[...] = jnp.zeros_like(pre_acc)
    part_ref[...] = jnp.zeros_like(part_ref)
    for load in loads[:5]:
        load.wait()
    u = jnp.concatenate(
        [cond_ref[...].astype(F32).reshape(1, -1), cctx_ref[...].astype(F32).reshape(1, -1)], axis=0
    )
    silu = (u / (1.0 + jnp.exp(-u))).astype(BF16)
    part_ref[0:2, :] = jnp.dot(silu, mod_w_ref[0], preferred_element_type=F32)
    part_ref[2:4, :] = jnp.dot(silu, mod_w_ref[1], preferred_element_type=F32)
    part_ref[4:5, :] = jnp.dot(silu, mod_w_ref[2], preferred_element_type=F32)[0:1]
    pl.semaphore_wait(barrier, 13)
    phase_x = [
        remote(part_ref, xbuf.at[n], send_sem.at[n], recv_sem.at[n], *peer) for n, peer in enumerate(xs)
    ]
    for copy in phase_x:
        copy.start()
    for load in loads[5:7]:
        load.wait()

    def norms(src_ref, base):
        def step(i, carry):
            x = src_ref[pl.ds(i * 16, 16), :].astype(F32)
            inv = lax.rsqrt(jnp.mean(x * x, axis=-1, keepdims=True) + EPS)
            inv_ref[pl.ds(base + i * 16, 16), :] = jnp.broadcast_to(inv, (16, TILE))
            return carry

        return step

    lax.fori_loop(0, n_lat // 16, norms(lat_ref, 0), 0)
    lax.fori_loop(0, n_ctx // 16, norms(ctx_ref, n_lat), 0)
    for copy in phase_x:
        copy.wait()
    sum_ref[...] = part_ref[...] + xbuf[0] + xbuf[1] + xbuf[2]
    phase_z = [
        remote(sum_ref, zbuf.at[n], send_sem.at[3 + n], recv_sem.at[3 + n], *peer) for n, peer in enumerate(zs)
    ]
    for copy in phase_z:
        copy.start()
    for load in loads[7:]:
        load.wait()
    for copy in phase_z:
        copy.wait()
    whole = sum_ref[...] + zbuf[0] + zbuf[1] + zbuf[2]
    own_ref[...] = whole[0:4]
    gate_row_ref[...] = whole[4:5]
    phase_t = [
        remote(own_ref, tbuf.at[t], send_sem.at[6 + n], recv_sem.at[6 + n], "tp", peer)
        for n, peer in enumerate(targets)
    ]
    for copy in phase_t:
        copy.start()
    tbuf[t] = own_ref[...]
    wide = own_ref.shape[1]

    def piece(n, block):
        cols = pl.ds(pl.multiple_of(block * wide, wide), wide)
        gain = gain_ref[:, cols]
        rows = tbuf[block]
        slot = n % 2
        for src_ref, base, count, s in ((lat_ref, 0, n_lat, 0), (ctx_ref, n_lat, n_ctx, 1)):
            a = gain * (1.0 + rows[2 + s : 3 + s, :])
            b = rows[s : s + 1, :]
            x = src_ref[:, cols].astype(F32)
            inv = inv_ref[base : base + count, :]
            y = [
                x[:, j : j + TILE] * inv * a[:, j : j + TILE] + b[:, j : j + TILE] for j in range(0, wide, TILE)
            ]
            piece_ref[slot, base : base + count, :] = jnp.concatenate(y, axis=1).astype(BF16)
        m = piece_ref[slot]
        acc_ref[0] += jnp.dot(m, w_ref[0, cols, :], preferred_element_type=F32)
        acc_ref[1] += jnp.dot(m, w_ref[1, cols, :], preferred_element_type=F32)
        acc_ref[2, 0:n_lat] += jnp.dot(m[0:n_lat], w_ref[2, cols, :], preferred_element_type=F32)
        pre_acc[0:n_all, 0:64] += mm_nt(m, wg_ref[:, cols])

    piece(0, t)
    for n, block in enumerate(sources):
        phase_t[n].wait_recv()
        piece(n + 1, block)
    k_ref[...] = acc_ref[0].astype(BF16)
    v_ref[...] = acc_ref[1].astype(BF16)
    q_ref[...] = acc_ref[2, 0:n_lat].astype(BF16)
    for j in range(0, n_lat + TILE, TILE):
        rounded = pre_acc[j : j + TILE, :].astype(BF16).astype(F32)
        pre_ref[:, j : j + TILE] = jnp.transpose(rounded)[0:64]
    for copy in phase_t:
        copy.wait_send()


def inverses(ad_ref, t_ref, base, count):
    xor = iota2((TILE, TILE), 0) ^ iota2((TILE, TILE), 1)
    eye = jnp.where(xor == 0, 1.0, 0.0)
    ts = []
    for n in range(count):
        a = ad_ref[base + n].astype(F32)
        ts.append((eye - jnp.where(xor == 1, a, 0.0)).astype(BF16))
    for level in LEVELS:
        xs = []
        for n in range(count):
            off = jnp.where((xor >> level) == 1, ad_ref[base + n].astype(F32), 0.0).astype(BF16)
            xs.append(mm(ts[n], off).astype(BF16))
        ts = [(t.astype(F32) - mm(x, t)).astype(BF16) for x, t in zip(xs, ts)]
    for n in range(count):
        t_ref[base + n] = ts[n]


def token_kernel(
    q_ref, k_ref, v_ref, pre_ref, gate_row_ref, gain_ref, wb_ref, db_ref, lr_ref, lat_hbm, ow_hbm,
    out_ref,
    ow_ref, res_ref, load_sem,
    rows_ref, cols_ref, gk_ref, qk_ref, ad_ref, t_ref, ao_ref, p_ref, x_ref, xl_ref, o1_ref, q2_ref,
    lat_map, ctx_map, lat_all, ctx_all, prefix_ref, lat_total, ctx_total, lat_totals, ctx_totals,
    start_ref, mine_ref, ho_ref, send_sem, recv_sem, ho_send, ho_recv,
):
    n_lat = q_ref.shape[0]
    n_ctx = k_ref.shape[0] - n_lat
    blocks = n_lat // TILE
    width = n_lat + TILE
    x_at, z_at, t_at = lax.axis_index("sp_1"), lax.axis_index("sp_0"), lax.axis_index("tp")
    y_at, core = t_at // 2, lax.rem(t_at, 2)
    up = lax.rem(y_at + 1, 4) * 2 + core
    down = lax.rem(y_at + 3, 4) * 2 + core
    across = lax.rem(y_at + 2, 4) * 2 + core
    mate = y_at * 2 + 1 - core
    barrier = pltpu.get_barrier_semaphore()
    xs, zs = ring_peers("sp_1", 4), ring_peers("sp_0", 4)
    greet(barrier, xs + zs + [("tp", up), ("tp", down), ("tp", mate)])
    own_cols = out_ref.shape[1]
    load_w = pltpu.make_async_copy(ow_hbm, ow_ref, load_sem.at[0])
    load_r = pltpu.make_async_copy(
        lat_hbm.at[:, pl.ds(pl.multiple_of(t_at * own_cols, own_cols), own_cols)], res_ref, load_sem.at[1]
    )
    load_w.start()
    load_r.start()

    dec_lat, dec_ctx = gate_rows(t_at * 2, pre_ref, wb_ref, db_ref, lr_ref, rows_ref, n_lat, n_ctx)
    for b in range(blocks + 1):
        cols_ref[b * TILE : (b + 1) * TILE, :] = jnp.transpose(rows_ref[:, b * TILE : (b + 1) * TILE])

    def kcols(h):
        return k_ref[0:n_lat, h * TILE : (h + 1) * TILE]

    def kctx(h):
        kc = k_ref[n_lat : n_lat + n_ctx, h * TILE : (h + 1) * TILE]
        return jnp.concatenate([kc, kc], axis=0)

    def vctx(h):
        vc = v_ref[n_lat : n_lat + n_ctx, h * TILE : (h + 1) * TILE]
        return jnp.concatenate([vc, vc], axis=0)

    kinv = []
    for h in range(2):
        kinv.append(jnp.concatenate([inv_norm(kcols(h)), inv_norm(kctx(h))], axis=0))
    lane128 = iota2((width, TILE), 1)
    both = jnp.where(lane128 == 0, kinv[0], jnp.where(lane128 == 1, kinv[1], 0.0))
    ii = iota2((TILE, TILE), 0)
    jj = iota2((TILE, TILE), 1)
    xor = ii ^ jj
    for b in range(blocks + 1):
        rows_ref[:, b * TILE : (b + 1) * TILE] = jnp.where(
            ii < KINV,
            rows_ref[:, b * TILE : (b + 1) * TILE],
            pltpu.roll(jnp.transpose(both[b * TILE : (b + 1) * TILE, :]), KINV, 0),
        )

    for h in range(2):
        kc = kctx(h)
        g2 = mm_nt(kc, kc) * kinv[h][n_lat:] * rows_ref[KINV + h : KINV + h + 1, n_lat:]
        keep = jnp.where(ii < n_ctx, jnp.where(jj < ii, 1, 0), jnp.where(jj > ii, 1, 0))
        keep = jnp.where((ii < n_ctx) == (jj < n_ctx), keep, 0) == 1
        sp = cols_ref[n_lat:, G + h : G + h + 1] - rows_ref[G + h : G + h + 1, n_lat:]
        dm = jnp.where(keep, jnp.exp(jnp.where(keep, sp, 0.0)), 0.0)
        ad_ref[4 * blocks + h] = (g2 * dm * cols_ref[n_lat:, RATE + h : RATE + h + 1]).astype(BF16)
    pl.semaphore_wait(barrier, 9)

    def to_row(base, maps, everyone):
        copies = [
            remote(maps.at[peer], everyone.at[x_at], send_sem.at[base + n], recv_sem.at[base + n], axis, peer)
            for n, (axis, peer) in enumerate(xs)
        ]
        for copy in copies:
            copy.start()
        everyone[x_at] = maps[x_at]
        return copies

    def to_column(base, total, everyone):
        copies = [
            remote(total, everyone.at[z_at], send_sem.at[base + n], recv_sem.at[base + n], axis, peer)
            for n, (axis, peer) in enumerate(zs)
        ]
        for copy in copies:
            copy.start()
        everyone[z_at] = total[...]
        return copies

    qinvs = []
    for h in range(2):
        qh = q_ref[0:n_lat, h * TILE : (h + 1) * TILE]
        qinv = inv_norm(qh) * (HEAD_DIM**-0.5)
        qinvs.append(qinv)
        krow = rows_ref[KINV + h : KINV + h + 1, 0:n_lat]
        gk_ref[h] = mm_nt(kcols(h), kcols(h)) * kinv[h][0:n_lat] * krow
        qk_ref[h] = mm_nt(qh, kcols(h)) * qinv * krow
    for c in range(4):
        d, h = c // 2, c % 2
        for i in range(blocks):
            ri = cols_ref[i * TILE : (i + 1) * TILE, RATE + c : RATE + c + 1]
            gi = cols_ref[i * TILE : (i + 1) * TILE, G + c : G + c + 1]
            for j in range(blocks):
                if (d == 0 and j > i) or (d == 1 and j < i):
                    continue
                at = (slice(i * TILE, (i + 1) * TILE), slice(j * TILE, (j + 1) * TILE))
                sp = gi - rows_ref[G + c : G + c + 1, j * TILE : (j + 1) * TILE]
                if i == j:
                    keep = (ii >= jj) if d == 0 else (ii <= jj)
                    dm = jnp.where(keep, jnp.exp(jnp.where(keep, sp, 0.0)), 0.0)
                else:
                    dm = jnp.exp(sp)
                a = gk_ref[(h, *at)] * dm * ri
                if i == j:
                    ad_ref[c * blocks + i] = jnp.where(ii == jj, 0.0, a).astype(BF16)
                else:
                    ao_ref[(c, *at)] = a.astype(BF16)
                p_ref[(c, *at)] = (qk_ref[(h, *at)] * dm).astype(BF16)

    def invert(part, carry):
        inverses(ad_ref, t_ref, part * (tiles // 2), tiles // 2)
        return carry

    tiles = ad_ref.shape[0]
    lax.fori_loop(0, 2, invert, 0)

    for h in range(2):
        ci = kinv[h][n_lat:]
        cr = slice(n_lat, n_lat + TILE)
        rate = cols_ref[cr, RATE + h : RATE + h + 1]
        eg = cols_ref[cr, EG + h : EG + h + 1]
        late = cols_ref[cr, LATE + h : LATE + h + 1]
        kc = kctx(h)
        b = jnp.concatenate([vctx(h).astype(F32) * rate, kc.astype(F32) * (rate * eg * ci)], axis=1)
        x = mm(t_ref[4 * blocks + h], b)
        xl = (x * (late * ci)).astype(BF16)
        for d in range(2):
            c = d * 2 + h
            m = mm_tn(kc[0:n_ctx], xl[d * n_ctx : (d + 1) * n_ctx])
            diag = jnp.where(xor == 0, dec_ctx[c : c + 1, :], 0.0)
            ctx_map[c] = jnp.concatenate([diag - m[:, TILE:], m[:, :TILE]], axis=1).astype(BF16)

    ctx_rows = to_row(0, ctx_map, ctx_all)

    backwards = x_at >= 2

    def place(n, size):
        return jnp.where(backwards, size - 1 - n, n)

    lates, fronts, sides = {}, {}, {}
    for n in range(blocks):
        for c in range(4):
            d, h = c // 2, c % 2
            i = n if d == 0 else blocks - 1 - n
            r = slice(i * TILE, (i + 1) * TILE)
            rate = cols_ref[r, RATE + c : RATE + c + 1]
            ki = kinv[h][r]
            vi = v_ref[r, h * TILE : (h + 1) * TILE].astype(F32) * rate
            wi = k_ref[r, h * TILE : (h + 1) * TILE].astype(F32) * (rate * cols_ref[r, EG + c : EG + c + 1] * ki)
            lates[c, n] = cols_ref[r, LATE + c : LATE + c + 1] * ki
            t = t_ref[c * blocks + i]
            fronts[c, n] = mm(t, jnp.concatenate([vi, wi], axis=1))
            if n > 0:
                done = slice(0, i * TILE) if d == 0 else slice((i + 1) * TILE, n_lat)
                sides[c, n] = mm(t, ao_ref[c, r, done]).astype(BF16)
    for n in range(blocks):
        for c in range(4):
            d = c // 2
            i = n if d == 0 else blocks - 1 - n
            r = slice(i * TILE, (i + 1) * TILE)
            x = fronts[c, n]
            if n > 0:
                done = slice(0, i * TILE) if d == 0 else slice((i + 1) * TILE, n_lat)
                x = x - mm(sides[c, n], x_ref[c, done, :])
            x_ref[c, r, :] = x.astype(BF16)
            xl_ref[c, r, :] = (x * lates[c, n]).astype(BF16)
    for c in range(4):
        m = mm_tn(kcols(c % 2), xl_ref[c])
        diag = jnp.where(xor == 0, dec_lat[c : c + 1, :], 0.0)
        lat_map[c] = jnp.concatenate([diag - m[:, TILE:], m[:, :TILE]], axis=1).astype(BF16)
    lat_rows = to_row(6, lat_map, lat_all)

    for copy in ctx_rows:
        copy.wait()
    total = ctx_all[place(0, 4)].astype(F32)
    for n in range(1, 4):
        total = then(ctx_all[place(n, 4)], total)
    ctx_total[...] = total.astype(BF16)
    ctx_columns = to_column(3, ctx_total, ctx_totals)

    for h in range(2):
        o1 = []
        for d in range(2):
            c = d * 2 + h
            for i in range(blocks):
                r = slice(i * TILE, (i + 1) * TILE)
                seen = slice(0, (i + 1) * TILE) if d == 0 else slice(i * TILE, n_lat)
                ow = mm(p_ref[c, r, seen], x_ref[c, seen, :])
                qi = q_ref[r, h * TILE : (h + 1) * TILE].astype(F32)
                early = qi * (cols_ref[r, EG + c : EG + c + 1] * qinvs[h][r])
                q2_ref[h, r, d * TILE : (d + 1) * TILE] = (early - ow[:, TILE:]).astype(BF16)
                if d == 0:
                    o1.append(ow[:, :TILE])
                else:
                    o1_ref[h, r, :] = o1[i] + ow[:, :TILE]

    for copy in lat_rows:
        copy.wait()
    total = lat_all[place(0, 4)].astype(F32)
    for n in range(1, 4):
        at = place(n, 4)
        prefix_ref[at] = total
        total = then(lat_all[at], total)
    lat_total[...] = total.astype(BF16)
    lat_columns = to_column(9, lat_total, lat_totals)
    for copy in ctx_columns:
        copy.wait()
    state = None
    for n in range(4):
        one = ctx_totals[place(n, 4)]
        off = one[:, TILE:].astype(F32)
        state = off if n == 0 else mul_precise(one[:, :TILE], state) + off
    for copy in lat_columns:
        copy.wait()
    z_place = place(z_at, 4)
    for n in range(3):
        one = lat_totals[place(n, 4)]
        new = mul_precise(one[:, :TILE], state) + one[:, TILE:].astype(F32)
        state = jnp.where(n < z_place, new, state)
    start_ref[place(0, 4)] = state.astype(BF16)
    for n in range(1, 4):
        at = place(n, 4)
        mk = prefix_ref[at]
        start_ref[at] = (mul_precise(mk[:, :TILE].astype(BF16), state) + mk[:, TILE:]).astype(BF16)
    starts = to_row(12, start_ref, mine_ref)
    for copy in starts:
        copy.wait()

    half = n_lat // 2
    A, B = slice(0, half), slice(half, n_lat)

    def finish(r):
        for h in range(2):
            both_s = jnp.concatenate([mine_ref[h], mine_ref[2 + h]], axis=0)
            y = o1_ref[h, r, :] + jnp.dot(q2_ref[h, r, :], both_s, preferred_element_type=F32)
            y = y * lax.rsqrt(jnp.mean(y * y, axis=-1, keepdims=True) + EPS) * gain_ref[...]
            ho_ref[t_at, r, h * TILE : (h + 1) * TILE] = y.astype(BF16)

    def hand(n, block, r, peer):
        copy = remote(ho_ref.at[block, r], ho_ref.at[block, r], ho_send.at[n], ho_recv.at[n], "tp", peer)
        copy.start()
        return copy

    hands = {}
    finish(A)
    hands[0] = hand(0, t_at, A, up)
    hands[4] = hand(4, t_at, A, mate)
    finish(B)
    hands[3] = hand(3, t_at, B, down)
    hands[1] = hand(1, t_at, B, up)
    hands[2] = hand(2, t_at, A, down)
    hands[5] = hand(5, t_at, B, mate)
    load_w.wait()
    load_r.wait()
    depth = 2 * TILE

    def add(block):
        w = ow_ref[pl.ds(pl.multiple_of(block * depth, depth), depth), :]
        return jnp.dot(ho_ref[block], w, preferred_element_type=F32)

    hands[0].wait_recv()
    hands[6] = hand(6, down, A, up)
    hands[8] = hand(8, down, A, mate)
    hands[3].wait_recv()
    hands[7] = hand(7, up, B, down)
    hands[11] = hand(11, up, B, mate)
    hands[4].wait_recv()
    hands[5].wait_recv()
    acc = add(t_at) + add(mate)
    hands[1].wait_recv()
    hands[9] = hand(9, down, B, mate)
    hands[2].wait_recv()
    hands[10] = hand(10, up, A, mate)
    acc = acc + add(down) + add(up)
    hands[6].wait_recv()
    hands[12] = hand(12, across, A, mate)
    hands[7].wait_recv()
    hands[13] = hand(13, across, B, mate)
    for n in range(8, 12):
        hands[n].wait_recv()

    def other(block):
        return block + 1 - 2 * core

    acc = acc + add(other(down)) + add(other(up)) + add(across)
    hands[12].wait_recv()
    hands[13].wait_recv()
    acc = acc + add(other(across))
    out_ref[...] = (res_ref[...].astype(F32) + gate_row_ref[...] * acc).astype(BF16)
    for n in range(14):
        hands[n].wait_send()


def body(
    latent, context, condition, context_condition, shift_weight, scale_weight, gate_weight, norm_gain,
    query_weight, key_weight, value_weight, write_weight, decay_weight, write_bias, decay_bias, log_rate,
    head_gain, out_weight,
):
    n_lat, d = latent.shape
    n_ctx = context.shape[0]
    n_all = n_lat + n_ctx
    own_cols = gate_weight.shape[1]
    pair = query_weight.shape[1]
    blocks = n_lat // TILE
    tiles = 4 * blocks + 2
    width = n_lat + TILE
    vm = pl.BlockSpec(memory_space=pltpu.VMEM)
    sm = pl.BlockSpec(memory_space=pltpu.SMEM)
    hb = pl.BlockSpec(memory_space=pltpu.HBM)
    gates = [jnp.transpose(w, (1, 2, 0)).reshape(32, -1) for w in (write_weight, decay_weight)]
    shape = jax.ShapeDtypeStruct
    q, k, v, pre, gate_row = pl.pallas_call(
        project_kernel,
        out_shape=(
            shape((n_lat, pair), BF16), shape((n_all, pair), BF16), shape((n_all, pair), BF16),
            shape((64, width), F32), shape((1, own_cols), F32),
        ),
        in_specs=[hb] * 13,
        out_specs=(vm,) * 5,
        scratch_shapes=[
            pltpu.VMEM(condition.shape, BF16), pltpu.VMEM(condition.shape, BF16),
            pltpu.VMEM((3, *shift_weight.shape), BF16), pltpu.VMEM((1, d), F32), pltpu.VMEM((64, d), BF16),
            pltpu.VMEM((n_lat, d), BF16), pltpu.VMEM((n_ctx, d), BF16), pltpu.VMEM((3, d, pair), BF16),
            pltpu.SemaphoreType.DMA((13,)), pltpu.VMEM((n_all, TILE), F32), pltpu.VMEM((2, n_all, own_cols), BF16),
            pltpu.VMEM((3, n_all, pair), F32), pltpu.VMEM((width, TILE), F32),
            pltpu.VMEM((8, own_cols), F32), pltpu.VMEM((8, own_cols), F32),
            pltpu.VMEM((4, own_cols), F32), pltpu.VMEM((3, 8, own_cols), F32), pltpu.VMEM((3, 8, own_cols), F32),
            pltpu.VMEM((8, 4, own_cols), F32), pltpu.SemaphoreType.DMA((13,)), pltpu.SemaphoreType.DMA((13,)),
        ],
        compiler_params=pltpu.CompilerParams(
            collective_id=0, has_side_effects=True, vmem_limit_bytes=48 * 1024 * 1024
        ),
        name="project",
    )(
        condition, context_condition, shift_weight, scale_weight, gate_weight,
        norm_gain.reshape(1, -1), *gates, latent, context, query_weight, key_weight, value_weight,
    )
    one_map = (TILE, 2 * TILE)
    return pl.pallas_call(
        token_kernel,
        out_shape=shape((n_lat, own_cols), BF16),
        in_specs=[vm] * 6 + [sm] * 3 + [hb] * 2,
        out_specs=vm,
        scratch_shapes=[
            pltpu.VMEM(out_weight.shape, BF16), pltpu.VMEM((n_lat, own_cols), BF16), pltpu.SemaphoreType.DMA((2,)),
            pltpu.VMEM((TILE, width), F32), pltpu.VMEM((width, TILE), F32),
            pltpu.VMEM((2, n_lat, n_lat), F32), pltpu.VMEM((2, n_lat, n_lat), F32),
            pltpu.VMEM((tiles, TILE, TILE), BF16), pltpu.VMEM((tiles, TILE, TILE), BF16),
            pltpu.VMEM((4, n_lat, n_lat), BF16), pltpu.VMEM((4, n_lat, n_lat), BF16),
            pltpu.VMEM((4, n_lat, 2 * TILE), BF16), pltpu.VMEM((4, n_lat, 2 * TILE), BF16),
            pltpu.VMEM((2, n_lat, TILE), F32), pltpu.VMEM((2, n_lat, 2 * TILE), BF16),
            pltpu.VMEM((4, *one_map), BF16), pltpu.VMEM((4, *one_map), BF16),
            pltpu.VMEM((4, *one_map), BF16), pltpu.VMEM((4, *one_map), BF16),
            pltpu.VMEM((4, *one_map), F32), pltpu.VMEM(one_map, BF16), pltpu.VMEM(one_map, BF16),
            pltpu.VMEM((4, *one_map), BF16), pltpu.VMEM((4, *one_map), BF16),
            pltpu.VMEM((4, TILE, TILE), BF16), pltpu.VMEM((4, TILE, TILE), BF16),
            pltpu.VMEM((8, n_lat, pair), BF16),
            pltpu.SemaphoreType.DMA((15,)), pltpu.SemaphoreType.DMA((15,)),
            pltpu.SemaphoreType.DMA((14,)), pltpu.SemaphoreType.DMA((14,)),
        ],
        compiler_params=pltpu.CompilerParams(
            collective_id=1, has_side_effects=True, vmem_limit_bytes=48 * 1024 * 1024
        ),
        name="tokens",
    )(q, k, v, pre, gate_row, head_gain.reshape(1, -1), write_bias, decay_bias, log_rate, latent, out_weight)


def solution(mesh):
    torus = Mesh(mesh.devices.reshape(4, 4, mesh.shape["tp"]), ("sp_0", "sp_1", "tp"))
    placed = (
        P(SP, None), P(SP, None), P(SP), P(SP), P(SP, "tp"), P(SP, "tp"), P(SP, "tp"), P(),
        P(None, "tp"), P(None, "tp"), P(None, "tp"), P(), P(), P(), P(), P(), P(), P(None, "tp"),
    )
    return jax.shard_map(body, mesh=torus, in_specs=placed, out_specs=P(SP, "tp"), check_vma=False)
```

```python
import jax
import jax.numpy as jnp
from jax import lax
from jax.experimental import pallas as pl
from jax.experimental.pallas import tpu as pltpu
from jax.sharding import Mesh
from jax.sharding import PartitionSpec as P

HEAD_DIM = 128
SP = ("sp_0", "sp_1")
EPS = 0.0001
F32 = jnp.float32
BF16 = jnp.bfloat16
TILE = 128
VMEM_LIMIT = 67043328
MESH = pl.DeviceIdType.MESH
LEVELS = (1, 2, 3, 4, 5, 6)


def mm(a, b):
    return jnp.dot(a.astype(BF16), b.astype(BF16), preferred_element_type=F32)


def mm_nt(a, b):
    return lax.dot_general(a, b, (((1,), (1,)), ((), ())), preferred_element_type=F32)


def mm_tn(a, b):
    return lax.dot_general(a, b, (((0,), (0,)), ((), ())), preferred_element_type=F32)


def iota2(shape, dim):
    return lax.broadcasted_iota(jnp.int32, shape, dim)


def softplus(u):
    return jnp.maximum(u, 0.0) + jnp.log1p(jnp.exp(-jnp.abs(u)))


def inv_norm(rows_bf16):
    r = rows_bf16.astype(F32)
    return lax.rsqrt(jnp.sum(r * r, axis=-1, keepdims=True) + EPS)


def gate_rows(first_head, pre_ref, wb_ref, db_ref, lr_ref, rows_ref, n_lat, n_ctx):
    width = n_lat + TILE
    lane = iota2((8, width), 1)
    is_ctx = lane >= n_lat
    pos = jnp.where(is_ctx, lane - n_lat, lane)
    size = jnp.where(is_ctx, n_ctx, n_lat)
    valid = pos < size
    row = iota2((8, width), 0)
    rates = jnp.zeros((8, width), F32)
    logd = jnp.zeros((8, width), F32)
    for c in range(4):
        d, h = c // 2, c % 2
        head = first_head + h
        at = d * 16 + head
        w = pre_ref[pl.ds(at, 1), :] + wb_ref[d, head]
        u = pre_ref[pl.ds(32 + at, 1), :] + db_ref[d, head]
        rate = 1.0 / (1.0 + jnp.exp(-w))
        step = -jnp.exp(jnp.full((1, width), lr_ref[d, head], F32)) * softplus(u)
        rates = jnp.where(row == c, rate, rates)
        logd = jnp.where(row == c, step, logd)
    rates = jnp.where(valid, rates, 0.0)
    logd = jnp.where(valid, logd, 0.0)
    fwd = logd
    bwd = logd
    s = 1
    while s < n_lat:
        fwd = fwd + jnp.where(pos >= s, pltpu.roll(fwd, s, 1), 0.0)
        bwd = bwd + jnp.where(pos + s < size, pltpu.roll(bwd, width - s, 1), 0.0)
        s *= 2
    g = jnp.where(row < 2, fwd, bwd)
    g = jnp.where(valid, g, 0.0)
    whole_lat = jnp.sum(jnp.where(is_ctx, 0.0, logd), axis=1, keepdims=True)
    whole_ctx = jnp.sum(jnp.where(is_ctx, logd, 0.0), axis=1, keepdims=True)
    late = jnp.exp(jnp.where(is_ctx, whole_ctx, whole_lat) - g)
    eg = jnp.exp(g)
    parts = []
    for a in (rates, g, late, eg):
        up = pltpu.roll(pltpu.roll(a, n_ctx, 1), 6, 0)
        a = jnp.where(lane >= n_lat + n_ctx, up, a)
        parts.append(a)
    rows_ref[...] = jnp.zeros_like(rows_ref)
    for n, a in enumerate(parts):
        rows_ref[8 * n : 8 * n + 8, :] = a
    return jnp.exp(whole_lat), jnp.exp(whole_ctx)


def split_rows(x):
    hi = x.astype(BF16)
    lo = (x - hi.astype(F32)).astype(BF16)
    return hi, lo


def mul_precise(m_bf16, x):
    hi, lo = split_rows(x)
    n = x.shape[1]
    y = jnp.dot(m_bf16, jnp.concatenate([hi, lo], axis=1), preferred_element_type=F32)
    return y[:, :n] + y[:, n:]


def then(next_map, total):
    y = mm(next_map[:, :TILE], total)
    zero = jnp.zeros((TILE, TILE), F32)
    return y + jnp.concatenate([zero, next_map[:, TILE:].astype(F32)], axis=1)


RATE, G, LATE, EG, KINV = 0, 8, 16, 24, 32


def remote(src, dst, send_sem, recv_sem, axis, peer):
    return pltpu.make_async_remote_copy(
        src_ref=src, dst_ref=dst, send_sem=send_sem, recv_sem=recv_sem, device_id={axis: peer}, device_id_type=MESH
    )


def greet(barrier, peers):
    for axis, peer in peers:
        pl.semaphore_signal(barrier, inc=1, device_id={axis: peer}, device_id_type=MESH)


def ring_peers(axis, size):
    me = lax.axis_index(axis)
    return [(axis, lax.rem(me + k, size)) for k in range(1, size)]


def inverses(ad_ref, t_ref, base, count):
    xor = iota2((TILE, TILE), 0) ^ iota2((TILE, TILE), 1)
    eye = jnp.where(xor == 0, 1.0, 0.0)
    ts = []
    for n in range(count):
        a = ad_ref[base + n].astype(F32)
        ts.append((eye - jnp.where(xor == 1, a, 0.0)).astype(BF16))
    for level in LEVELS:
        xs = []
        for n in range(count):
            off = jnp.where((xor >> level) == 1, ad_ref[base + n].astype(F32), 0.0).astype(BF16)
            xs.append(mm(ts[n], off).astype(BF16))
        ts = [(t.astype(F32) - mm(x, t)).astype(BF16) for x, t in zip(xs, ts)]
    for n in range(count):
        t_ref[base + n] = ts[n]


def mix_tokens(
    q_ref, k_ref, v_ref, pre_ref, gate_row_ref, gain_ref, wb_ref, db_ref, lr_ref, lat_ref, ow_ref,
    out_ref,
    rows_ref, cols_ref, gk_ref, qk_ref, dm_ref, ad_ref, t_ref, ao_ref, p_ref, x_ref, xl_ref, o1_ref, q2_ref,
    lat_map, ctx_map, lat_all, ctx_all, prefix_ref, lat_total, ctx_total, lat_totals, ctx_totals,
    start_ref, mine_ref, ho_ref, send_sem, recv_sem, ho_send, ho_recv,
):
    n_lat = q_ref.shape[0]
    n_ctx = k_ref.shape[0] - n_lat
    blocks = n_lat // TILE
    width = n_lat + TILE
    x_at, z_at, t_at = lax.axis_index("sp_1"), lax.axis_index("sp_0"), lax.axis_index("tp")
    y_at, core = t_at // 2, lax.rem(t_at, 2)
    up = lax.rem(y_at + 1, 4) * 2 + core
    down = lax.rem(y_at + 3, 4) * 2 + core
    across = lax.rem(y_at + 2, 4) * 2 + core
    mate = y_at * 2 + 1 - core
    xs, zs = ring_peers("sp_1", 4), ring_peers("sp_0", 4)
    own_cols = out_ref.shape[1]

    dec_lat, dec_ctx = gate_rows(t_at * 2, pre_ref, wb_ref, db_ref, lr_ref, rows_ref, n_lat, n_ctx)
    for b in range(blocks + 1):
        cols_ref[b * TILE : (b + 1) * TILE, :] = jnp.transpose(rows_ref[:, b * TILE : (b + 1) * TILE])

    def kcols(h):
        return k_ref[0:n_lat, h * TILE : (h + 1) * TILE]

    def kctx(h):
        kc = k_ref[n_lat : n_lat + n_ctx, h * TILE : (h + 1) * TILE]
        return jnp.concatenate([kc, kc], axis=0)

    def vctx(h):
        vc = v_ref[n_lat : n_lat + n_ctx, h * TILE : (h + 1) * TILE]
        return jnp.concatenate([vc, vc], axis=0)

    kinv = []
    for h in range(2):
        kinv.append(jnp.concatenate([inv_norm(kcols(h)), inv_norm(kctx(h))], axis=0))
    lane128 = iota2((width, TILE), 1)
    both = jnp.where(lane128 == 0, kinv[0], jnp.where(lane128 == 1, kinv[1], 0.0))
    ii = iota2((TILE, TILE), 0)
    jj = iota2((TILE, TILE), 1)
    xor = ii ^ jj
    for b in range(blocks + 1):
        rows_ref[:, b * TILE : (b + 1) * TILE] = jnp.where(
            ii < KINV,
            rows_ref[:, b * TILE : (b + 1) * TILE],
            pltpu.roll(jnp.transpose(both[b * TILE : (b + 1) * TILE, :]), KINV, 0),
        )

    for h in range(2):
        kc = kctx(h)
        g2 = mm_nt(kc, kc) * kinv[h][n_lat:] * rows_ref[KINV + h : KINV + h + 1, n_lat:]
        keep = jnp.where(ii < n_ctx, jnp.where(jj < ii, 1, 0), jnp.where(jj > ii, 1, 0))
        keep = jnp.where((ii < n_ctx) == (jj < n_ctx), keep, 0) == 1
        sp = cols_ref[n_lat:, G + h : G + h + 1] - rows_ref[G + h : G + h + 1, n_lat:]
        dm = jnp.where(keep, jnp.exp(jnp.where(keep, sp, 0.0)), 0.0)
        ad_ref[4 * blocks + h] = (g2 * dm * cols_ref[n_lat:, RATE + h : RATE + h + 1]).astype(BF16)
    def to_row(base, maps, everyone):
        copies = [
            remote(maps.at[peer], everyone.at[x_at], send_sem.at[base + n], recv_sem.at[base + n], axis, peer)
            for n, (axis, peer) in enumerate(xs)
        ]
        for copy in copies:
            copy.start()
        everyone[x_at] = maps[x_at]
        return copies

    def to_column(base, total, everyone):
        copies = [
            remote(total, everyone.at[z_at], send_sem.at[base + n], recv_sem.at[base + n], axis, peer)
            for n, (axis, peer) in enumerate(zs)
        ]
        for copy in copies:
            copy.start()
        everyone[z_at] = total[...]
        return copies

    for h in range(2):
        krow = rows_ref[KINV + h : KINV + h + 1, 0:n_lat]
        gk_ref[h] = mm_nt(kcols(h), kcols(h)) * kinv[h][0:n_lat] * krow
    for c in range(4):
        d, h = c // 2, c % 2
        for i in range(blocks):
            ri = cols_ref[i * TILE : (i + 1) * TILE, RATE + c : RATE + c + 1]
            gi = cols_ref[i * TILE : (i + 1) * TILE, G + c : G + c + 1]
            for j in range(blocks):
                if (d == 0 and j > i) or (d == 1 and j < i):
                    continue
                at = (slice(i * TILE, (i + 1) * TILE), slice(j * TILE, (j + 1) * TILE))
                sp = gi - rows_ref[G + c : G + c + 1, j * TILE : (j + 1) * TILE]
                if i == j:
                    keep = (ii >= jj) if d == 0 else (ii <= jj)
                    dm = jnp.where(keep, jnp.exp(jnp.where(keep, sp, 0.0)), 0.0)
                else:
                    dm = jnp.exp(sp)
                a = gk_ref[(h, *at)] * dm * ri
                if i == j:
                    ad_ref[c * blocks + i] = jnp.where(ii == jj, 0.0, a).astype(BF16)
                else:
                    ao_ref[(c, *at)] = a.astype(BF16)
                dm_ref[(c, *at)] = dm

    inverses(ad_ref, t_ref, 0, ad_ref.shape[0])
    for h in range(2):
        ci = kinv[h][n_lat:]
        cr = slice(n_lat, n_lat + TILE)
        rate = cols_ref[cr, RATE + h : RATE + h + 1]
        eg = cols_ref[cr, EG + h : EG + h + 1]
        late = cols_ref[cr, LATE + h : LATE + h + 1]
        kc = kctx(h)
        b = jnp.concatenate([vctx(h).astype(F32) * rate, kc.astype(F32) * (rate * eg * ci)], axis=1)
        x = mm(t_ref[4 * blocks + h], b)
        xl = (x * (late * ci)).astype(BF16)
        for d in range(2):
            c = d * 2 + h
            m = mm_tn(kc[0:n_ctx], xl[d * n_ctx : (d + 1) * n_ctx])
            diag = jnp.where(xor == 0, dec_ctx[c : c + 1, :], 0.0)
            ctx_map[c] = jnp.concatenate([diag - m[:, TILE:], m[:, :TILE]], axis=1).astype(BF16)

    ctx_rows = to_row(0, ctx_map, ctx_all)

    backwards = x_at >= 2

    def place(n, size):
        return jnp.where(backwards, size - 1 - n, n)

    lates, fronts, sides = {}, {}, {}
    for n in range(blocks):
        for c in range(4):
            d, h = c // 2, c % 2
            i = n if d == 0 else blocks - 1 - n
            r = slice(i * TILE, (i + 1) * TILE)
            rate = cols_ref[r, RATE + c : RATE + c + 1]
            ki = kinv[h][r]
            vi = v_ref[r, h * TILE : (h + 1) * TILE].astype(F32) * rate
            wi = k_ref[r, h * TILE : (h + 1) * TILE].astype(F32) * (rate * cols_ref[r, EG + c : EG + c + 1] * ki)
            lates[c, n] = cols_ref[r, LATE + c : LATE + c + 1] * ki
            t = t_ref[c * blocks + i]
            fronts[c, n] = mm(t, jnp.concatenate([vi, wi], axis=1))
            if n > 0:
                done = slice(0, i * TILE) if d == 0 else slice((i + 1) * TILE, n_lat)
                sides[c, n] = mm(t, ao_ref[c, r, done]).astype(BF16)
    for n in range(blocks):
        for c in range(4):
            d = c // 2
            i = n if d == 0 else blocks - 1 - n
            r = slice(i * TILE, (i + 1) * TILE)
            x = fronts[c, n]
            if n > 0:
                done = slice(0, i * TILE) if d == 0 else slice((i + 1) * TILE, n_lat)
                x = x - mm(sides[c, n], x_ref[c, done, :])
            x_ref[c, r, :] = x.astype(BF16)
            xl_ref[c, r, :] = (x * lates[c, n]).astype(BF16)
    for c in range(4):
        m = mm_tn(kcols(c % 2), xl_ref[c])
        diag = jnp.where(xor == 0, dec_lat[c : c + 1, :], 0.0)
        lat_map[c] = jnp.concatenate([diag - m[:, TILE:], m[:, :TILE]], axis=1).astype(BF16)
    lat_rows = to_row(6, lat_map, lat_all)

    for copy in ctx_rows:
        copy.wait()
    total = ctx_all[place(0, 4)].astype(F32)
    for n in range(1, 4):
        total = then(ctx_all[place(n, 4)], total)
    ctx_total[...] = total.astype(BF16)
    ctx_columns = to_column(3, ctx_total, ctx_totals)

    qinvs = []
    for h in range(2):
        qh = q_ref[0:n_lat, h * TILE : (h + 1) * TILE]
        qinv = inv_norm(qh) * (HEAD_DIM**-0.5)
        qinvs.append(qinv)
        qk_ref[h] = mm_nt(qh, kcols(h)) * qinv * rows_ref[KINV + h : KINV + h + 1, 0:n_lat]
    for c in range(4):
        d, h = c // 2, c % 2
        for i in range(blocks):
            r = slice(i * TILE, (i + 1) * TILE)
            seen = slice(0, (i + 1) * TILE) if d == 0 else slice(i * TILE, n_lat)
            p_ref[c, r, seen] = (qk_ref[h, r, seen] * dm_ref[c, r, seen]).astype(BF16)
    for h in range(2):
        o1 = []
        for d in range(2):
            c = d * 2 + h
            for i in range(blocks):
                r = slice(i * TILE, (i + 1) * TILE)
                seen = slice(0, (i + 1) * TILE) if d == 0 else slice(i * TILE, n_lat)
                ow = mm(p_ref[c, r, seen], x_ref[c, seen, :])
                qi = q_ref[r, h * TILE : (h + 1) * TILE].astype(F32)
                early = qi * (cols_ref[r, EG + c : EG + c + 1] * qinvs[h][r])
                q2_ref[h, r, d * TILE : (d + 1) * TILE] = (early - ow[:, TILE:]).astype(BF16)
                if d == 0:
                    o1.append(ow[:, :TILE])
                else:
                    o1_ref[h, r, :] = o1[i] + ow[:, :TILE]

    for copy in lat_rows:
        copy.wait()
    total = lat_all[place(0, 4)].astype(F32)
    for n in range(1, 4):
        at = place(n, 4)
        prefix_ref[at] = total
        total = then(lat_all[at], total)
    lat_total[...] = total.astype(BF16)
    lat_columns = to_column(9, lat_total, lat_totals)
    for copy in ctx_columns:
        copy.wait()
    state = None
    for n in range(4):
        one = ctx_totals[place(n, 4)]
        off = one[:, TILE:].astype(F32)
        state = off if n == 0 else mul_precise(one[:, :TILE], state) + off
    for copy in lat_columns:
        copy.wait()
    z_place = place(z_at, 4)
    for n in range(3):
        one = lat_totals[place(n, 4)]
        new = mul_precise(one[:, :TILE], state) + one[:, TILE:].astype(F32)
        state = jnp.where(n < z_place, new, state)
    start_ref[place(0, 4)] = state.astype(BF16)
    for n in range(1, 4):
        at = place(n, 4)
        mk = prefix_ref[at]
        start_ref[at] = (mul_precise(mk[:, :TILE].astype(BF16), state) + mk[:, TILE:]).astype(BF16)
    starts = to_row(12, start_ref, mine_ref)
    for copy in starts:
        copy.wait()

    half = n_lat // 2
    A, B = slice(0, half), slice(half, n_lat)

    def finish(r):
        for h in range(2):
            both_s = jnp.concatenate([mine_ref[h], mine_ref[2 + h]], axis=0)
            y = o1_ref[h, r, :] + jnp.dot(q2_ref[h, r, :], both_s, preferred_element_type=F32)
            y = y * lax.rsqrt(jnp.mean(y * y, axis=-1, keepdims=True) + EPS) * gain_ref[...]
            ho_ref[t_at, r, h * TILE : (h + 1) * TILE] = y.astype(BF16)

    def hand(n, block, r, peer):
        copy = remote(ho_ref.at[block, r], ho_ref.at[block, r], ho_send.at[n], ho_recv.at[n], "tp", peer)
        copy.start()
        return copy

    hands = {}
    finish(A)
    hands[0] = hand(0, t_at, A, up)
    hands[4] = hand(4, t_at, A, mate)
    finish(B)
    hands[3] = hand(3, t_at, B, down)
    hands[1] = hand(1, t_at, B, up)
    hands[2] = hand(2, t_at, A, down)
    hands[5] = hand(5, t_at, B, mate)
    depth = 2 * TILE

    def add(block):
        w = ow_ref[pl.ds(pl.multiple_of(block * depth, depth), depth), :]
        return jnp.dot(ho_ref[block], w, preferred_element_type=F32)

    hands[0].wait_recv()
    hands[6] = hand(6, down, A, up)
    hands[8] = hand(8, down, A, mate)
    hands[3].wait_recv()
    hands[7] = hand(7, up, B, down)
    hands[11] = hand(11, up, B, mate)
    hands[4].wait_recv()
    hands[5].wait_recv()
    acc = add(t_at) + add(mate)
    hands[1].wait_recv()
    hands[9] = hand(9, down, B, mate)
    hands[2].wait_recv()
    hands[10] = hand(10, up, A, mate)
    acc = acc + add(down) + add(up)
    hands[6].wait_recv()
    hands[12] = hand(12, across, A, mate)
    hands[7].wait_recv()
    hands[13] = hand(13, across, B, mate)
    for n in range(8, 12):
        hands[n].wait_recv()

    def other(block):
        return block + 1 - 2 * core

    acc = acc + add(other(down)) + add(other(up)) + add(across)
    hands[12].wait_recv()
    hands[13].wait_recv()
    acc = acc + add(other(across))
    own = lat_ref[:, pl.ds(pl.multiple_of(t_at * own_cols, own_cols), own_cols)]
    out_ref[...] = (own.astype(F32) + gate_row_ref[...] * acc).astype(BF16)
    for n in range(14):
        hands[n].wait_send()


def mixer_kernel(
    cond_hbm, cctx_hbm, shift_hbm, scale_hbm, gate_hbm, gain_hbm, ww_hbm, wd_hbm,
    lat_hbm, ctx_hbm, wq_hbm, wk_hbm, wv_hbm, wb_hbm, db_hbm, lr_hbm, hg_hbm, ow_hbm,
    out_ref,
    q_ref, k_ref, v_ref, pre_ref, gate_row_ref,
    cond_ref, cctx_ref, mod_w_ref, gain_ref, wg_ref, lat_ref, ctx_ref, w_ref, wb_ref, db_ref, lr_ref, hg_ref, ow_ref,
    load_sem, inv_ref, piece_ref, acc_ref, pre_acc,
    part_ref, sum_ref, own_ref, xbuf, zbuf, tbuf, mod_send, mod_recv, *scratch,
):
    barrier = pltpu.get_barrier_semaphore()
    t = lax.axis_index("tp")
    y_at, core = t // 2, lax.rem(t, 2)
    up = lax.rem(y_at + 1, 4) * 2 + core
    down = lax.rem(y_at + 3, 4) * 2 + core
    across = lax.rem(y_at + 2, 4) * 2 + core

    def other(block):
        return block + 1 - 2 * core

    targets = [other(t), up, down, other(up), other(down), across, other(across)]
    sources = [other(t), down, up, other(down), other(up), across, other(across)]
    xs, zs = ring_peers("sp_1", 4), ring_peers("sp_0", 4)
    greet(barrier, xs + zs + [("tp", peer) for peer in targets])
    loads = [
        pltpu.make_async_copy(src, dst, load_sem.at[n])
        for n, (src, dst) in enumerate(
            (
                (cond_hbm, cond_ref), (cctx_hbm, cctx_ref), (shift_hbm, mod_w_ref.at[0]), (scale_hbm, mod_w_ref.at[1]),
                (gate_hbm, mod_w_ref.at[2]), (lat_hbm, lat_ref), (ctx_hbm, ctx_ref), (gain_hbm, gain_ref),
                (ww_hbm, wg_ref.at[0:32]), (wd_hbm, wg_ref.at[32:64]),
                (wk_hbm, w_ref.at[0]), (wv_hbm, w_ref.at[1]), (wq_hbm, w_ref.at[2]),
                (wb_hbm, wb_ref), (db_hbm, db_ref), (lr_hbm, lr_ref), (hg_hbm, hg_ref), (ow_hbm, ow_ref),
            )
        )
    ]
    for load in loads:
        load.start()
    n_lat, n_ctx = lat_ref.shape[0], ctx_ref.shape[0]
    n_all = n_lat + n_ctx
    acc_ref[...] = jnp.zeros_like(acc_ref)
    pre_acc[...] = jnp.zeros_like(pre_acc)
    part_ref[...] = jnp.zeros_like(part_ref)
    for load in loads[:5]:
        load.wait()
    u = jnp.concatenate(
        [cond_ref[...].astype(F32).reshape(1, -1), cctx_ref[...].astype(F32).reshape(1, -1)], axis=0
    )
    silu = (u / (1.0 + jnp.exp(-u))).astype(BF16)
    part_ref[0:2, :] = jnp.dot(silu, mod_w_ref[0], preferred_element_type=F32)
    part_ref[2:4, :] = jnp.dot(silu, mod_w_ref[1], preferred_element_type=F32)
    part_ref[4:5, :] = jnp.dot(silu, mod_w_ref[2], preferred_element_type=F32)[0:1]
    pl.semaphore_wait(barrier, 13)
    phase_x = [
        remote(part_ref, xbuf.at[n], mod_send.at[n], mod_recv.at[n], *peer) for n, peer in enumerate(xs)
    ]
    for copy in phase_x:
        copy.start()
    for load in loads[5:7]:
        load.wait()

    def norms(src_ref, base):
        def step(i, carry):
            for j in range(4):
                x = src_ref[pl.ds(i * 64 + j * 16, 16), :].astype(F32)
                inv = lax.rsqrt(jnp.mean(x * x, axis=-1, keepdims=True) + EPS)
                inv_ref[pl.ds(base + i * 64 + j * 16, 16), :] = jnp.broadcast_to(inv, (16, TILE))
            return carry

        return step

    lax.fori_loop(0, n_lat // 64, norms(lat_ref, 0), 0)
    lax.fori_loop(0, n_ctx // 64, norms(ctx_ref, n_lat), 0)
    for copy in phase_x:
        copy.wait()
    sum_ref[...] = part_ref[...] + xbuf[0] + xbuf[1] + xbuf[2]
    phase_z = [
        remote(sum_ref, zbuf.at[n], mod_send.at[3 + n], mod_recv.at[3 + n], *peer) for n, peer in enumerate(zs)
    ]
    for copy in phase_z:
        copy.start()
    for load in loads[7:]:
        load.wait()
    for copy in phase_z:
        copy.wait()
    whole = sum_ref[...] + zbuf[0] + zbuf[1] + zbuf[2]
    own_ref[...] = whole[0:4]
    gate_row_ref[...] = whole[4:5]
    phase_t = [
        remote(own_ref, tbuf.at[t], mod_send.at[6 + n], mod_recv.at[6 + n], "tp", peer)
        for n, peer in enumerate(targets)
    ]
    for copy in phase_t:
        copy.start()
    tbuf[t] = own_ref[...]
    wide = own_ref.shape[1]

    def piece(n, block):
        cols = pl.ds(pl.multiple_of(block * wide, wide), wide)
        gain = gain_ref[:, cols]
        rows = tbuf[block]
        slot = n % 2
        for src_ref, base, count, s in ((lat_ref, 0, n_lat, 0), (ctx_ref, n_lat, n_ctx, 1)):
            a = gain * (1.0 + rows[2 + s : 3 + s, :])
            b = rows[s : s + 1, :]
            x = src_ref[:, cols].astype(F32)
            inv = inv_ref[base : base + count, :]
            y = [
                x[:, j : j + TILE] * inv * a[:, j : j + TILE] + b[:, j : j + TILE] for j in range(0, wide, TILE)
            ]
            piece_ref[slot, base : base + count, :] = jnp.concatenate(y, axis=1).astype(BF16)
        m = piece_ref[slot]
        acc_ref[0] += jnp.dot(m, w_ref[0, cols, :], preferred_element_type=F32)
        acc_ref[1] += jnp.dot(m, w_ref[1, cols, :], preferred_element_type=F32)
        acc_ref[2, 0:n_lat] += jnp.dot(m[0:n_lat], w_ref[2, cols, :], preferred_element_type=F32)
        pre_acc[0:n_all, 0:64] += mm_nt(m, wg_ref[:, cols])

    piece(0, t)
    for n, block in enumerate(sources):
        phase_t[n].wait_recv()
        piece(n + 1, block)
    k_ref[...] = acc_ref[0].astype(BF16)
    v_ref[...] = acc_ref[1].astype(BF16)
    q_ref[...] = acc_ref[2, 0:n_lat].astype(BF16)
    for j in range(0, n_lat + TILE, TILE):
        rounded = pre_acc[j : j + TILE, :].astype(BF16).astype(F32)
        pre_ref[:, j : j + TILE] = jnp.transpose(rounded)[0:64]
    mix_tokens(
        q_ref, k_ref, v_ref, pre_ref, gate_row_ref, hg_ref, wb_ref, db_ref, lr_ref, lat_ref, ow_ref, out_ref, *scratch
    )
    for copy in phase_t:
        copy.wait_send()


def body(
    latent, context, condition, context_condition, shift_weight, scale_weight, gate_weight, norm_gain,
    query_weight, key_weight, value_weight, write_weight, decay_weight, write_bias, decay_bias, log_rate,
    head_gain, out_weight,
):
    n_lat, d = latent.shape
    n_ctx = context.shape[0]
    n_all = n_lat + n_ctx
    own_cols = gate_weight.shape[1]
    pair = query_weight.shape[1]
    blocks = n_lat // TILE
    tiles = 4 * blocks + 2
    width = n_lat + TILE
    vm = pl.BlockSpec(memory_space=pltpu.VMEM)
    hb = pl.BlockSpec(memory_space=pltpu.HBM)
    gates = [jnp.transpose(w, (1, 2, 0)).reshape(32, -1) for w in (write_weight, decay_weight)]
    shape = jax.ShapeDtypeStruct
    one_map = (TILE, 2 * TILE)
    small = write_bias.shape
    return pl.pallas_call(
        mixer_kernel,
        out_shape=shape((n_lat, own_cols), BF16),
        in_specs=[hb] * 18,
        out_specs=vm,
        scratch_shapes=[
            pltpu.VMEM((n_lat, pair), BF16), pltpu.VMEM((n_all, pair), BF16), pltpu.VMEM((n_all, pair), BF16),
            pltpu.VMEM((64, width), F32), pltpu.VMEM((1, own_cols), F32),
            pltpu.VMEM(condition.shape, BF16), pltpu.VMEM(condition.shape, BF16),
            pltpu.VMEM((3, *shift_weight.shape), BF16), pltpu.VMEM((1, d), F32), pltpu.VMEM((64, d), BF16),
            pltpu.VMEM((n_lat, d), BF16), pltpu.VMEM((n_ctx, d), BF16), pltpu.VMEM((3, d, pair), BF16),
            pltpu.SMEM(small, F32), pltpu.SMEM(small, F32), pltpu.SMEM(small, F32), pltpu.VMEM((1, TILE), F32),
            pltpu.VMEM(out_weight.shape, BF16), pltpu.SemaphoreType.DMA((18,)),
            pltpu.VMEM((n_all, TILE), F32), pltpu.VMEM((2, n_all, own_cols), BF16),
            pltpu.VMEM((3, n_all, pair), F32), pltpu.VMEM((width, TILE), F32),
            pltpu.VMEM((8, own_cols), F32), pltpu.VMEM((8, own_cols), F32),
            pltpu.VMEM((4, own_cols), F32), pltpu.VMEM((3, 8, own_cols), F32), pltpu.VMEM((3, 8, own_cols), F32),
            pltpu.VMEM((8, 4, own_cols), F32), pltpu.SemaphoreType.DMA((13,)), pltpu.SemaphoreType.DMA((13,)),
            pltpu.VMEM((TILE, width), F32), pltpu.VMEM((width, TILE), F32),
            pltpu.VMEM((2, n_lat, n_lat), F32), pltpu.VMEM((2, n_lat, n_lat), F32), pltpu.VMEM((4, n_lat, n_lat), F32),
            pltpu.VMEM((tiles, TILE, TILE), BF16), pltpu.VMEM((tiles, TILE, TILE), BF16),
            pltpu.VMEM((4, n_lat, n_lat), BF16), pltpu.VMEM((4, n_lat, n_lat), BF16),
            pltpu.VMEM((4, n_lat, 2 * TILE), BF16), pltpu.VMEM((4, n_lat, 2 * TILE), BF16),
            pltpu.VMEM((2, n_lat, TILE), F32), pltpu.VMEM((2, n_lat, 2 * TILE), BF16),
            pltpu.VMEM((4, *one_map), BF16), pltpu.VMEM((4, *one_map), BF16),
            pltpu.VMEM((4, *one_map), BF16), pltpu.VMEM((4, *one_map), BF16),
            pltpu.VMEM((4, *one_map), F32), pltpu.VMEM(one_map, BF16), pltpu.VMEM(one_map, BF16),
            pltpu.VMEM((4, *one_map), BF16), pltpu.VMEM((4, *one_map), BF16),
            pltpu.VMEM((4, TILE, TILE), BF16), pltpu.VMEM((4, TILE, TILE), BF16),
            pltpu.VMEM((8, n_lat, pair), BF16),
            pltpu.SemaphoreType.DMA((15,)), pltpu.SemaphoreType.DMA((15,)),
            pltpu.SemaphoreType.DMA((14,)), pltpu.SemaphoreType.DMA((14,)),
        ],
        compiler_params=pltpu.CompilerParams(
            collective_id=0, has_side_effects=True, vmem_limit_bytes=VMEM_LIMIT
        ),
        name="mixer",
    )(
        condition, context_condition, shift_weight, scale_weight, gate_weight, norm_gain.reshape(1, -1), *gates,
        latent, context, query_weight, key_weight, value_weight, write_bias, decay_bias, log_rate,
        head_gain.reshape(1, -1), out_weight,
    )


def solution(mesh):
    torus = Mesh(mesh.devices.reshape(4, 4, mesh.shape["tp"]), ("sp_0", "sp_1", "tp"))
    placed = (
        P(SP, None), P(SP, None), P(SP), P(SP), P(SP, "tp"), P(SP, "tp"), P(SP, "tp"), P(),
        P(None, "tp"), P(None, "tp"), P(None, "tp"), P(), P(), P(), P(), P(), P(), P(None, "tp"),
    )
    return jax.shard_map(body, mesh=torus, in_specs=placed, out_specs=P(SP, "tp"), check_vma=False)
```

```python
import jax
import jax.numpy as jnp
from jax import lax
from jax.experimental import pallas as pl
from jax.experimental.pallas import tpu as pltpu
from jax.sharding import Mesh
from jax.sharding import PartitionSpec as P

HEAD_DIM = 128
SP = ("sp_0", "sp_1")
EPS = 0.0001
F32 = jnp.float32
BF16 = jnp.bfloat16
TILE = 128
VMEM_LIMIT = 63_000_000
MESH = pl.DeviceIdType.MESH
LEVELS = (1, 2, 3, 4, 5, 6)


def mm(a, b):
    return jnp.dot(a.astype(BF16), b.astype(BF16), preferred_element_type=F32)


def mm_nt(a, b):
    return lax.dot_general(a, b, (((1,), (1,)), ((), ())), preferred_element_type=F32)


def mm_tn(a, b):
    return lax.dot_general(a, b, (((0,), (0,)), ((), ())), preferred_element_type=F32)


def iota2(shape, dim):
    return lax.broadcasted_iota(jnp.int32, shape, dim)


def softplus(u):
    return jnp.maximum(u, 0.0) + jnp.log1p(jnp.exp(-jnp.abs(u)))


def inv_norm(rows_bf16):
    r = rows_bf16.astype(F32)
    return lax.rsqrt(jnp.sum(r * r, axis=-1, keepdims=True) + EPS)


def gate_rows(first_head, pre_ref, wb_ref, db_ref, lr_ref, rows_ref, n_lat, n_ctx):
    width = n_lat + TILE
    lane = iota2((8, width), 1)
    is_ctx = lane >= n_lat
    pos = jnp.where(is_ctx, lane - n_lat, lane)
    size = jnp.where(is_ctx, n_ctx, n_lat)
    valid = pos < size
    row = iota2((8, width), 0)
    rates = jnp.zeros((8, width), F32)
    logd = jnp.zeros((8, width), F32)
    for c in range(4):
        d, h = c // 2, c % 2
        head = first_head + h
        at = d * 16 + head
        w = pre_ref[pl.ds(at, 1), :] + wb_ref[d, head]
        u = pre_ref[pl.ds(32 + at, 1), :] + db_ref[d, head]
        rate = 1.0 / (1.0 + jnp.exp(-w))
        step = -jnp.exp(jnp.full((1, width), lr_ref[d, head], F32)) * softplus(u)
        rates = jnp.where(row == c, rate, rates)
        logd = jnp.where(row == c, step, logd)
    rates = jnp.where(valid, rates, 0.0)
    logd = jnp.where(valid, logd, 0.0)
    fwd = logd
    bwd = logd
    s = 1
    while s < n_lat:
        ahead = [jnp.where(pos >= m * s, pltpu.roll(fwd, m * s, 1), 0.0) for m in range(1, 8)]
        after = [jnp.where(pos + m * s < size, pltpu.roll(bwd, width - m * s, 1), 0.0) for m in range(1, 8)]
        fwd = fwd + (((ahead[0] + ahead[1]) + (ahead[2] + ahead[3])) + ((ahead[4] + ahead[5]) + ahead[6]))
        bwd = bwd + (((after[0] + after[1]) + (after[2] + after[3])) + ((after[4] + after[5]) + after[6]))
        s *= 8
    g = jnp.where(row < 2, fwd, bwd)
    g = jnp.where(valid, g, 0.0)
    whole_lat = jnp.sum(jnp.where(is_ctx, 0.0, logd), axis=1, keepdims=True)
    whole_ctx = jnp.sum(jnp.where(is_ctx, logd, 0.0), axis=1, keepdims=True)
    late = jnp.exp(jnp.where(is_ctx, whole_ctx, whole_lat) - g)
    eg = jnp.exp(g)
    parts = []
    for a in (rates, g, late, eg):
        up = pltpu.roll(pltpu.roll(a, n_ctx, 1), 6, 0)
        a = jnp.where(lane >= n_lat + n_ctx, up, a)
        parts.append(a)
    rows_ref[...] = jnp.zeros_like(rows_ref)
    for n, a in enumerate(parts):
        rows_ref[8 * n : 8 * n + 8, :] = a
    return jnp.exp(whole_lat), jnp.exp(whole_ctx)


def split_rows(x):
    hi = x.astype(BF16)
    lo = (x - hi.astype(F32)).astype(BF16)
    return hi, lo


def mul_precise(m_bf16, x):
    hi, lo = split_rows(x)
    n = x.shape[1]
    y = jnp.dot(m_bf16, jnp.concatenate([hi, lo], axis=1), preferred_element_type=F32)
    return y[:, :n] + y[:, n:]


def then(next_map, total):
    y = mm(next_map[:, :TILE], total)
    zero = jnp.zeros((TILE, TILE), F32)
    return y + jnp.concatenate([zero, next_map[:, TILE:].astype(F32)], axis=1)


RATE, G, LATE, EG, KINV = 0, 8, 16, 24, 32


HANDS = (
    "u0", "u1", "u2", "u3", "d0", "d1", "d2", "d3", "mA", "mB", "ru0", "ru1", "rd2", "rd3",
    "mdA", "mdB", "muA", "muB", "ma0", "ma1", "ma2", "ma3",
)


def remote(src, dst, send_sem, recv_sem, axis, peer):
    return pltpu.make_async_remote_copy(
        src_ref=src, dst_ref=dst, send_sem=send_sem, recv_sem=recv_sem, device_id={axis: peer}, device_id_type=MESH
    )


def greet(barrier, peers):
    for axis, peer in peers:
        pl.semaphore_signal(barrier, inc=1, device_id={axis: peer}, device_id_type=MESH)


def ring_peers(axis, size):
    me = lax.axis_index(axis)
    return [(axis, lax.rem(me + k, size)) for k in range(1, size)]


def inverses(ad_ref, t_ref, base, count):
    xor = iota2((TILE, TILE), 0) ^ iota2((TILE, TILE), 1)
    eye = jnp.where(xor == 0, 1.0, 0.0).astype(BF16)
    near = jnp.where(xor == 1, 1.0, 0.0).astype(BF16)
    ts = [eye - ad_ref[base + n] * near for n in range(count)]
    for level in LEVELS:
        keep = jnp.where((xor >> level) == 1, 1.0, 0.0).astype(BF16)
        xs = [mm(ts[n], ad_ref[base + n] * keep).astype(BF16) for n in range(count)]
        ts = [t - mm(x, t).astype(BF16) for x, t in zip(xs, ts)]
    for n in range(count):
        t_ref[base + n] = ts[n]


def mix_tokens(
    q_ref, k_ref, v_ref, pre_ref, gate_row_ref, gain_ref, wb_ref, db_ref, lr_ref, lat_ref, ow_ref,
    out_ref,
    rows_ref, cols_ref, gk_ref, qk_ref, dm_ref, ad_ref, t_ref, ao_ref, p_ref, x_ref, xl_ref, o1_ref, q2_ref,
    lat_map, ctx_map, lat_all, ctx_all, prefix_ref, lat_total, ctx_total, lat_totals, ctx_totals,
    start_ref, mine_ref, ho_ref, acc_out, send_sem, recv_sem, ho_send, ho_recv,
):
    n_lat = q_ref.shape[0]
    n_ctx = k_ref.shape[0] - n_lat
    blocks = n_lat // TILE
    width = n_lat + TILE
    x_at, z_at, t_at = lax.axis_index("sp_1"), lax.axis_index("sp_0"), lax.axis_index("tp")
    y_at, core = t_at // 2, lax.rem(t_at, 2)
    up = lax.rem(y_at + 1, 4) * 2 + core
    down = lax.rem(y_at + 3, 4) * 2 + core
    across = lax.rem(y_at + 2, 4) * 2 + core
    mate = y_at * 2 + 1 - core
    xs, zs = ring_peers("sp_1", 4), ring_peers("sp_0", 4)
    own_cols = out_ref.shape[1]

    dec_lat, dec_ctx = gate_rows(t_at * 2, pre_ref, wb_ref, db_ref, lr_ref, rows_ref, n_lat, n_ctx)
    for b in range(blocks + 1):
        cols_ref[b * TILE : (b + 1) * TILE, :] = jnp.transpose(rows_ref[:, b * TILE : (b + 1) * TILE])

    def kcols(h):
        return k_ref[0:n_lat, h * TILE : (h + 1) * TILE]

    def kctx(h):
        kc = k_ref[n_lat : n_lat + n_ctx, h * TILE : (h + 1) * TILE]
        return jnp.concatenate([kc, kc], axis=0)

    def vctx(h):
        vc = v_ref[n_lat : n_lat + n_ctx, h * TILE : (h + 1) * TILE]
        return jnp.concatenate([vc, vc], axis=0)

    kinv = []
    for h in range(2):
        kinv.append(jnp.concatenate([inv_norm(kcols(h)), inv_norm(kctx(h))], axis=0))
    lane128 = iota2((width, TILE), 1)
    both = jnp.where(lane128 == 0, kinv[0], jnp.where(lane128 == 1, kinv[1], 0.0))
    ii = iota2((TILE, TILE), 0)
    jj = iota2((TILE, TILE), 1)
    xor = ii ^ jj
    for b in range(blocks + 1):
        rows_ref[:, b * TILE : (b + 1) * TILE] = jnp.where(
            ii < KINV,
            rows_ref[:, b * TILE : (b + 1) * TILE],
            pltpu.roll(jnp.transpose(both[b * TILE : (b + 1) * TILE, :]), KINV, 0),
        )

    for h in range(2):
        kc = kctx(h)
        g2 = mm_nt(kc, kc) * kinv[h][n_lat:] * rows_ref[KINV + h : KINV + h + 1, n_lat:]
        keep = jnp.where(ii < n_ctx, jnp.where(jj < ii, 1, 0), jnp.where(jj > ii, 1, 0))
        keep = jnp.where((ii < n_ctx) == (jj < n_ctx), keep, 0) == 1
        sp = cols_ref[n_lat:, G + h : G + h + 1] - rows_ref[G + h : G + h + 1, n_lat:]
        dm = jnp.where(keep, jnp.exp(jnp.where(keep, sp, 0.0)), 0.0)
        ad_ref[4 * blocks + h] = (g2 * dm * cols_ref[n_lat:, RATE + h : RATE + h + 1]).astype(BF16)
    def to_row(base, maps, everyone):
        copies = [
            remote(maps.at[peer], everyone.at[x_at], send_sem.at[base + n], recv_sem.at[base + n], axis, peer)
            for n, (axis, peer) in enumerate(xs)
        ]
        for copy in copies:
            copy.start()
        everyone[x_at] = maps[x_at]
        return copies

    def to_column(base, total, everyone):
        copies = [
            remote(total, everyone.at[z_at], send_sem.at[base + n], recv_sem.at[base + n], axis, peer)
            for n, (axis, peer) in enumerate(zs)
        ]
        for copy in copies:
            copy.start()
        everyone[z_at] = total[...]
        return copies

    krows = []
    for h in range(2):
        krows.append(jnp.log(rows_ref[KINV + h : KINV + h + 1, 0:n_lat]))
        gk_ref[h] = mm_nt(kcols(h), kcols(h))
    for c in range(4):
        d, h = c // 2, c % 2
        for i in range(blocks):
            ri = cols_ref[i * TILE : (i + 1) * TILE, RATE + c : RATE + c + 1] * kinv[h][i * TILE : (i + 1) * TILE]
            gi = cols_ref[i * TILE : (i + 1) * TILE, G + c : G + c + 1]
            for j in range(blocks):
                if (d == 0 and j > i) or (d == 1 and j < i):
                    continue
                at = (slice(i * TILE, (i + 1) * TILE), slice(j * TILE, (j + 1) * TILE))
                cj = slice(j * TILE, (j + 1) * TILE)
                sp = gi - (rows_ref[G + c : G + c + 1, cj] - krows[h][:, cj])
                if i == j:
                    keep = (ii >= jj) if d == 0 else (ii <= jj)
                    dm = jnp.where(keep, jnp.exp(jnp.where(keep, sp, 0.0)), 0.0)
                else:
                    dm = jnp.exp(sp)
                a = gk_ref[(h, *at)] * dm * ri
                if i == j:
                    ad_ref[c * blocks + i] = jnp.where(ii == jj, 0.0, a).astype(BF16)
                else:
                    ao_ref[(c, *at)] = a.astype(BF16)
                dm_ref[(c, *at)] = dm

    inverses(ad_ref, t_ref, 0, ad_ref.shape[0])
    for h in range(2):
        ci = kinv[h][n_lat:]
        cr = slice(n_lat, n_lat + TILE)
        rate = cols_ref[cr, RATE + h : RATE + h + 1]
        eg = cols_ref[cr, EG + h : EG + h + 1]
        late = cols_ref[cr, LATE + h : LATE + h + 1]
        kc = kctx(h)
        b = jnp.concatenate([vctx(h).astype(F32) * rate, kc.astype(F32) * (rate * eg * ci)], axis=1)
        x = mm(t_ref[4 * blocks + h], b)
        xl = (x * (late * ci)).astype(BF16)
        for d in range(2):
            c = d * 2 + h
            m = mm_tn(kc[0:n_ctx], xl[d * n_ctx : (d + 1) * n_ctx])
            diag = jnp.where(xor == 0, dec_ctx[c : c + 1, :], 0.0)
            ctx_map[c] = jnp.concatenate([diag - m[:, TILE:], m[:, :TILE]], axis=1).astype(BF16)

    ctx_rows = to_row(0, ctx_map, ctx_all)

    backwards = x_at >= 2

    def place(n, size):
        return jnp.where(backwards, size - 1 - n, n)

    lates, fronts, sides = {}, {}, {}
    for n in range(blocks):
        for c in range(4):
            d, h = c // 2, c % 2
            i = n if d == 0 else blocks - 1 - n
            r = slice(i * TILE, (i + 1) * TILE)
            rate = cols_ref[r, RATE + c : RATE + c + 1]
            ki = kinv[h][r]
            vi = v_ref[r, h * TILE : (h + 1) * TILE].astype(F32) * rate
            wi = k_ref[r, h * TILE : (h + 1) * TILE].astype(F32) * (rate * cols_ref[r, EG + c : EG + c + 1] * ki)
            lates[c, n] = cols_ref[r, LATE + c : LATE + c + 1] * ki
            t = t_ref[c * blocks + i]
            fronts[c, n] = mm(t, jnp.concatenate([vi, wi], axis=1))
            if n > 0:
                done = slice(0, i * TILE) if d == 0 else slice((i + 1) * TILE, n_lat)
                sides[c, n] = mm(t, ao_ref[c, r, done]).astype(BF16)
    for n in range(blocks):
        for c in range(4):
            d = c // 2
            i = n if d == 0 else blocks - 1 - n
            r = slice(i * TILE, (i + 1) * TILE)
            x = fronts[c, n]
            if n > 0:
                done = slice(0, i * TILE) if d == 0 else slice((i + 1) * TILE, n_lat)
                x = x - mm(sides[c, n], x_ref[c, done, :])
            x_ref[c, r, :] = x.astype(BF16)
            xl_ref[c, r, :] = (x * lates[c, n]).astype(BF16)
    for c in range(4):
        m = mm_tn(kcols(c % 2), xl_ref[c])
        diag = jnp.where(xor == 0, dec_lat[c : c + 1, :], 0.0)
        lat_map[c] = jnp.concatenate([diag - m[:, TILE:], m[:, :TILE]], axis=1).astype(BF16)
    lat_rows = to_row(6, lat_map, lat_all)

    for copy in ctx_rows:
        copy.wait()
    total = ctx_all[place(0, 4)].astype(F32)
    for n in range(1, 4):
        total = then(ctx_all[place(n, 4)], total)
    ctx_total[...] = total.astype(BF16)
    ctx_columns = to_column(3, ctx_total, ctx_totals)

    qinvs = []
    for h in range(2):
        qh = q_ref[0:n_lat, h * TILE : (h + 1) * TILE]
        qinv = inv_norm(qh) * (HEAD_DIM**-0.5)
        qinvs.append(qinv)
        qk_ref[h] = mm_nt(qh, kcols(h)) * qinv
    for c in range(4):
        d, h = c // 2, c % 2
        for i in range(blocks):
            r = slice(i * TILE, (i + 1) * TILE)
            seen = slice(0, (i + 1) * TILE) if d == 0 else slice(i * TILE, n_lat)
            p_ref[c, r, seen] = (qk_ref[h, r, seen] * dm_ref[c, r, seen]).astype(BF16)
    for h in range(2):
        o1 = []
        for d in range(2):
            c = d * 2 + h
            for i in range(blocks):
                r = slice(i * TILE, (i + 1) * TILE)
                seen = slice(0, (i + 1) * TILE) if d == 0 else slice(i * TILE, n_lat)
                ow = mm(p_ref[c, r, seen], x_ref[c, seen, :])
                qi = q_ref[r, h * TILE : (h + 1) * TILE].astype(F32)
                early = qi * (cols_ref[r, EG + c : EG + c + 1] * qinvs[h][r])
                q2_ref[h, r, d * TILE : (d + 1) * TILE] = (early - ow[:, TILE:]).astype(BF16)
                if d == 0:
                    o1.append(ow[:, :TILE])
                else:
                    o1_ref[h, r, :] = o1[i] + ow[:, :TILE]

    for copy in lat_rows:
        copy.wait()
    low = lat_all[place(0, 4)].astype(F32)
    pair = then(lat_all[place(1, 4)], low)
    lat_total[...] = then(then(lat_all[place(3, 4)], lat_all[place(2, 4)].astype(F32)), pair).astype(BF16)
    lat_columns = to_column(9, lat_total, lat_totals)
    prefix_ref[place(1, 4)] = low
    prefix_ref[place(2, 4)] = pair
    prefix_ref[place(3, 4)] = then(lat_all[place(2, 4)], pair)
    for copy in ctx_columns:
        copy.wait()
    state = None
    for n in range(4):
        one = ctx_totals[place(n, 4)]
        off = one[:, TILE:].astype(F32)
        state = off if n == 0 else mul_precise(one[:, :TILE], state) + off
    for copy in lat_columns:
        copy.wait()
    z_place = place(z_at, 4)
    for n in range(3):
        one = lat_totals[place(n, 4)]
        new = mul_precise(one[:, :TILE], state) + one[:, TILE:].astype(F32)
        state = jnp.where(n < z_place, new, state)
    start_ref[place(0, 4)] = state.astype(BF16)
    for n in range(1, 4):
        at = place(n, 4)
        mk = prefix_ref[at]
        start_ref[at] = (mul_precise(mk[:, :TILE].astype(BF16), state) + mk[:, TILE:]).astype(BF16)
    starts = to_row(12, start_ref, mine_ref)
    for copy in starts:
        copy.wait()

    quarter = n_lat // 4
    Q = [slice(n * quarter, (n + 1) * quarter) for n in range(4)]
    A, B = slice(0, n_lat // 2), slice(n_lat // 2, n_lat)
    both_s = [jnp.concatenate([mine_ref[h], mine_ref[2 + h]], axis=0) for h in range(2)]

    def finish(r):
        for h in range(2):
            y = o1_ref[h, r, :] + jnp.dot(q2_ref[h, r, :], both_s[h], preferred_element_type=F32)
            y = y * lax.rsqrt(jnp.mean(y * y, axis=-1, keepdims=True) + EPS) * gain_ref[...]
            ho_ref[t_at, r, h * TILE : (h + 1) * TILE] = y.astype(BF16)

    def other(block):
        return block + 1 - 2 * core

    hands = {}

    def hand(name, block, r, peer):
        n = HANDS.index(name)
        hands[name] = remote(ho_ref.at[block, r], ho_ref.at[block, r], ho_send.at[n], ho_recv.at[n], "tp", peer)
        hands[name].start()

    def got(*names):
        for name in names:
            hands[name].wait_recv()

    depth = 2 * TILE

    def add(block, r=slice(None)):
        w = ow_ref[pl.ds(pl.multiple_of(block * depth, depth), depth), :]
        return jnp.dot(ho_ref[block, r], w, preferred_element_type=F32)

    finish(Q[0])
    hand("u0", t_at, Q[0], up)
    finish(Q[3])
    hand("d3", t_at, Q[3], down)
    finish(Q[1])
    hand("u1", t_at, Q[1], up)
    hand("mA", t_at, A, mate)
    finish(Q[2])
    hand("d2", t_at, Q[2], down)
    hand("u2", t_at, Q[2], up)
    hand("u3", t_at, Q[3], up)
    hand("d1", t_at, Q[1], down)
    hand("d0", t_at, Q[0], down)
    hand("mB", t_at, B, mate)
    acc_out[...] = add(t_at)
    got("mA", "mB")
    acc_out[...] += add(mate)
    got("u0")
    hand("ru0", down, Q[0], up)
    got("d3")
    hand("rd3", up, Q[3], down)
    got("u1")
    hand("ru1", down, Q[1], up)
    hand("mdA", down, A, mate)
    got("d2")
    hand("rd2", up, Q[2], down)
    hand("muB", up, B, mate)
    got("u2", "u3")
    hand("mdB", down, B, mate)
    got("d1", "d0")
    hand("muA", up, A, mate)
    acc_out[...] += add(down) + add(up)
    got("ru0")
    hand("ma0", across, Q[0], mate)
    got("rd3")
    hand("ma3", across, Q[3], mate)
    got("mdA", "mdB", "muA", "muB")
    acc_out[...] += add(other(down)) + add(other(up))
    got("ru1")
    hand("ma1", across, Q[1], mate)
    got("rd2")
    hand("ma2", across, Q[2], mate)
    acc_out[...] += add(across)
    gate = gate_row_ref[...]
    own = pl.ds(pl.multiple_of(t_at * own_cols, own_cols), own_cols)
    got("ma0", "ma3", "ma1", "ma2")
    total = acc_out[...] + add(other(across))
    out_ref[...] = (lat_ref[:, own].astype(F32) + gate * total).astype(BF16)
    for name in HANDS:
        hands[name].wait_send()


def mixer_kernel(
    cond_hbm, cctx_hbm, shift_hbm, scale_hbm, gate_hbm, gain_hbm, ww_hbm, wd_hbm,
    lat_hbm, ctx_hbm, wq_hbm, wk_hbm, wv_hbm, wb_hbm, db_hbm, lr_hbm, hg_hbm, ow_hbm,
    out_ref,
    q_ref, k_ref, v_ref, pre_ref, gate_row_ref,
    cond_ref, cctx_ref, mod_w_ref, gain_ref, wg_ref, lat_ref, ctx_ref, w_ref, wb_ref, db_ref, lr_ref, hg_ref, ow_ref,
    load_sem, inv_ref, piece_ref, acc_ref, pre_acc,
    part_ref, sum_ref, own_ref, xbuf, zbuf, tbuf, mod_send, mod_recv, *scratch,
):
    barrier = pltpu.get_barrier_semaphore()
    t = lax.axis_index("tp")
    y_at, core = t // 2, lax.rem(t, 2)
    up = lax.rem(y_at + 1, 4) * 2 + core
    down = lax.rem(y_at + 3, 4) * 2 + core
    across = lax.rem(y_at + 2, 4) * 2 + core

    def other(block):
        return block + 1 - 2 * core

    targets = [other(t), up, down, other(up), other(down), across, other(across)]
    sources = [other(t), down, up, other(down), other(up), across, other(across)]
    xs, zs = ring_peers("sp_1", 4), ring_peers("sp_0", 4)
    greet(barrier, xs + zs + [("tp", peer) for peer in targets])
    loads = [
        pltpu.make_async_copy(src, dst, load_sem.at[n])
        for n, (src, dst) in enumerate(
            (
                (cond_hbm, cond_ref), (cctx_hbm, cctx_ref), (shift_hbm, mod_w_ref.at[0]), (scale_hbm, mod_w_ref.at[1]),
                (gate_hbm, mod_w_ref.at[2]), (lat_hbm, lat_ref), (ctx_hbm, ctx_ref), (gain_hbm, gain_ref),
                (ww_hbm, wg_ref.at[0:32]), (wd_hbm, wg_ref.at[32:64]),
                (wk_hbm, w_ref.at[0]), (wv_hbm, w_ref.at[1]), (wq_hbm, w_ref.at[2]),
                (wb_hbm, wb_ref), (db_hbm, db_ref), (lr_hbm, lr_ref), (hg_hbm, hg_ref), (ow_hbm, ow_ref),
            )
        )
    ]
    for load in loads[:5]:
        load.start()
    n_lat, n_ctx = lat_ref.shape[0], ctx_ref.shape[0]
    n_all = n_lat + n_ctx
    acc_ref[...] = jnp.zeros_like(acc_ref)
    pre_acc[...] = jnp.zeros_like(pre_acc)
    part_ref[...] = jnp.zeros_like(part_ref)
    for load in loads[:5]:
        load.wait()
    for load in loads[5:7]:
        load.start()
    u = jnp.concatenate(
        [cond_ref[...].astype(F32).reshape(1, -1), cctx_ref[...].astype(F32).reshape(1, -1)], axis=0
    )
    silu = (u / (1.0 + jnp.exp(-u))).astype(BF16)
    part_ref[0:2, :] = jnp.dot(silu, mod_w_ref[0], preferred_element_type=F32)
    part_ref[2:4, :] = jnp.dot(silu, mod_w_ref[1], preferred_element_type=F32)
    part_ref[4:5, :] = jnp.dot(silu, mod_w_ref[2], preferred_element_type=F32)[0:1]
    pl.semaphore_wait(barrier, 13)
    phase_x = [
        remote(part_ref, xbuf.at[n], mod_send.at[n], mod_recv.at[n], *peer) for n, peer in enumerate(xs)
    ]
    for copy in phase_x:
        copy.start()
    for load in loads[5:7]:
        load.wait()
    for load in loads[7:]:
        load.start()

    def norms(src_ref, base):
        def step(i, carry):
            for j in range(4):
                x = src_ref[pl.ds(i * 64 + j * 16, 16), :].astype(F32)
                inv = lax.rsqrt(jnp.mean(x * x, axis=-1, keepdims=True) + EPS)
                inv_ref[pl.ds(base + i * 64 + j * 16, 16), :] = jnp.broadcast_to(inv, (16, TILE))
            return carry

        return step

    lax.fori_loop(0, n_lat // 64, norms(lat_ref, 0), 0)
    lax.fori_loop(0, n_ctx // 64, norms(ctx_ref, n_lat), 0)
    for copy in phase_x:
        copy.wait()
    sum_ref[...] = part_ref[...] + xbuf[0] + xbuf[1] + xbuf[2]
    phase_z = [
        remote(sum_ref, zbuf.at[n], mod_send.at[3 + n], mod_recv.at[3 + n], *peer) for n, peer in enumerate(zs)
    ]
    for copy in phase_z:
        copy.start()
    for load in loads[7:]:
        load.wait()
    for copy in phase_z:
        copy.wait()
    whole = sum_ref[...] + zbuf[0] + zbuf[1] + zbuf[2]
    own_ref[...] = whole[0:4]
    gate_row_ref[...] = whole[4:5]
    phase_t = [
        remote(own_ref, tbuf.at[t], mod_send.at[6 + n], mod_recv.at[6 + n], "tp", peer)
        for n, peer in enumerate(targets)
    ]
    for copy in phase_t:
        copy.start()
    tbuf[t] = own_ref[...]
    wide = own_ref.shape[1]

    def piece(n, block):
        cols = pl.ds(pl.multiple_of(block * wide, wide), wide)
        gain = gain_ref[:, cols]
        rows = tbuf[block]
        slot = n % 2
        for src_ref, base, count, s in ((lat_ref, 0, n_lat, 0), (ctx_ref, n_lat, n_ctx, 1)):
            a = gain * (1.0 + rows[2 + s : 3 + s, :])
            b = rows[s : s + 1, :]
            x = src_ref[:, cols].astype(F32)
            inv = inv_ref[base : base + count, :]
            y = [
                x[:, j : j + TILE] * inv * a[:, j : j + TILE] + b[:, j : j + TILE] for j in range(0, wide, TILE)
            ]
            piece_ref[slot, base : base + count, :] = jnp.concatenate(y, axis=1).astype(BF16)
        m = piece_ref[slot]
        acc_ref[0] += jnp.dot(m, w_ref[0, cols, :], preferred_element_type=F32)
        acc_ref[1] += jnp.dot(m, w_ref[1, cols, :], preferred_element_type=F32)
        acc_ref[2, 0:n_lat] += jnp.dot(m[0:n_lat], w_ref[2, cols, :], preferred_element_type=F32)
        pre_acc[0:n_all, 0:64] += mm_nt(m, wg_ref[:, cols])

    piece(0, t)
    for n, block in enumerate(sources):
        phase_t[n].wait_recv()
        piece(n + 1, block)
    k_ref[...] = acc_ref[0].astype(BF16)
    v_ref[...] = acc_ref[1].astype(BF16)
    q_ref[...] = acc_ref[2, 0:n_lat].astype(BF16)
    for j in range(0, n_lat + TILE, TILE):
        rounded = pre_acc[j : j + TILE, :].astype(BF16).astype(F32)
        pre_ref[:, j : j + TILE] = jnp.transpose(rounded)[0:64]
    mix_tokens(
        q_ref, k_ref, v_ref, pre_ref, gate_row_ref, hg_ref, wb_ref, db_ref, lr_ref, lat_ref, ow_ref, out_ref, *scratch
    )
    for copy in phase_t:
        copy.wait_send()


def body(
    latent, context, condition, context_condition, shift_weight, scale_weight, gate_weight, norm_gain,
    query_weight, key_weight, value_weight, write_weight, decay_weight, write_bias, decay_bias, log_rate,
    head_gain, out_weight,
):
    n_lat, d = latent.shape
    n_ctx = context.shape[0]
    n_all = n_lat + n_ctx
    own_cols = gate_weight.shape[1]
    pair = query_weight.shape[1]
    blocks = n_lat // TILE
    tiles = 4 * blocks + 2
    width = n_lat + TILE
    vm = pl.BlockSpec(memory_space=pltpu.VMEM)
    hb = pl.BlockSpec(memory_space=pltpu.HBM)
    gates = [jnp.transpose(w, (1, 2, 0)).reshape(32, -1) for w in (write_weight, decay_weight)]
    shape = jax.ShapeDtypeStruct
    one_map = (TILE, 2 * TILE)
    small = write_bias.shape
    return pl.pallas_call(
        mixer_kernel,
        out_shape=pltpu.VMEM((n_lat, own_cols), BF16),
        in_specs=[hb] * 18,
        out_specs=vm,
        scratch_shapes=[
            pltpu.VMEM((n_lat, pair), BF16), pltpu.VMEM((n_all, pair), BF16), pltpu.VMEM((n_all, pair), BF16),
            pltpu.VMEM((64, width), F32), pltpu.VMEM((1, own_cols), F32),
            pltpu.VMEM(condition.shape, BF16), pltpu.VMEM(condition.shape, BF16),
            pltpu.VMEM((3, *shift_weight.shape), BF16), pltpu.VMEM((1, d), F32), pltpu.VMEM((64, d), BF16),
            pltpu.VMEM((n_lat, d), BF16), pltpu.VMEM((n_ctx, d), BF16), pltpu.VMEM((3, d, pair), BF16),
            pltpu.SMEM(small, F32), pltpu.SMEM(small, F32), pltpu.SMEM(small, F32), pltpu.VMEM((1, TILE), F32),
            pltpu.VMEM(out_weight.shape, BF16), pltpu.SemaphoreType.DMA((18,)),
            pltpu.VMEM((n_all, TILE), F32), pltpu.VMEM((2, n_all, own_cols), BF16),
            pltpu.VMEM((3, n_all, pair), F32), pltpu.VMEM((width, TILE), F32),
            pltpu.VMEM((8, own_cols), F32), pltpu.VMEM((8, own_cols), F32),
            pltpu.VMEM((4, own_cols), F32), pltpu.VMEM((3, 8, own_cols), F32), pltpu.VMEM((3, 8, own_cols), F32),
            pltpu.VMEM((8, 4, own_cols), F32), pltpu.SemaphoreType.DMA((13,)), pltpu.SemaphoreType.DMA((13,)),
            pltpu.VMEM((TILE, width), F32), pltpu.VMEM((width, TILE), F32),
            pltpu.VMEM((2, n_lat, n_lat), F32), pltpu.VMEM((2, n_lat, n_lat), F32), pltpu.VMEM((4, n_lat, n_lat), F32),
            pltpu.VMEM((tiles, TILE, TILE), BF16), pltpu.VMEM((tiles, TILE, TILE), BF16),
            pltpu.VMEM((4, n_lat, n_lat), BF16), pltpu.VMEM((4, n_lat, n_lat), BF16),
            pltpu.VMEM((4, n_lat, 2 * TILE), BF16), pltpu.VMEM((4, n_lat, 2 * TILE), BF16),
            pltpu.VMEM((2, n_lat, TILE), F32), pltpu.VMEM((2, n_lat, 2 * TILE), BF16),
            pltpu.VMEM((4, *one_map), BF16), pltpu.VMEM((4, *one_map), BF16),
            pltpu.VMEM((4, *one_map), BF16), pltpu.VMEM((4, *one_map), BF16),
            pltpu.VMEM((4, *one_map), F32), pltpu.VMEM(one_map, BF16), pltpu.VMEM(one_map, BF16),
            pltpu.VMEM((4, *one_map), BF16), pltpu.VMEM((4, *one_map), BF16),
            pltpu.VMEM((4, TILE, TILE), BF16), pltpu.VMEM((4, TILE, TILE), BF16),
            pltpu.VMEM((8, n_lat, pair), BF16), pltpu.VMEM((n_lat, own_cols), F32),
            pltpu.SemaphoreType.DMA((15,)), pltpu.SemaphoreType.DMA((15,)),
            pltpu.SemaphoreType.DMA((len(HANDS),)), pltpu.SemaphoreType.DMA((len(HANDS),)),
        ],
        compiler_params=pltpu.CompilerParams(
            collective_id=0, has_side_effects=True, vmem_limit_bytes=VMEM_LIMIT
        ),
        name="mixer",
    )(
        condition, context_condition, shift_weight, scale_weight, gate_weight, norm_gain.reshape(1, -1), *gates,
        latent, context, query_weight, key_weight, value_weight, write_bias, decay_bias, log_rate,
        head_gain.reshape(1, -1), out_weight,
    )


def solution(mesh):
    torus = Mesh(mesh.devices.reshape(4, 4, mesh.shape["tp"]), ("sp_0", "sp_1", "tp"))
    placed = (
        P(SP, None), P(SP, None), P(SP), P(SP), P(SP, "tp"), P(SP, "tp"), P(SP, "tp"), P(),
        P(None, "tp"), P(None, "tp"), P(None, "tp"), P(), P(), P(), P(), P(), P(), P(None, "tp"),
    )
    return jax.shard_map(body, mesh=torus, in_specs=placed, out_specs=P(SP, "tp"), check_vma=False)
```

```python
import jax
import jax.numpy as jnp
from jax import lax
from jax.experimental import pallas as pl
from jax.experimental.pallas import tpu as pltpu
from jax.sharding import Mesh
from jax.sharding import PartitionSpec as P

HEAD_DIM = 128
SP = ("sp_0", "sp_1")
EPS = 0.0001
F32 = jnp.float32
BF16 = jnp.bfloat16
TILE = 128
VMEM_LIMIT = 63_000_000
MESH = pl.DeviceIdType.MESH
LEVELS = (1, 2, 3, 4, 5, 6)


def mm(a, b):
    return jnp.dot(a.astype(BF16), b.astype(BF16), preferred_element_type=F32)


def mm_nt(a, b):
    return lax.dot_general(a, b, (((1,), (1,)), ((), ())), preferred_element_type=F32)


def mm_tn(a, b):
    return lax.dot_general(a, b, (((0,), (0,)), ((), ())), preferred_element_type=F32)


def iota2(shape, dim):
    return lax.broadcasted_iota(jnp.int32, shape, dim)


def softplus(u):
    return jnp.maximum(u, 0.0) + jnp.log1p(jnp.exp(-jnp.abs(u)))


def inv_norm(rows_bf16):
    r = rows_bf16.astype(F32)
    return lax.rsqrt(jnp.sum(r * r, axis=-1, keepdims=True) + EPS)


def gate_rows(first_head, pre_ref, wb_ref, db_ref, lr_ref, rows_ref, n_lat, n_ctx):
    width = n_lat + TILE
    lane = iota2((8, width), 1)
    is_ctx = lane >= n_lat
    pos = jnp.where(is_ctx, lane - n_lat, lane)
    size = jnp.where(is_ctx, n_ctx, n_lat)
    valid = pos < size
    row = iota2((8, width), 0)
    rates = jnp.zeros((8, width), F32)
    logd = jnp.zeros((8, width), F32)
    for c in range(4):
        d, h = c // 2, c % 2
        head = first_head + h
        at = d * 16 + head
        w = pre_ref[pl.ds(at, 1), :] + wb_ref[d, head]
        u = pre_ref[pl.ds(32 + at, 1), :] + db_ref[d, head]
        rate = 1.0 / (1.0 + jnp.exp(-w))
        step = -jnp.exp(jnp.full((1, width), lr_ref[d, head], F32)) * softplus(u)
        rates = jnp.where(row == c, rate, rates)
        logd = jnp.where(row == c, step, logd)
    rates = jnp.where(valid, rates, 0.0)
    logd = jnp.where(valid, logd, 0.0)
    fwd = logd
    bwd = logd
    s = 1
    while s < n_lat:
        ahead = [jnp.where(pos >= m * s, pltpu.roll(fwd, m * s, 1), 0.0) for m in range(1, 8)]
        after = [jnp.where(pos + m * s < size, pltpu.roll(bwd, width - m * s, 1), 0.0) for m in range(1, 8)]
        fwd = fwd + (((ahead[0] + ahead[1]) + (ahead[2] + ahead[3])) + ((ahead[4] + ahead[5]) + ahead[6]))
        bwd = bwd + (((after[0] + after[1]) + (after[2] + after[3])) + ((after[4] + after[5]) + after[6]))
        s *= 8
    g = jnp.where(row < 2, fwd, bwd)
    g = jnp.where(valid, g, 0.0)
    whole_lat = jnp.sum(jnp.where(is_ctx, 0.0, logd), axis=1, keepdims=True)
    whole_ctx = jnp.sum(jnp.where(is_ctx, logd, 0.0), axis=1, keepdims=True)
    late = jnp.exp(jnp.where(is_ctx, whole_ctx, whole_lat) - g)
    eg = jnp.exp(g)
    parts = []
    for a in (rates, g, late, eg):
        up = pltpu.roll(pltpu.roll(a, n_ctx, 1), 6, 0)
        a = jnp.where(lane >= n_lat + n_ctx, up, a)
        parts.append(a)
    rows_ref[...] = jnp.zeros_like(rows_ref)
    for n, a in enumerate(parts):
        rows_ref[8 * n : 8 * n + 8, :] = a
    return jnp.exp(whole_lat), jnp.exp(whole_ctx)


def split_rows(x):
    hi = x.astype(BF16)
    lo = (x - hi.astype(F32)).astype(BF16)
    return hi, lo


def mul_precise(m_bf16, x):
    hi, lo = split_rows(x)
    n = x.shape[1]
    y = jnp.dot(m_bf16, jnp.concatenate([hi, lo], axis=1), preferred_element_type=F32)
    return y[:, :n] + y[:, n:]


def then(next_map, total):
    y = mm(next_map[:, :TILE], total)
    zero = jnp.zeros((TILE, TILE), F32)
    return y + jnp.concatenate([zero, next_map[:, TILE:].astype(F32)], axis=1)


RATE, G, LATE, EG, KINV = 0, 8, 16, 24, 32


HANDS = (
    "u0", "u1", "u2", "u3", "d0", "d1", "d2", "d3", "mA", "mB", "ru0", "ru1", "rd2", "rd3",
    "mdA", "mdB", "muA", "muB", "ma0", "ma1", "ma2", "ma3",
)


def remote(src, dst, send_sem, recv_sem, axis, peer):
    return pltpu.make_async_remote_copy(
        src_ref=src, dst_ref=dst, send_sem=send_sem, recv_sem=recv_sem, device_id={axis: peer}, device_id_type=MESH
    )


def greet(barrier, peers):
    for axis, peer in peers:
        pl.semaphore_signal(barrier, inc=1, device_id={axis: peer}, device_id_type=MESH)


def ring_peers(axis, size):
    me = lax.axis_index(axis)
    return [(axis, lax.rem(me + k, size)) for k in range(1, size)]


def inverses(ad_ref, t_ref, base, count):
    xor = iota2((TILE, TILE), 0) ^ iota2((TILE, TILE), 1)
    eye = jnp.where(xor == 0, 1.0, 0.0).astype(BF16)
    near = jnp.where(xor == 1, 1.0, 0.0).astype(BF16)
    ts = [eye - ad_ref[base + n] * near for n in range(count)]
    for level in LEVELS:
        keep = jnp.where((xor >> level) == 1, 1.0, 0.0).astype(BF16)
        xs = [mm(ts[n], ad_ref[base + n] * keep).astype(BF16) for n in range(count)]
        ts = [t - mm(x, t).astype(BF16) for x, t in zip(xs, ts)]
    for n in range(count):
        t_ref[base + n] = ts[n]


def mix_tokens(
    q_ref, k_ref, v_ref, pre_ref, gate_row_ref, gain_ref, wb_ref, db_ref, lr_ref, lat_ref, ow_ref,
    out_ref,
    rows_ref, cols_ref, gk_ref, qk_ref, dm_ref, ad_ref, t_ref, ao_ref, p_ref, x_ref, xl_ref, o1_ref, q2_ref,
    lat_map, ctx_map, lat_all, ctx_all, prefix_ref, lat_total, ctx_total, lat_totals, ctx_totals,
    start_ref, mine_ref, ho_ref, acc_out, send_sem, recv_sem, ho_send, ho_recv,
):
    n_lat = q_ref.shape[0]
    n_ctx = k_ref.shape[0] - n_lat
    blocks = n_lat // TILE
    width = n_lat + TILE
    x_at, z_at, t_at = lax.axis_index("sp_1"), lax.axis_index("sp_0"), lax.axis_index("tp")
    y_at, core = t_at // 2, lax.rem(t_at, 2)
    up = lax.rem(y_at + 1, 4) * 2 + core
    down = lax.rem(y_at + 3, 4) * 2 + core
    across = lax.rem(y_at + 2, 4) * 2 + core
    mate = y_at * 2 + 1 - core
    xs, zs = ring_peers("sp_1", 4), ring_peers("sp_0", 4)
    own_cols = out_ref.shape[1]

    dec_lat, dec_ctx = gate_rows(t_at * 2, pre_ref, wb_ref, db_ref, lr_ref, rows_ref, n_lat, n_ctx)
    for b in range(blocks + 1):
        cols_ref[b * TILE : (b + 1) * TILE, :] = jnp.transpose(rows_ref[:, b * TILE : (b + 1) * TILE])

    def kcols(h):
        return k_ref[0:n_lat, h * TILE : (h + 1) * TILE]

    def kctx(h):
        kc = k_ref[n_lat : n_lat + n_ctx, h * TILE : (h + 1) * TILE]
        return jnp.concatenate([kc, kc], axis=0)

    def vctx(h):
        vc = v_ref[n_lat : n_lat + n_ctx, h * TILE : (h + 1) * TILE]
        return jnp.concatenate([vc, vc], axis=0)

    kinv = []
    for h in range(2):
        kinv.append(jnp.concatenate([inv_norm(kcols(h)), inv_norm(kctx(h))], axis=0))
    lane128 = iota2((width, TILE), 1)
    both = jnp.where(lane128 == 0, kinv[0], jnp.where(lane128 == 1, kinv[1], 0.0))
    ii = iota2((TILE, TILE), 0)
    jj = iota2((TILE, TILE), 1)
    xor = ii ^ jj
    for b in range(blocks + 1):
        rows_ref[:, b * TILE : (b + 1) * TILE] = jnp.where(
            ii < KINV,
            rows_ref[:, b * TILE : (b + 1) * TILE],
            pltpu.roll(jnp.transpose(both[b * TILE : (b + 1) * TILE, :]), KINV, 0),
        )

    for h in range(2):
        kc = kctx(h)
        g2 = mm_nt(kc, kc) * kinv[h][n_lat:] * rows_ref[KINV + h : KINV + h + 1, n_lat:]
        keep = jnp.where(ii < n_ctx, jnp.where(jj < ii, 1, 0), jnp.where(jj > ii, 1, 0))
        keep = jnp.where((ii < n_ctx) == (jj < n_ctx), keep, 0) == 1
        sp = cols_ref[n_lat:, G + h : G + h + 1] - rows_ref[G + h : G + h + 1, n_lat:]
        dm = jnp.where(keep, jnp.exp(jnp.where(keep, sp, 0.0)), 0.0)
        ad_ref[4 * blocks + h] = (g2 * dm * cols_ref[n_lat:, RATE + h : RATE + h + 1]).astype(BF16)
    def to_row(base, maps, everyone):
        copies = [
            remote(maps.at[peer], everyone.at[x_at], send_sem.at[base + n], recv_sem.at[base + n], axis, peer)
            for n, (axis, peer) in enumerate(xs)
        ]
        for copy in copies:
            copy.start()
        everyone[x_at] = maps[x_at]
        return copies

    def to_column(base, total, everyone):
        copies = [
            remote(total, everyone.at[z_at], send_sem.at[base + n], recv_sem.at[base + n], axis, peer)
            for n, (axis, peer) in enumerate(zs)
        ]
        for copy in copies:
            copy.start()
        everyone[z_at] = total[...]
        return copies

    krows = []
    for h in range(2):
        krows.append(jnp.log(rows_ref[KINV + h : KINV + h + 1, 0:n_lat]))
        gk_ref[h] = mm_nt(kcols(h), kcols(h))
    for c in range(4):
        d, h = c // 2, c % 2
        for i in range(blocks):
            ri = cols_ref[i * TILE : (i + 1) * TILE, RATE + c : RATE + c + 1] * kinv[h][i * TILE : (i + 1) * TILE]
            gi = cols_ref[i * TILE : (i + 1) * TILE, G + c : G + c + 1]
            for j in range(blocks):
                if (d == 0 and j > i) or (d == 1 and j < i):
                    continue
                at = (slice(i * TILE, (i + 1) * TILE), slice(j * TILE, (j + 1) * TILE))
                cj = slice(j * TILE, (j + 1) * TILE)
                sp = gi - (rows_ref[G + c : G + c + 1, cj] - krows[h][:, cj])
                if i == j:
                    keep = (ii >= jj) if d == 0 else (ii <= jj)
                    dm = jnp.where(keep, jnp.exp(jnp.where(keep, sp, 0.0)), 0.0)
                else:
                    dm = jnp.exp(sp)
                a = gk_ref[(h, *at)] * dm * ri
                if i == j:
                    ad_ref[c * blocks + i] = jnp.where(ii == jj, 0.0, a).astype(BF16)
                else:
                    ao_ref[(c, *at)] = a.astype(BF16)
                dm_ref[(c, *at)] = dm

    inverses(ad_ref, t_ref, 4 * blocks, 2)
    for h in range(2):
        ci = kinv[h][n_lat:]
        cr = slice(n_lat, n_lat + TILE)
        rate = cols_ref[cr, RATE + h : RATE + h + 1]
        eg = cols_ref[cr, EG + h : EG + h + 1]
        late = cols_ref[cr, LATE + h : LATE + h + 1]
        kc = kctx(h)
        b = jnp.concatenate([vctx(h).astype(F32) * rate, kc.astype(F32) * (rate * eg * ci)], axis=1)
        x = mm(t_ref[4 * blocks + h], b)
        xl = (x * (late * ci)).astype(BF16)
        for d in range(2):
            c = d * 2 + h
            m = mm_tn(kc[0:n_ctx], xl[d * n_ctx : (d + 1) * n_ctx])
            diag = jnp.where(xor == 0, dec_ctx[c : c + 1, :], 0.0)
            ctx_map[c] = jnp.concatenate([diag - m[:, TILE:], m[:, :TILE]], axis=1).astype(BF16)

    ctx_rows = to_row(0, ctx_map, ctx_all)

    inverses(ad_ref, t_ref, 0, 4 * blocks)

    backwards = x_at >= 2

    def place(n, size):
        return jnp.where(backwards, size - 1 - n, n)

    lates, fronts, sides = {}, {}, {}
    for n in range(blocks):
        for c in range(4):
            d, h = c // 2, c % 2
            i = n if d == 0 else blocks - 1 - n
            r = slice(i * TILE, (i + 1) * TILE)
            rate = cols_ref[r, RATE + c : RATE + c + 1]
            ki = kinv[h][r]
            vi = v_ref[r, h * TILE : (h + 1) * TILE].astype(F32) * rate
            wi = k_ref[r, h * TILE : (h + 1) * TILE].astype(F32) * (rate * cols_ref[r, EG + c : EG + c + 1] * ki)
            lates[c, n] = cols_ref[r, LATE + c : LATE + c + 1] * ki
            t = t_ref[c * blocks + i]
            fronts[c, n] = mm(t, jnp.concatenate([vi, wi], axis=1))
            if n > 0:
                done = slice(0, i * TILE) if d == 0 else slice((i + 1) * TILE, n_lat)
                sides[c, n] = mm(t, ao_ref[c, r, done]).astype(BF16)
    for n in range(blocks):
        for c in range(4):
            d = c // 2
            i = n if d == 0 else blocks - 1 - n
            r = slice(i * TILE, (i + 1) * TILE)
            x = fronts[c, n]
            if n > 0:
                done = slice(0, i * TILE) if d == 0 else slice((i + 1) * TILE, n_lat)
                x = x - mm(sides[c, n], x_ref[c, done, :])
            x_ref[c, r, :] = x.astype(BF16)
            xl_ref[c, r, :] = (x * lates[c, n]).astype(BF16)
    for c in range(4):
        m = mm_tn(kcols(c % 2), xl_ref[c])
        diag = jnp.where(xor == 0, dec_lat[c : c + 1, :], 0.0)
        lat_map[c] = jnp.concatenate([diag - m[:, TILE:], m[:, :TILE]], axis=1).astype(BF16)
    lat_rows = to_row(6, lat_map, lat_all)

    qinvs = []
    for h in range(2):
        qh = q_ref[0:n_lat, h * TILE : (h + 1) * TILE]
        qinv = inv_norm(qh) * (HEAD_DIM**-0.5)
        qinvs.append(qinv)
        qk_ref[h] = mm_nt(qh, kcols(h)) * qinv
    for c in range(4):
        d, h = c // 2, c % 2
        for i in range(blocks):
            r = slice(i * TILE, (i + 1) * TILE)
            seen = slice(0, (i + 1) * TILE) if d == 0 else slice(i * TILE, n_lat)
            p_ref[c, r, seen] = (qk_ref[h, r, seen] * dm_ref[c, r, seen]).astype(BF16)
    for h in range(2):
        o1 = []
        for d in range(2):
            c = d * 2 + h
            for i in range(blocks):
                r = slice(i * TILE, (i + 1) * TILE)
                seen = slice(0, (i + 1) * TILE) if d == 0 else slice(i * TILE, n_lat)
                ow = mm(p_ref[c, r, seen], x_ref[c, seen, :])
                qi = q_ref[r, h * TILE : (h + 1) * TILE].astype(F32)
                early = qi * (cols_ref[r, EG + c : EG + c + 1] * qinvs[h][r])
                q2_ref[h, r, d * TILE : (d + 1) * TILE] = (early - ow[:, TILE:]).astype(BF16)
                if d == 0:
                    o1.append(ow[:, :TILE])
                else:
                    o1_ref[h, r, :] = o1[i] + ow[:, :TILE]

    for copy in ctx_rows:
        copy.wait()
    total = ctx_all[place(0, 4)].astype(F32)
    for n in range(1, 4):
        total = then(ctx_all[place(n, 4)], total)
    ctx_total[...] = total.astype(BF16)
    ctx_columns = to_column(3, ctx_total, ctx_totals)

    for copy in lat_rows:
        copy.wait()
    low = lat_all[place(0, 4)].astype(F32)
    pair = then(lat_all[place(1, 4)], low)
    lat_total[...] = then(then(lat_all[place(3, 4)], lat_all[place(2, 4)].astype(F32)), pair).astype(BF16)
    lat_columns = to_column(9, lat_total, lat_totals)
    prefix_ref[place(1, 4)] = low
    prefix_ref[place(2, 4)] = pair
    prefix_ref[place(3, 4)] = then(lat_all[place(2, 4)], pair)
    for copy in ctx_columns:
        copy.wait()
    state = None
    for n in range(4):
        one = ctx_totals[place(n, 4)]
        off = one[:, TILE:].astype(F32)
        state = off if n == 0 else mul_precise(one[:, :TILE], state) + off
    for copy in lat_columns:
        copy.wait()
    z_place = place(z_at, 4)
    for n in range(3):
        one = lat_totals[place(n, 4)]
        new = mul_precise(one[:, :TILE], state) + one[:, TILE:].astype(F32)
        state = jnp.where(n < z_place, new, state)
    start_ref[place(0, 4)] = state.astype(BF16)
    for n in range(1, 4):
        at = place(n, 4)
        mk = prefix_ref[at]
        start_ref[at] = (mul_precise(mk[:, :TILE].astype(BF16), state) + mk[:, TILE:]).astype(BF16)
    starts = to_row(12, start_ref, mine_ref)
    for copy in starts:
        copy.wait()

    quarter = n_lat // 4
    Q = [slice(n * quarter, (n + 1) * quarter) for n in range(4)]
    A, B = slice(0, n_lat // 2), slice(n_lat // 2, n_lat)
    both_s = [jnp.concatenate([mine_ref[h], mine_ref[2 + h]], axis=0) for h in range(2)]

    def finish(r):
        for h in range(2):
            y = o1_ref[h, r, :] + jnp.dot(q2_ref[h, r, :], both_s[h], preferred_element_type=F32)
            y = y * lax.rsqrt(jnp.mean(y * y, axis=-1, keepdims=True) + EPS) * gain_ref[...]
            ho_ref[t_at, r, h * TILE : (h + 1) * TILE] = y.astype(BF16)

    def other(block):
        return block + 1 - 2 * core

    hands = {}

    def hand(name, block, r, peer):
        n = HANDS.index(name)
        hands[name] = remote(ho_ref.at[block, r], ho_ref.at[block, r], ho_send.at[n], ho_recv.at[n], "tp", peer)
        hands[name].start()

    def got(*names):
        for name in names:
            hands[name].wait_recv()

    depth = 2 * TILE

    def add(block, r=slice(None)):
        w = ow_ref[pl.ds(pl.multiple_of(block * depth, depth), depth), :]
        return jnp.dot(ho_ref[block, r], w, preferred_element_type=F32)

    finish(Q[0])
    hand("u0", t_at, Q[0], up)
    finish(Q[3])
    hand("d3", t_at, Q[3], down)
    finish(Q[1])
    hand("u1", t_at, Q[1], up)
    hand("mA", t_at, A, mate)
    finish(Q[2])
    hand("d2", t_at, Q[2], down)
    hand("u2", t_at, Q[2], up)
    hand("u3", t_at, Q[3], up)
    hand("d1", t_at, Q[1], down)
    hand("d0", t_at, Q[0], down)
    hand("mB", t_at, B, mate)
    acc_out[...] = add(t_at)
    got("mA", "mB")
    acc_out[...] += add(mate)
    got("u0")
    hand("ru0", down, Q[0], up)
    got("d3")
    hand("rd3", up, Q[3], down)
    got("u1")
    hand("ru1", down, Q[1], up)
    hand("mdA", down, A, mate)
    got("d2")
    hand("rd2", up, Q[2], down)
    hand("muB", up, B, mate)
    got("u2", "u3")
    hand("mdB", down, B, mate)
    got("d1", "d0")
    hand("muA", up, A, mate)
    acc_out[...] += add(down) + add(up)
    got("ru0")
    hand("ma0", across, Q[0], mate)
    got("rd3")
    hand("ma3", across, Q[3], mate)
    got("mdA", "mdB", "muA", "muB")
    acc_out[...] += add(other(down)) + add(other(up))
    got("ru1")
    hand("ma1", across, Q[1], mate)
    got("rd2")
    hand("ma2", across, Q[2], mate)
    acc_out[...] += add(across)
    gate = gate_row_ref[...]
    own = pl.ds(pl.multiple_of(t_at * own_cols, own_cols), own_cols)
    got("ma0", "ma3", "ma1")
    for r in (A, Q[3]):
        total = acc_out[r, :] + add(other(across), r)
        out_ref[r, :] = (lat_ref[r, own].astype(F32) + gate * total).astype(BF16)
    got("ma2")
    total = acc_out[Q[2], :] + add(other(across), Q[2])
    out_ref[Q[2], :] = (lat_ref[Q[2], own].astype(F32) + gate * total).astype(BF16)
    for name in HANDS:
        hands[name].wait_send()


def mixer_kernel(
    cond_hbm, cctx_hbm, shift_hbm, scale_hbm, gate_hbm, gain_hbm, ww_hbm, wd_hbm,
    lat_hbm, ctx_hbm, wq_hbm, wk_hbm, wv_hbm, wb_hbm, db_hbm, lr_hbm, hg_hbm, ow_hbm,
    out_ref,
    q_ref, k_ref, v_ref, pre_ref, gate_row_ref,
    cond_ref, cctx_ref, mod_w_ref, gain_ref, wg_ref, lat_ref, ctx_ref, w_ref, wb_ref, db_ref, lr_ref, hg_ref, ow_ref,
    load_sem, inv_ref, piece_ref, acc_ref, pre_acc,
    part_ref, sum_ref, own_ref, xbuf, zbuf, tbuf, mod_send, mod_recv, *scratch,
):
    barrier = pltpu.get_barrier_semaphore()
    t = lax.axis_index("tp")
    y_at, core = t // 2, lax.rem(t, 2)
    up = lax.rem(y_at + 1, 4) * 2 + core
    down = lax.rem(y_at + 3, 4) * 2 + core
    across = lax.rem(y_at + 2, 4) * 2 + core

    def other(block):
        return block + 1 - 2 * core

    targets = [other(t), up, down, other(up), other(down), across, other(across)]
    sources = [other(t), down, up, other(down), other(up), across, other(across)]
    xs, zs = ring_peers("sp_1", 4), ring_peers("sp_0", 4)
    greet(barrier, xs + zs + [("tp", peer) for peer in targets])
    loads = [
        pltpu.make_async_copy(src, dst, load_sem.at[n])
        for n, (src, dst) in enumerate(
            (
                (cond_hbm, cond_ref), (cctx_hbm, cctx_ref), (shift_hbm, mod_w_ref.at[0]), (scale_hbm, mod_w_ref.at[1]),
                (gate_hbm, mod_w_ref.at[2]), (lat_hbm, lat_ref), (ctx_hbm, ctx_ref), (gain_hbm, gain_ref),
                (ww_hbm, wg_ref.at[0:32]), (wd_hbm, wg_ref.at[32:64]),
                (wk_hbm, w_ref.at[0]), (wv_hbm, w_ref.at[1]), (wq_hbm, w_ref.at[2]),
                (wb_hbm, wb_ref), (db_hbm, db_ref), (lr_hbm, lr_ref), (hg_hbm, hg_ref), (ow_hbm, ow_ref),
            )
        )
    ]
    for load in loads[:5]:
        load.start()
    n_lat, n_ctx = lat_ref.shape[0], ctx_ref.shape[0]
    n_all = n_lat + n_ctx
    acc_ref[...] = jnp.zeros_like(acc_ref)
    pre_acc[...] = jnp.zeros_like(pre_acc)
    part_ref[...] = jnp.zeros_like(part_ref)
    for load in loads[:5]:
        load.wait()
    for load in loads[5:7]:
        load.start()
    u = jnp.concatenate(
        [cond_ref[...].astype(F32).reshape(1, -1), cctx_ref[...].astype(F32).reshape(1, -1)], axis=0
    )
    silu = (u / (1.0 + jnp.exp(-u))).astype(BF16)
    part_ref[0:2, :] = jnp.dot(silu, mod_w_ref[0], preferred_element_type=F32)
    part_ref[2:4, :] = jnp.dot(silu, mod_w_ref[1], preferred_element_type=F32)
    part_ref[4:5, :] = jnp.dot(silu, mod_w_ref[2], preferred_element_type=F32)[0:1]
    pl.semaphore_wait(barrier, 13)
    phase_x = [
        remote(part_ref, xbuf.at[n], mod_send.at[n], mod_recv.at[n], *peer) for n, peer in enumerate(xs)
    ]
    for copy in phase_x:
        copy.start()
    for load in loads[5:7]:
        load.wait()
    for load in loads[7:]:
        load.start()

    def norms(src_ref, base):
        def step(i, carry):
            for j in range(4):
                x = src_ref[pl.ds(i * 64 + j * 16, 16), :].astype(F32)
                inv = lax.rsqrt(jnp.mean(x * x, axis=-1, keepdims=True) + EPS)
                inv_ref[pl.ds(base + i * 64 + j * 16, 16), :] = jnp.broadcast_to(inv, (16, TILE))
            return carry

        return step

    lax.fori_loop(0, n_lat // 64, norms(lat_ref, 0), 0)
    lax.fori_loop(0, n_ctx // 64, norms(ctx_ref, n_lat), 0)
    for copy in phase_x:
        copy.wait()
    sum_ref[...] = part_ref[...] + xbuf[0] + xbuf[1] + xbuf[2]
    phase_z = [
        remote(sum_ref, zbuf.at[n], mod_send.at[3 + n], mod_recv.at[3 + n], *peer) for n, peer in enumerate(zs)
    ]
    for copy in phase_z:
        copy.start()
    for load in loads[7:]:
        load.wait()
    for copy in phase_z:
        copy.wait()
    whole = sum_ref[...] + zbuf[0] + zbuf[1] + zbuf[2]
    own_ref[...] = whole[0:4]
    gate_row_ref[...] = whole[4:5]
    phase_t = [
        remote(own_ref, tbuf.at[t], mod_send.at[6 + n], mod_recv.at[6 + n], "tp", peer)
        for n, peer in enumerate(targets)
    ]
    for copy in phase_t:
        copy.start()
    tbuf[t] = own_ref[...]
    wide = own_ref.shape[1]

    def piece(n, block):
        cols = pl.ds(pl.multiple_of(block * wide, wide), wide)
        gain = gain_ref[:, cols]
        rows = tbuf[block]
        slot = n % 2
        for src_ref, base, count, s in ((lat_ref, 0, n_lat, 0), (ctx_ref, n_lat, n_ctx, 1)):
            a = gain * (1.0 + rows[2 + s : 3 + s, :])
            b = rows[s : s + 1, :]
            x = src_ref[:, cols].astype(F32)
            inv = inv_ref[base : base + count, :]
            y = [
                x[:, j : j + TILE] * inv * a[:, j : j + TILE] + b[:, j : j + TILE] for j in range(0, wide, TILE)
            ]
            piece_ref[slot, base : base + count, :] = jnp.concatenate(y, axis=1).astype(BF16)
        m = piece_ref[slot]
        acc_ref[0] += jnp.dot(m, w_ref[0, cols, :], preferred_element_type=F32)
        acc_ref[1] += jnp.dot(m, w_ref[1, cols, :], preferred_element_type=F32)
        acc_ref[2, 0:n_lat] += jnp.dot(m[0:n_lat], w_ref[2, cols, :], preferred_element_type=F32)
        pre_acc[0:n_all, 0:64] += mm_nt(m, wg_ref[:, cols])

    piece(0, t)
    for n, block in enumerate(sources):
        phase_t[n].wait_recv()
        piece(n + 1, block)
    k_ref[...] = acc_ref[0].astype(BF16)
    v_ref[...] = acc_ref[1].astype(BF16)
    q_ref[...] = acc_ref[2, 0:n_lat].astype(BF16)
    for j in range(0, n_lat + TILE, TILE):
        rounded = pre_acc[j : j + TILE, :].astype(BF16).astype(F32)
        pre_ref[:, j : j + TILE] = jnp.transpose(rounded)[0:64]
    mix_tokens(
        q_ref, k_ref, v_ref, pre_ref, gate_row_ref, hg_ref, wb_ref, db_ref, lr_ref, lat_ref, ow_ref, out_ref, *scratch
    )
    for copy in phase_t:
        copy.wait_send()


def body(
    latent, context, condition, context_condition, shift_weight, scale_weight, gate_weight, norm_gain,
    query_weight, key_weight, value_weight, write_weight, decay_weight, write_bias, decay_bias, log_rate,
    head_gain, out_weight,
):
    n_lat, d = latent.shape
    n_ctx = context.shape[0]
    n_all = n_lat + n_ctx
    own_cols = gate_weight.shape[1]
    pair = query_weight.shape[1]
    blocks = n_lat // TILE
    tiles = 4 * blocks + 2
    width = n_lat + TILE
    vm = pl.BlockSpec(memory_space=pltpu.VMEM)
    hb = pl.BlockSpec(memory_space=pltpu.HBM)
    gates = [jnp.transpose(w, (1, 2, 0)).reshape(32, -1) for w in (write_weight, decay_weight)]
    shape = jax.ShapeDtypeStruct
    one_map = (TILE, 2 * TILE)
    small = write_bias.shape
    return pl.pallas_call(
        mixer_kernel,
        out_shape=pltpu.VMEM((n_lat, own_cols), BF16),
        in_specs=[hb] * 18,
        out_specs=vm,
        scratch_shapes=[
            pltpu.VMEM((n_lat, pair), BF16), pltpu.VMEM((n_all, pair), BF16), pltpu.VMEM((n_all, pair), BF16),
            pltpu.VMEM((64, width), F32), pltpu.VMEM((1, own_cols), F32),
            pltpu.VMEM(condition.shape, BF16), pltpu.VMEM(condition.shape, BF16),
            pltpu.VMEM((3, *shift_weight.shape), BF16), pltpu.VMEM((1, d), F32), pltpu.VMEM((64, d), BF16),
            pltpu.VMEM((n_lat, d), BF16), pltpu.VMEM((n_ctx, d), BF16), pltpu.VMEM((3, d, pair), BF16),
            pltpu.SMEM(small, F32), pltpu.SMEM(small, F32), pltpu.SMEM(small, F32), pltpu.VMEM((1, TILE), F32),
            pltpu.VMEM(out_weight.shape, BF16), pltpu.SemaphoreType.DMA((18,)),
            pltpu.VMEM((n_all, TILE), F32), pltpu.VMEM((2, n_all, own_cols), BF16),
            pltpu.VMEM((3, n_all, pair), F32), pltpu.VMEM((width, TILE), F32),
            pltpu.VMEM((8, own_cols), F32), pltpu.VMEM((8, own_cols), F32),
            pltpu.VMEM((4, own_cols), F32), pltpu.VMEM((3, 8, own_cols), F32), pltpu.VMEM((3, 8, own_cols), F32),
            pltpu.VMEM((8, 4, own_cols), F32), pltpu.SemaphoreType.DMA((13,)), pltpu.SemaphoreType.DMA((13,)),
            pltpu.VMEM((TILE, width), F32), pltpu.VMEM((width, TILE), F32),
            pltpu.VMEM((2, n_lat, n_lat), F32), pltpu.VMEM((2, n_lat, n_lat), F32), pltpu.VMEM((4, n_lat, n_lat), F32),
            pltpu.VMEM((tiles, TILE, TILE), BF16), pltpu.VMEM((tiles, TILE, TILE), BF16),
            pltpu.VMEM((4, n_lat, n_lat), BF16), pltpu.VMEM((4, n_lat, n_lat), BF16),
            pltpu.VMEM((4, n_lat, 2 * TILE), BF16), pltpu.VMEM((4, n_lat, 2 * TILE), BF16),
            pltpu.VMEM((2, n_lat, TILE), F32), pltpu.VMEM((2, n_lat, 2 * TILE), BF16),
            pltpu.VMEM((4, *one_map), BF16), pltpu.VMEM((4, *one_map), BF16),
            pltpu.VMEM((4, *one_map), BF16), pltpu.VMEM((4, *one_map), BF16),
            pltpu.VMEM((4, *one_map), F32), pltpu.VMEM(one_map, BF16), pltpu.VMEM(one_map, BF16),
            pltpu.VMEM((4, *one_map), BF16), pltpu.VMEM((4, *one_map), BF16),
            pltpu.VMEM((4, TILE, TILE), BF16), pltpu.VMEM((4, TILE, TILE), BF16),
            pltpu.VMEM((8, n_lat, pair), BF16), pltpu.VMEM((n_lat, own_cols), F32),
            pltpu.SemaphoreType.DMA((15,)), pltpu.SemaphoreType.DMA((15,)),
            pltpu.SemaphoreType.DMA((len(HANDS),)), pltpu.SemaphoreType.DMA((len(HANDS),)),
        ],
        compiler_params=pltpu.CompilerParams(
            collective_id=0, has_side_effects=True, vmem_limit_bytes=VMEM_LIMIT
        ),
        name="mixer",
    )(
        condition, context_condition, shift_weight, scale_weight, gate_weight, norm_gain.reshape(1, -1), *gates,
        latent, context, query_weight, key_weight, value_weight, write_bias, decay_bias, log_rate,
        head_gain.reshape(1, -1), out_weight,
    )


def solution(mesh):
    torus = Mesh(mesh.devices.reshape(4, 4, mesh.shape["tp"]), ("sp_0", "sp_1", "tp"))
    placed = (
        P(SP, None), P(SP, None), P(SP), P(SP), P(SP, "tp"), P(SP, "tp"), P(SP, "tp"), P(),
        P(None, "tp"), P(None, "tp"), P(None, "tp"), P(), P(), P(), P(), P(), P(), P(None, "tp"),
    )
    return jax.shard_map(body, mesh=torus, in_specs=placed, out_specs=P(SP, "tp"), check_vma=False)
```

```python
import jax
import jax.numpy as jnp
from jax import lax
from jax.experimental import pallas as pl
from jax.experimental.pallas import tpu as pltpu
from jax.sharding import Mesh
from jax.sharding import PartitionSpec as P

HEAD_DIM = 128
SP = ("sp_0", "sp_1")
EPS = 0.0001
F32 = jnp.float32
BF16 = jnp.bfloat16
TILE = 128
VMEM_LIMIT = 63_000_000
MESH = pl.DeviceIdType.MESH
LEVELS = (1, 2, 3, 4, 5, 6)


def mm(a, b):
    return jnp.dot(a.astype(BF16), b.astype(BF16), preferred_element_type=F32)


def mm_nt(a, b):
    return lax.dot_general(a, b, (((1,), (1,)), ((), ())), preferred_element_type=F32)


def mm_tn(a, b):
    return lax.dot_general(a, b, (((0,), (0,)), ((), ())), preferred_element_type=F32)


def iota2(shape, dim):
    return lax.broadcasted_iota(jnp.int32, shape, dim)


def softplus(u):
    return jnp.maximum(u, 0.0) + jnp.log1p(jnp.exp(-jnp.abs(u)))


def inv_norm(rows_bf16):
    r = rows_bf16.astype(F32)
    return lax.rsqrt(jnp.sum(r * r, axis=-1, keepdims=True) + EPS)


def gate_rows(first_head, pre_ref, wb_ref, db_ref, lr_ref, rows_ref, n_lat, n_ctx):
    width = n_lat + TILE
    lane = iota2((8, width), 1)
    is_ctx = lane >= n_lat
    pos = jnp.where(is_ctx, lane - n_lat, lane)
    size = jnp.where(is_ctx, n_ctx, n_lat)
    valid = pos < size
    row = iota2((8, width), 0)
    rates = jnp.zeros((8, width), F32)
    logd = jnp.zeros((8, width), F32)
    for c in range(4):
        d, h = c // 2, c % 2
        head = first_head + h
        at = d * 16 + head
        w = pre_ref[pl.ds(at, 1), :] + wb_ref[d, head]
        u = pre_ref[pl.ds(32 + at, 1), :] + db_ref[d, head]
        rate = 1.0 / (1.0 + jnp.exp(-w))
        step = -jnp.exp(jnp.full((1, width), lr_ref[d, head], F32)) * softplus(u)
        rates = jnp.where(row == c, rate, rates)
        logd = jnp.where(row == c, step, logd)
    rates = jnp.where(valid, rates, 0.0)
    logd = jnp.where(valid, logd, 0.0)
    fwd = logd
    bwd = logd
    s = 1
    while s < n_lat:
        ahead = [jnp.where(pos >= m * s, pltpu.roll(fwd, m * s, 1), 0.0) for m in range(1, 8)]
        after = [jnp.where(pos + m * s < size, pltpu.roll(bwd, width - m * s, 1), 0.0) for m in range(1, 8)]
        fwd = fwd + (((ahead[0] + ahead[1]) + (ahead[2] + ahead[3])) + ((ahead[4] + ahead[5]) + ahead[6]))
        bwd = bwd + (((after[0] + after[1]) + (after[2] + after[3])) + ((after[4] + after[5]) + after[6]))
        s *= 8
    g = jnp.where(row < 2, fwd, bwd)
    g = jnp.where(valid, g, 0.0)
    whole_lat = jnp.sum(jnp.where(is_ctx, 0.0, logd), axis=1, keepdims=True)
    whole_ctx = jnp.sum(jnp.where(is_ctx, logd, 0.0), axis=1, keepdims=True)
    late = jnp.exp(jnp.where(is_ctx, whole_ctx, whole_lat) - g)
    eg = jnp.exp(g)
    parts = []
    for a in (rates, g, late, eg):
        up = pltpu.roll(pltpu.roll(a, n_ctx, 1), 6, 0)
        a = jnp.where(lane >= n_lat + n_ctx, up, a)
        parts.append(a)
    rows_ref[...] = jnp.zeros_like(rows_ref)
    for n, a in enumerate(parts):
        rows_ref[8 * n : 8 * n + 8, :] = a
    return jnp.exp(whole_lat), jnp.exp(whole_ctx)


def split_rows(x):
    hi = x.astype(BF16)
    lo = (x - hi.astype(F32)).astype(BF16)
    return hi, lo


def mul_precise(m_bf16, x):
    hi, lo = split_rows(x)
    n = x.shape[1]
    y = jnp.dot(m_bf16, jnp.concatenate([hi, lo], axis=1), preferred_element_type=F32)
    return y[:, :n] + y[:, n:]


def then(next_map, total):
    y = mm(next_map[:, :TILE], total)
    zero = jnp.zeros((TILE, TILE), F32)
    return y + jnp.concatenate([zero, next_map[:, TILE:].astype(F32)], axis=1)


RATE, G, LATE, EG, KINV = 0, 8, 16, 24, 32


HANDS = (
    "u0", "u1", "u2", "u3", "d0", "d1", "d2", "d3", "mA", "mB", "ru0", "ru1", "rd2", "rd3",
    "mdA", "mdB", "muA", "muB", "ma0", "ma1", "ma2", "ma3",
)


def remote(src, dst, send_sem, recv_sem, axis, peer):
    return pltpu.make_async_remote_copy(
        src_ref=src, dst_ref=dst, send_sem=send_sem, recv_sem=recv_sem, device_id={axis: peer}, device_id_type=MESH
    )


def greet(barrier, peers):
    for axis, peer in peers:
        pl.semaphore_signal(barrier, inc=1, device_id={axis: peer}, device_id_type=MESH)


def ring_peers(axis, size):
    me = lax.axis_index(axis)
    return [(axis, lax.rem(me + k, size)) for k in range(1, size)]


def inverses(ad_ref, t_ref, base, count):
    xor = iota2((TILE, TILE), 0) ^ iota2((TILE, TILE), 1)
    eye = jnp.where(xor == 0, 1.0, 0.0).astype(BF16)
    near = jnp.where(xor == 1, 1.0, 0.0).astype(BF16)
    ts = [eye - ad_ref[base + n] * near for n in range(count)]
    for level in LEVELS:
        keep = jnp.where((xor >> level) == 1, 1.0, 0.0).astype(BF16)
        xs = [mm(ts[n], ad_ref[base + n] * keep).astype(BF16) for n in range(count)]
        ts = [t - mm(x, t).astype(BF16) for x, t in zip(xs, ts)]
    for n in range(count):
        t_ref[base + n] = ts[n]


def mix_tokens(
    q_ref, k_ref, v_ref, pre_ref, gate_row_ref, gain_ref, wb_ref, db_ref, lr_ref, lat_ref, ow_ref,
    out_ref,
    rows_ref, cols_ref, gk_ref, qk_ref, dm_ref, ad_ref, t_ref, ao_ref, p_ref, x_ref, xl_ref, o1_ref, q2_ref,
    lat_map, ctx_map, lat_all, ctx_all, prefix_ref, lat_total, ctx_total, lat_totals, ctx_totals,
    start_ref, mine_ref, ho_ref, acc_out, send_sem, recv_sem, ho_send, ho_recv,
):
    n_lat = q_ref.shape[0]
    n_ctx = k_ref.shape[0] - n_lat
    blocks = n_lat // TILE
    width = n_lat + TILE
    x_at, z_at, t_at = lax.axis_index("sp_1"), lax.axis_index("sp_0"), lax.axis_index("tp")
    y_at, core = t_at // 2, lax.rem(t_at, 2)
    up = lax.rem(y_at + 1, 4) * 2 + core
    down = lax.rem(y_at + 3, 4) * 2 + core
    across = lax.rem(y_at + 2, 4) * 2 + core
    mate = y_at * 2 + 1 - core
    xs, zs = ring_peers("sp_1", 4), ring_peers("sp_0", 4)
    own_cols = out_ref.shape[1]

    dec_lat, dec_ctx = gate_rows(t_at * 2, pre_ref, wb_ref, db_ref, lr_ref, rows_ref, n_lat, n_ctx)
    for b in range(blocks + 1):
        cols_ref[b * TILE : (b + 1) * TILE, :] = jnp.transpose(rows_ref[:, b * TILE : (b + 1) * TILE])

    def kcols(h):
        return k_ref[0:n_lat, h * TILE : (h + 1) * TILE]

    def kctx(h):
        kc = k_ref[n_lat : n_lat + n_ctx, h * TILE : (h + 1) * TILE]
        return jnp.concatenate([kc, kc], axis=0)

    def vctx(h):
        vc = v_ref[n_lat : n_lat + n_ctx, h * TILE : (h + 1) * TILE]
        return jnp.concatenate([vc, vc], axis=0)

    kinv = []
    for h in range(2):
        kinv.append(jnp.concatenate([inv_norm(kcols(h)), inv_norm(kctx(h))], axis=0))
    lane128 = iota2((width, TILE), 1)
    both = jnp.where(lane128 == 0, kinv[0], jnp.where(lane128 == 1, kinv[1], 0.0))
    ii = iota2((TILE, TILE), 0)
    jj = iota2((TILE, TILE), 1)
    xor = ii ^ jj
    for b in range(blocks + 1):
        rows_ref[:, b * TILE : (b + 1) * TILE] = jnp.where(
            ii < KINV,
            rows_ref[:, b * TILE : (b + 1) * TILE],
            pltpu.roll(jnp.transpose(both[b * TILE : (b + 1) * TILE, :]), KINV, 0),
        )

    for h in range(2):
        kc = kctx(h)
        g2 = mm_nt(kc, kc) * kinv[h][n_lat:] * rows_ref[KINV + h : KINV + h + 1, n_lat:]
        keep = jnp.where(ii < n_ctx, jnp.where(jj < ii, 1, 0), jnp.where(jj > ii, 1, 0))
        keep = jnp.where((ii < n_ctx) == (jj < n_ctx), keep, 0) == 1
        sp = cols_ref[n_lat:, G + h : G + h + 1] - rows_ref[G + h : G + h + 1, n_lat:]
        dm = jnp.where(keep, jnp.exp(jnp.where(keep, sp, 0.0)), 0.0)
        ad_ref[4 * blocks + h] = (g2 * dm * cols_ref[n_lat:, RATE + h : RATE + h + 1]).astype(BF16)
    def to_row(base, maps, everyone):
        copies = [
            remote(maps.at[peer], everyone.at[x_at], send_sem.at[base + n], recv_sem.at[base + n], axis, peer)
            for n, (axis, peer) in enumerate(xs)
        ]
        for copy in copies:
            copy.start()
        everyone[x_at] = maps[x_at]
        return copies

    def to_column(base, total, everyone):
        copies = [
            remote(total, everyone.at[z_at], send_sem.at[base + n], recv_sem.at[base + n], axis, peer)
            for n, (axis, peer) in enumerate(zs)
        ]
        for copy in copies:
            copy.start()
        everyone[z_at] = total[...]
        return copies

    krows = []
    for h in range(2):
        krows.append(jnp.log(rows_ref[KINV + h : KINV + h + 1, 0:n_lat]))
        gk_ref[h] = mm_nt(kcols(h), kcols(h))
    for c in range(4):
        d, h = c // 2, c % 2
        for i in range(blocks):
            ri = cols_ref[i * TILE : (i + 1) * TILE, RATE + c : RATE + c + 1] * kinv[h][i * TILE : (i + 1) * TILE]
            gi = cols_ref[i * TILE : (i + 1) * TILE, G + c : G + c + 1]
            for j in range(blocks):
                if (d == 0 and j > i) or (d == 1 and j < i):
                    continue
                at = (slice(i * TILE, (i + 1) * TILE), slice(j * TILE, (j + 1) * TILE))
                cj = slice(j * TILE, (j + 1) * TILE)
                sp = gi - (rows_ref[G + c : G + c + 1, cj] - krows[h][:, cj])
                if i == j:
                    keep = (ii >= jj) if d == 0 else (ii <= jj)
                    dm = jnp.where(keep, jnp.exp(jnp.where(keep, sp, 0.0)), 0.0)
                else:
                    dm = jnp.exp(sp)
                a = gk_ref[(h, *at)] * dm * ri
                if i == j:
                    ad_ref[c * blocks + i] = jnp.where(ii == jj, 0.0, a).astype(BF16)
                else:
                    ao_ref[(c, *at)] = a.astype(BF16)
                dm_ref[(c, *at)] = dm

    inverses(ad_ref, t_ref, 4 * blocks, 2)
    for h in range(2):
        ci = kinv[h][n_lat:]
        cr = slice(n_lat, n_lat + TILE)
        rate = cols_ref[cr, RATE + h : RATE + h + 1]
        eg = cols_ref[cr, EG + h : EG + h + 1]
        late = cols_ref[cr, LATE + h : LATE + h + 1]
        kc = kctx(h)
        b = jnp.concatenate([vctx(h).astype(F32) * rate, kc.astype(F32) * (rate * eg * ci)], axis=1)
        x = mm(t_ref[4 * blocks + h], b)
        xl = (x * (late * ci)).astype(BF16)
        for d in range(2):
            c = d * 2 + h
            m = mm_tn(kc[0:n_ctx], xl[d * n_ctx : (d + 1) * n_ctx])
            diag = jnp.where(xor == 0, dec_ctx[c : c + 1, :], 0.0)
            ctx_map[c] = jnp.concatenate([diag - m[:, TILE:], m[:, :TILE]], axis=1).astype(BF16)

    ctx_rows = to_row(0, ctx_map, ctx_all)

    inverses(ad_ref, t_ref, 0, 4 * blocks)

    backwards = x_at >= 2

    def place(n, size):
        return jnp.where(backwards, size - 1 - n, n)

    lates, fronts, sides = {}, {}, {}
    for n in range(blocks):
        for c in range(4):
            d, h = c // 2, c % 2
            i = n if d == 0 else blocks - 1 - n
            r = slice(i * TILE, (i + 1) * TILE)
            rate = cols_ref[r, RATE + c : RATE + c + 1]
            ki = kinv[h][r]
            vi = v_ref[r, h * TILE : (h + 1) * TILE].astype(F32) * rate
            wi = k_ref[r, h * TILE : (h + 1) * TILE].astype(F32) * (rate * cols_ref[r, EG + c : EG + c + 1] * ki)
            lates[c, n] = cols_ref[r, LATE + c : LATE + c + 1] * ki
            t = t_ref[c * blocks + i]
            fronts[c, n] = mm(t, jnp.concatenate([vi, wi], axis=1))
            if n > 0:
                done = slice(0, i * TILE) if d == 0 else slice((i + 1) * TILE, n_lat)
                sides[c, n] = mm(t, ao_ref[c, r, done]).astype(BF16)
    for n in range(blocks):
        for c in range(4):
            d = c // 2
            i = n if d == 0 else blocks - 1 - n
            r = slice(i * TILE, (i + 1) * TILE)
            x = fronts[c, n]
            if n > 0:
                done = slice(0, i * TILE) if d == 0 else slice((i + 1) * TILE, n_lat)
                x = x - mm(sides[c, n], x_ref[c, done, :])
            x_ref[c, r, :] = x.astype(BF16)
            xl_ref[c, r, :] = (x * lates[c, n]).astype(BF16)
    for c in range(4):
        m = mm_tn(kcols(c % 2), xl_ref[c])
        diag = jnp.where(xor == 0, dec_lat[c : c + 1, :], 0.0)
        lat_map[c] = jnp.concatenate([diag - m[:, TILE:], m[:, :TILE]], axis=1).astype(BF16)
    lat_rows = to_row(6, lat_map, lat_all)

    qinvs = []
    for h in range(2):
        qh = q_ref[0:n_lat, h * TILE : (h + 1) * TILE]
        qinv = inv_norm(qh) * (HEAD_DIM**-0.5)
        qinvs.append(qinv)
        qk_ref[h] = mm_nt(qh, kcols(h)) * qinv
    for c in range(4):
        d, h = c // 2, c % 2
        for i in range(blocks):
            r = slice(i * TILE, (i + 1) * TILE)
            seen = slice(0, (i + 1) * TILE) if d == 0 else slice(i * TILE, n_lat)
            p_ref[c, r, seen] = (qk_ref[h, r, seen] * dm_ref[c, r, seen]).astype(BF16)
    for h in range(2):
        o1 = []
        for d in range(2):
            c = d * 2 + h
            for i in range(blocks):
                r = slice(i * TILE, (i + 1) * TILE)
                seen = slice(0, (i + 1) * TILE) if d == 0 else slice(i * TILE, n_lat)
                ow = mm(p_ref[c, r, seen], x_ref[c, seen, :])
                qi = q_ref[r, h * TILE : (h + 1) * TILE].astype(F32)
                early = qi * (cols_ref[r, EG + c : EG + c + 1] * qinvs[h][r])
                q2_ref[h, r, d * TILE : (d + 1) * TILE] = (early - ow[:, TILE:]).astype(BF16)
                if d == 0:
                    o1.append(ow[:, :TILE])
                else:
                    o1_ref[h, r, :] = o1[i] + ow[:, :TILE]

    for copy in ctx_rows:
        copy.wait()
    total = ctx_all[place(0, 4)].astype(F32)
    for n in range(1, 4):
        total = then(ctx_all[place(n, 4)], total)
    ctx_total[...] = total.astype(BF16)
    ctx_columns = to_column(3, ctx_total, ctx_totals)

    for copy in lat_rows:
        copy.wait()
    low = lat_all[place(0, 4)].astype(F32)
    pair = then(lat_all[place(1, 4)], low)
    lat_total[...] = then(then(lat_all[place(3, 4)], lat_all[place(2, 4)].astype(F32)), pair).astype(BF16)
    lat_columns = to_column(9, lat_total, lat_totals)
    prefix_ref[place(1, 4)] = low
    prefix_ref[place(2, 4)] = pair
    prefix_ref[place(3, 4)] = then(lat_all[place(2, 4)], pair)
    for copy in ctx_columns:
        copy.wait()
    state = None
    for n in range(4):
        one = ctx_totals[place(n, 4)]
        off = one[:, TILE:].astype(F32)
        state = off if n == 0 else mul_precise(one[:, :TILE], state) + off
    for copy in lat_columns:
        copy.wait()
    z_place = place(z_at, 4)
    for n in range(3):
        one = lat_totals[place(n, 4)]
        new = mul_precise(one[:, :TILE], state) + one[:, TILE:].astype(F32)
        state = jnp.where(n < z_place, new, state)
    start_ref[place(0, 4)] = state.astype(BF16)
    for n in range(1, 4):
        at = place(n, 4)
        mk = prefix_ref[at]
        start_ref[at] = (mul_precise(mk[:, :TILE].astype(BF16), state) + mk[:, TILE:]).astype(BF16)
    starts = to_row(12, start_ref, mine_ref)
    for copy in starts:
        copy.wait()

    quarter = n_lat // 4
    Q = [slice(n * quarter, (n + 1) * quarter) for n in range(4)]
    A, B = slice(0, n_lat // 2), slice(n_lat // 2, n_lat)
    both_s = [jnp.concatenate([mine_ref[h], mine_ref[2 + h]], axis=0) for h in range(2)]

    def finish(r):
        for h in range(2):
            y = o1_ref[h, r, :] + jnp.dot(q2_ref[h, r, :], both_s[h], preferred_element_type=F32)
            y = y * lax.rsqrt(jnp.mean(y * y, axis=-1, keepdims=True) + EPS) * gain_ref[...]
            ho_ref[t_at, r, h * TILE : (h + 1) * TILE] = y.astype(BF16)

    def other(block):
        return block + 1 - 2 * core

    hands = {}

    def hand(name, block, r, peer):
        n = HANDS.index(name)
        hands[name] = remote(ho_ref.at[block, r], ho_ref.at[block, r], ho_send.at[n], ho_recv.at[n], "tp", peer)
        hands[name].start()

    def got(*names):
        for name in names:
            hands[name].wait_recv()

    depth = 2 * TILE

    def add(block, r=slice(None)):
        w = ow_ref[pl.ds(pl.multiple_of(block * depth, depth), depth), :]
        return jnp.dot(ho_ref[block, r], w, preferred_element_type=F32)

    finish(Q[0])
    finish(Q[3])
    hand("u0", t_at, Q[0], up)
    hand("d3", t_at, Q[3], down)
    finish(Q[1])
    finish(Q[2])
    hand("u1", t_at, Q[1], up)
    hand("d2", t_at, Q[2], down)
    hand("mA", t_at, A, mate)
    hand("u2", t_at, Q[2], up)
    hand("u3", t_at, Q[3], up)
    hand("d1", t_at, Q[1], down)
    hand("d0", t_at, Q[0], down)
    hand("mB", t_at, B, mate)
    acc_out[...] = add(t_at)
    got("mA", "mB")
    acc_out[...] += add(mate)
    got("u0")
    hand("ru0", down, Q[0], up)
    got("d3")
    hand("rd3", up, Q[3], down)
    got("u1")
    hand("ru1", down, Q[1], up)
    hand("mdA", down, A, mate)
    got("d2")
    hand("rd2", up, Q[2], down)
    hand("muB", up, B, mate)
    got("u2", "u3")
    hand("mdB", down, B, mate)
    got("d1", "d0")
    hand("muA", up, A, mate)
    acc_out[...] += add(down) + add(up)
    got("ru0")
    hand("ma0", across, Q[0], mate)
    got("rd3")
    hand("ma3", across, Q[3], mate)
    got("mdA", "mdB", "muA", "muB")
    acc_out[...] += add(other(down)) + add(other(up))
    got("ru1")
    hand("ma1", across, Q[1], mate)
    got("rd2")
    hand("ma2", across, Q[2], mate)
    acc_out[...] += add(across)
    gate = gate_row_ref[...]
    own = pl.ds(pl.multiple_of(t_at * own_cols, own_cols), own_cols)
    got("ma0", "ma3", "ma1")
    for r in (A, Q[3]):
        total = acc_out[r, :] + add(other(across), r)
        out_ref[r, :] = (lat_ref[r, own].astype(F32) + gate * total).astype(BF16)
    got("ma2")
    total = acc_out[Q[2], :] + add(other(across), Q[2])
    out_ref[Q[2], :] = (lat_ref[Q[2], own].astype(F32) + gate * total).astype(BF16)
    for name in HANDS:
        hands[name].wait_send()


def mixer_kernel(
    cond_hbm, cctx_hbm, shift_hbm, scale_hbm, gate_hbm, gain_hbm, ww_hbm, wd_hbm,
    lat_hbm, ctx_hbm, wq_hbm, wk_hbm, wv_hbm, wb_hbm, db_hbm, lr_hbm, hg_hbm, ow_hbm,
    out_ref,
    q_ref, k_ref, v_ref, pre_ref, gate_row_ref,
    cond_ref, cctx_ref, mod_w_ref, gain_ref, wg_ref, lat_ref, ctx_ref, w_ref, wb_ref, db_ref, lr_ref, hg_ref, ow_ref,
    load_sem, inv_ref, piece_ref, acc_ref, pre_acc,
    part_ref, sum_ref, own_ref, xbuf, zbuf, tbuf, mod_send, mod_recv, *scratch,
):
    barrier = pltpu.get_barrier_semaphore()
    t = lax.axis_index("tp")
    y_at, core = t // 2, lax.rem(t, 2)
    up = lax.rem(y_at + 1, 4) * 2 + core
    down = lax.rem(y_at + 3, 4) * 2 + core
    across = lax.rem(y_at + 2, 4) * 2 + core

    def other(block):
        return block + 1 - 2 * core

    targets = [other(t), up, down, other(up), other(down), across, other(across)]
    sources = [other(t), down, up, other(down), other(up), across, other(across)]
    xs, zs = ring_peers("sp_1", 4), ring_peers("sp_0", 4)
    greet(barrier, xs + zs + [("tp", peer) for peer in targets])
    loads = [
        pltpu.make_async_copy(src, dst, load_sem.at[n])
        for n, (src, dst) in enumerate(
            (
                (cond_hbm, cond_ref), (cctx_hbm, cctx_ref), (shift_hbm, mod_w_ref.at[0]), (scale_hbm, mod_w_ref.at[1]),
                (gate_hbm, mod_w_ref.at[2]), (lat_hbm, lat_ref), (ctx_hbm, ctx_ref), (gain_hbm, gain_ref),
                (ww_hbm, wg_ref.at[0:32]), (wd_hbm, wg_ref.at[32:64]),
                (wk_hbm, w_ref.at[0]), (wv_hbm, w_ref.at[1]), (wq_hbm, w_ref.at[2]),
                (wb_hbm, wb_ref), (db_hbm, db_ref), (lr_hbm, lr_ref), (hg_hbm, hg_ref), (ow_hbm, ow_ref),
            )
        )
    ]
    for load in loads[:5]:
        load.start()
    n_lat, n_ctx = lat_ref.shape[0], ctx_ref.shape[0]
    n_all = n_lat + n_ctx
    acc_ref[...] = jnp.zeros_like(acc_ref)
    pre_acc[...] = jnp.zeros_like(pre_acc)
    part_ref[...] = jnp.zeros_like(part_ref)
    for load in loads[:5]:
        load.wait()
    for load in loads[5:7]:
        load.start()
    u = jnp.concatenate(
        [cond_ref[...].astype(F32).reshape(1, -1), cctx_ref[...].astype(F32).reshape(1, -1)], axis=0
    )
    silu = (u / (1.0 + jnp.exp(-u))).astype(BF16)
    part_ref[0:2, :] = jnp.dot(silu, mod_w_ref[0], preferred_element_type=F32)
    part_ref[2:4, :] = jnp.dot(silu, mod_w_ref[1], preferred_element_type=F32)
    part_ref[4:5, :] = jnp.dot(silu, mod_w_ref[2], preferred_element_type=F32)[0:1]
    pl.semaphore_wait(barrier, 13)
    phase_x = [
        remote(part_ref, xbuf.at[n], mod_send.at[n], mod_recv.at[n], *peer) for n, peer in enumerate(xs)
    ]
    for copy in phase_x:
        copy.start()
    for load in loads[5:7]:
        load.wait()
    for load in loads[7:]:
        load.start()

    def norms(src_ref, base):
        def step(i, carry):
            for j in range(4):
                x = src_ref[pl.ds(i * 64 + j * 16, 16), :].astype(F32)
                inv = lax.rsqrt(jnp.mean(x * x, axis=-1, keepdims=True) + EPS)
                inv_ref[pl.ds(base + i * 64 + j * 16, 16), :] = jnp.broadcast_to(inv, (16, TILE))
            return carry

        return step

    lax.fori_loop(0, n_lat // 64, norms(lat_ref, 0), 0)
    lax.fori_loop(0, n_ctx // 64, norms(ctx_ref, n_lat), 0)
    for copy in phase_x:
        copy.wait()
    sum_ref[...] = part_ref[...] + xbuf[0] + xbuf[1] + xbuf[2]
    phase_z = [
        remote(sum_ref, zbuf.at[n], mod_send.at[3 + n], mod_recv.at[3 + n], *peer) for n, peer in enumerate(zs)
    ]
    for copy in phase_z:
        copy.start()
    for load in loads[7:]:
        load.wait()
    for copy in phase_z:
        copy.wait()
    whole = sum_ref[...] + zbuf[0] + zbuf[1] + zbuf[2]
    own_ref[...] = whole[0:4]
    gate_row_ref[...] = whole[4:5]
    phase_t = [
        remote(own_ref, tbuf.at[t], mod_send.at[6 + n], mod_recv.at[6 + n], "tp", peer)
        for n, peer in enumerate(targets)
    ]
    for copy in phase_t:
        copy.start()
    tbuf[t] = own_ref[...]
    wide = own_ref.shape[1]

    def piece(n, block):
        cols = pl.ds(pl.multiple_of(block * wide, wide), wide)
        gain = gain_ref[:, cols]
        rows = tbuf[block]
        slot = n % 2
        for src_ref, base, count, s in ((lat_ref, 0, n_lat, 0), (ctx_ref, n_lat, n_ctx, 1)):
            a = gain * (1.0 + rows[2 + s : 3 + s, :])
            b = rows[s : s + 1, :]
            x = src_ref[:, cols].astype(F32)
            inv = inv_ref[base : base + count, :]
            y = [
                x[:, j : j + TILE] * inv * a[:, j : j + TILE] + b[:, j : j + TILE] for j in range(0, wide, TILE)
            ]
            piece_ref[slot, base : base + count, :] = jnp.concatenate(y, axis=1).astype(BF16)
        m = piece_ref[slot]
        pre_acc[0:n_all, 0:64] += mm_nt(m, wg_ref[:, cols])
        acc_ref[0] += jnp.dot(m, w_ref[0, cols, :], preferred_element_type=F32)
        acc_ref[1] += jnp.dot(m, w_ref[1, cols, :], preferred_element_type=F32)
        acc_ref[2, 0:n_lat] += jnp.dot(m[0:n_lat], w_ref[2, cols, :], preferred_element_type=F32)

    piece(0, t)
    for n, block in enumerate(sources):
        phase_t[n].wait_recv()
        piece(n + 1, block)
    k_ref[...] = acc_ref[0].astype(BF16)
    v_ref[...] = acc_ref[1].astype(BF16)
    q_ref[...] = acc_ref[2, 0:n_lat].astype(BF16)
    for j in range(0, n_lat + TILE, TILE):
        rounded = pre_acc[j : j + TILE, :].astype(BF16).astype(F32)
        pre_ref[:, j : j + TILE] = jnp.transpose(rounded)[0:64]
    mix_tokens(
        q_ref, k_ref, v_ref, pre_ref, gate_row_ref, hg_ref, wb_ref, db_ref, lr_ref, lat_ref, ow_ref, out_ref, *scratch
    )
    for copy in phase_t:
        copy.wait_send()


def body(
    latent, context, condition, context_condition, shift_weight, scale_weight, gate_weight, norm_gain,
    query_weight, key_weight, value_weight, write_weight, decay_weight, write_bias, decay_bias, log_rate,
    head_gain, out_weight,
):
    n_lat, d = latent.shape
    n_ctx = context.shape[0]
    n_all = n_lat + n_ctx
    own_cols = gate_weight.shape[1]
    pair = query_weight.shape[1]
    blocks = n_lat // TILE
    tiles = 4 * blocks + 2
    width = n_lat + TILE
    vm = pl.BlockSpec(memory_space=pltpu.VMEM)
    hb = pl.BlockSpec(memory_space=pltpu.HBM)
    gates = [jnp.transpose(w, (1, 2, 0)).reshape(32, -1) for w in (write_weight, decay_weight)]
    shape = jax.ShapeDtypeStruct
    one_map = (TILE, 2 * TILE)
    small = write_bias.shape
    return pl.pallas_call(
        mixer_kernel,
        out_shape=pltpu.VMEM((n_lat, own_cols), BF16),
        in_specs=[hb] * 18,
        out_specs=vm,
        scratch_shapes=[
            pltpu.VMEM((n_lat, pair), BF16), pltpu.VMEM((n_all, pair), BF16), pltpu.VMEM((n_all, pair), BF16),
            pltpu.VMEM((64, width), F32), pltpu.VMEM((1, own_cols), F32),
            pltpu.VMEM(condition.shape, BF16), pltpu.VMEM(condition.shape, BF16),
            pltpu.VMEM((3, *shift_weight.shape), BF16), pltpu.VMEM((1, d), F32), pltpu.VMEM((64, d), BF16),
            pltpu.VMEM((n_lat, d), BF16), pltpu.VMEM((n_ctx, d), BF16), pltpu.VMEM((3, d, pair), BF16),
            pltpu.SMEM(small, F32), pltpu.SMEM(small, F32), pltpu.SMEM(small, F32), pltpu.VMEM((1, TILE), F32),
            pltpu.VMEM(out_weight.shape, BF16), pltpu.SemaphoreType.DMA((18,)),
            pltpu.VMEM((n_all, TILE), F32), pltpu.VMEM((2, n_all, own_cols), BF16),
            pltpu.VMEM((3, n_all, pair), F32), pltpu.VMEM((width, TILE), F32),
            pltpu.VMEM((8, own_cols), F32), pltpu.VMEM((8, own_cols), F32),
            pltpu.VMEM((4, own_cols), F32), pltpu.VMEM((3, 8, own_cols), F32), pltpu.VMEM((3, 8, own_cols), F32),
            pltpu.VMEM((8, 4, own_cols), F32), pltpu.SemaphoreType.DMA((13,)), pltpu.SemaphoreType.DMA((13,)),
            pltpu.VMEM((TILE, width), F32), pltpu.VMEM((width, TILE), F32),
            pltpu.VMEM((2, n_lat, n_lat), F32), pltpu.VMEM((2, n_lat, n_lat), F32), pltpu.VMEM((4, n_lat, n_lat), F32),
            pltpu.VMEM((tiles, TILE, TILE), BF16), pltpu.VMEM((tiles, TILE, TILE), BF16),
            pltpu.VMEM((4, n_lat, n_lat), BF16), pltpu.VMEM((4, n_lat, n_lat), BF16),
            pltpu.VMEM((4, n_lat, 2 * TILE), BF16), pltpu.VMEM((4, n_lat, 2 * TILE), BF16),
            pltpu.VMEM((2, n_lat, TILE), F32), pltpu.VMEM((2, n_lat, 2 * TILE), BF16),
            pltpu.VMEM((4, *one_map), BF16), pltpu.VMEM((4, *one_map), BF16),
            pltpu.VMEM((4, *one_map), BF16), pltpu.VMEM((4, *one_map), BF16),
            pltpu.VMEM((4, *one_map), F32), pltpu.VMEM(one_map, BF16), pltpu.VMEM(one_map, BF16),
            pltpu.VMEM((4, *one_map), BF16), pltpu.VMEM((4, *one_map), BF16),
            pltpu.VMEM((4, TILE, TILE), BF16), pltpu.VMEM((4, TILE, TILE), BF16),
            pltpu.VMEM((8, n_lat, pair), BF16), pltpu.VMEM((n_lat, own_cols), F32),
            pltpu.SemaphoreType.DMA((15,)), pltpu.SemaphoreType.DMA((15,)),
            pltpu.SemaphoreType.DMA((len(HANDS),)), pltpu.SemaphoreType.DMA((len(HANDS),)),
        ],
        compiler_params=pltpu.CompilerParams(
            collective_id=0, has_side_effects=True, vmem_limit_bytes=VMEM_LIMIT
        ),
        name="mixer",
    )(
        condition, context_condition, shift_weight, scale_weight, gate_weight, norm_gain.reshape(1, -1), *gates,
        latent, context, query_weight, key_weight, value_weight, write_bias, decay_bias, log_rate,
        head_gain.reshape(1, -1), out_weight,
    )


def solution(mesh):
    torus = Mesh(mesh.devices.reshape(4, 4, mesh.shape["tp"]), ("sp_0", "sp_1", "tp"))
    placed = (
        P(SP, None), P(SP, None), P(SP), P(SP), P(SP, "tp"), P(SP, "tp"), P(SP, "tp"), P(),
        P(None, "tp"), P(None, "tp"), P(None, "tp"), P(), P(), P(), P(), P(), P(), P(None, "tp"),
    )
    return jax.shard_map(body, mesh=torus, in_specs=placed, out_specs=P(SP, "tp"), check_vma=False)
```
